32 devices in a mesh: sp: 8 (over z, x), tp: 4 (over y, core).
Axes of the slice: x: 2, y: 2, z: 4, core: 2. Of those that a mesh axis runs over, the one named last changes fastest.
Arguments:
- tokens: bfloat16 [4096, 2048], P('sp', 'tp'), may hold values from -400 to 400
- lru_in: bfloat16 [2048, 1024], P(None, 'tp'), may hold values from -0.125 to 0.125
- lru_gate_in: bfloat16 [2048, 1024], P(None, 'tp'), may hold values from -0.125 to 0.125
- query_w: bfloat16 [2048, 1024], P(None, 'tp'), may hold values from -1 to 1
- key_w: bfloat16 [2048, 1024], P(None, 'tp'), may hold values from -10 to 10
- value_w: bfloat16 [2048, 1024], P(None, 'tp'), may hold values from -0.125 to 0.125
- conv_weight: bfloat16 [4, 1024], replicated, may hold values from -3 to 3
- recur_gate_w: bfloat16 [16, 64, 64], replicated, may hold values from -0.75 to 0.75
- input_gate_w: bfloat16 [16, 64, 64], replicated, may hold values from -0.75 to 0.75
- rate_param: float32 [1024], replicated, may hold values from 0 to 16
- decay_extra: float32 [4096, 1024], P('sp', 'tp'), may hold values from -2 to 0
- forget_cum: float32 [4096, 8], P('sp', 'tp'), may hold values from -386 to 0, as said below
- out_lru: bfloat16 [1024, 2048], P('tp'), may hold values from -0.1875 to 0.1875
- out_fox: bfloat16 [1024, 2048], P('tp'), may hold values from -0.1875 to 0.1875
Outputs:
- mixed_out: bfloat16 [4096, 2048], P('sp', 'tp')
The draws below stay inside these ranges and needn't reach their ends.
Inputs may be any that keep to these rules, and one draw needn't show every extreme that they name: `forget_cum`: non-increasing along positions in every head.
All inputs are finite; a program needn't handle non-finite values.
Results may differ from the reference program's by a relative error of at most 0.014.
Values may be sent and summed in bfloat16 or wider, within the bound.
A program may use at most 64 MiB of HBM per device.

```python
import math
import jax
import jax.numpy as jnp
from jax import lax

D = 2048
LRU_W = 1024
LRU_BLOCKS = 16
BLOCK_W = 64
CONV_W = 4
FOX_HEADS = 8
HEAD_DIM = 128
FOX_W = 1024
TOKENS_PER_SHARD = 512
SEQUENCE_TOKENS = 4096


decay_sharpness = 8.0


def draw_tokens(key, part):
    random_subkeys = jax.random.split(key, 4)
    feature_scale = jnp.exp(jnp.linspace(0.0, math.log(4.0), D) + jax.random.uniform(random_subkeys[0], (D,), jnp.float32, -0.5, 0.5))
    row_scale = jnp.exp(jax.random.uniform(random_subkeys[1], (SEQUENCE_TOKENS, 1), jnp.float32, 0.0, math.log(10.0)))
    reference_level = jax.random.truncated_normal(random_subkeys[2], -4.0, 4.0, (SEQUENCE_TOKENS, D), jnp.float32)
    return (reference_level * feature_scale[None, :] * row_scale).astype(jnp.bfloat16)


def shared_query(key):
    return jax.random.truncated_normal(jax.random.fold_in(key, 11), -6.0, 6.0, (D, FOX_W), jnp.float32) * D ** (-0.5)


def draw_query_w(key, part):
    return shared_query(key).astype(jnp.bfloat16)


def draw_key_w(key, part):
    independent = jax.random.truncated_normal(jax.random.fold_in(key, 12), -6.0, 6.0, (D, FOX_W), jnp.float32) * D ** (-0.5)
    combined = 3.0 * independent
    return combined.astype(jnp.bfloat16)


def draw_rate_param(key, part):
    random_subkeys = jax.random.split(key, 3)
    ranking = jax.random.permutation(random_subkeys[0], LRU_W)
    slow_mask = ranking < LRU_W // 2
    slow_rate = jnp.exp(jax.random.uniform(random_subkeys[1], (LRU_W,), jnp.float32, math.log(0.2), math.log(0.8))) / (0.5 * decay_sharpness * SEQUENCE_TOKENS)
    fast_len = jnp.exp(jax.random.uniform(random_subkeys[2], (LRU_W,), jnp.float32, math.log(TOKENS_PER_SHARD / 16.0), math.log(TOKENS_PER_SHARD / 5.0)))
    fast_rate = 1.0 / (0.5 * decay_sharpness * fast_len)
    softplus_value = jnp.where(slow_mask, slow_rate, fast_rate)
    return -jnp.log(jnp.expm1(softplus_value))


def draw_decay_extra(key, part):
    random_subkeys = jax.random.split(key, 4)
    multiplier = jnp.exp(jax.random.uniform(random_subkeys[0], (SEQUENCE_TOKENS // TOKENS_PER_SHARD,), jnp.float32, math.log(0.4), math.log(1.6)))
    jaggedness = jax.random.uniform(random_subkeys[1], (SEQUENCE_TOKENS, LRU_W), jnp.float32, 0.2, 1.8)
    reference_level = -jnp.repeat(multiplier, TOKENS_PER_SHARD)[:, None] * jaggedness * (0.4 / SEQUENCE_TOKENS)
    spike_position = jax.random.randint(random_subkeys[2], (3,), 0, SEQUENCE_TOKENS)
    spike_penalty = jnp.log(jax.random.uniform(random_subkeys[3], (3,), jnp.float32, 0.6, 0.8))
    spike_events = jnp.zeros((SEQUENCE_TOKENS,), jnp.float32).at[spike_position].add(spike_penalty)
    return reference_level + spike_events[:, None]


def draw_forget_cum(key, part):
    random_subkeys = jax.random.split(key, 7)
    ranking = jax.random.permutation(random_subkeys[0], FOX_HEADS)
    slow_mask = ranking < FOX_HEADS // 2
    slow_rate = jnp.exp(jax.random.uniform(random_subkeys[1], (FOX_HEADS,), jnp.float32, math.log(0.3), math.log(1.0))) / SEQUENCE_TOKENS
    fast_len = jnp.exp(jax.random.uniform(random_subkeys[2], (FOX_HEADS,), jnp.float32, math.log(TOKENS_PER_SHARD / 16.0), math.log(TOKENS_PER_SHARD / 5.0)))
    head_decay_rate = jnp.where(slow_mask, slow_rate, 1.0 / fast_len)
    multiplier = jnp.exp(jax.random.uniform(random_subkeys[3], (SEQUENCE_TOKENS // TOKENS_PER_SHARD,), jnp.float32, math.log(0.4), math.log(1.6)))
    jaggedness = jax.random.uniform(random_subkeys[4], (SEQUENCE_TOKENS, FOX_HEADS), jnp.float32, 0.2, 1.8)
    spike_position = jax.random.randint(random_subkeys[5], (3,), 0, SEQUENCE_TOKENS)
    spike_penalty = jnp.log(jax.random.uniform(random_subkeys[6], (3,), jnp.float32, 0.6, 0.8))
    spike_events = jnp.zeros((SEQUENCE_TOKENS,), jnp.float32).at[spike_position].add(spike_penalty)
    logarithmic_steps = -head_decay_rate[None, :] * jnp.repeat(multiplier, TOKENS_PER_SHARD)[:, None] * jaggedness + spike_events[:, None]
    return jnp.cumsum(logarithmic_steps, axis=0)


def strengthened(values, own_key, source, target, parts, factor):
    def block_of(dim):
        return (jnp.arange(values.shape[dim]) // (values.shape[dim] // parts)).reshape((-1,) + (1,) * (values.ndim - 1 - dim))

    one_side = jax.random.permutation(own_key, parts)[block_of(target)]
    far = (block_of(target) + parts // 2) % parts
    return jnp.where((block_of(source) == one_side) | (block_of(source) == far), factor * values, values)


def block_levels(key, extent, cuts, smallest, top_value):
    level = 1.0
    for dim, parts in cuts:
        heights = jax.random.uniform(jax.random.fold_in(jax.random.fold_in(key, 6), dim), (parts,), jnp.float32, smallest / len(cuts), top_value / len(cuts))
        level = level * jnp.repeat(jnp.exp(heights), extent[dim] // parts).reshape((-1,) + (1,) * (len(extent) - 1 - dim))
    return level


def centred(own_key, extent, deviation, most, cuts=(), dtype=jnp.bfloat16):
    array = jax.random.normal(own_key, extent, jnp.float32) * deviation
    if len(cuts) > 0:
        array = block_levels(own_key, extent, cuts, -0.22, 0.18) * array
    return jnp.clip(array, min=-most, max=most).astype(dtype)


def noise_with(rng, extent, deviation, reach, shards, heavy, kind=jnp.bfloat16):
    values = deviation * jax.random.normal(rng, extent, jnp.float32)
    if shards:
        values = values * block_levels(rng, extent, shards, -0.22, 0.18)
    return jnp.clip(strengthened(values, jax.random.fold_in(rng, 3), *heavy), -reach, reach).astype(kind)


def setup_inputs(seed: int = 0) -> dict:
    streams_of = jax.random.split(jax.random.key(seed), 15)
    tokens = draw_tokens(jax.random.fold_in(streams_of[14], 71), 0)
    lru_in = centred(streams_of[1], (D, LRU_W), D ** -0.5, 0.125, ((1, 4),))
    lru_gate_in = centred(streams_of[2], (D, LRU_W), D ** -0.5, 0.125, ((1, 4),))
    query_w = draw_query_w(jax.random.fold_in(streams_of[14], 71), 0)
    key_w = draw_key_w(jax.random.fold_in(streams_of[14], 71), 0)
    value_w = centred(streams_of[5], (D, FOX_W), D ** -0.5, 0.125, ((1, 4),))
    conv_weight = centred(streams_of[6], (CONV_W, LRU_W), CONV_W ** -0.5, 3.0)
    recur_gate_w = centred(streams_of[7], (LRU_BLOCKS, BLOCK_W, BLOCK_W), BLOCK_W ** -0.5, 0.75)
    input_gate_w = centred(streams_of[8], (LRU_BLOCKS, BLOCK_W, BLOCK_W), BLOCK_W ** -0.5, 0.75)
    rate_param = draw_rate_param(jax.random.fold_in(streams_of[14], 71), 0)
    decay_extra = draw_decay_extra(jax.random.fold_in(streams_of[14], 71), 0)
    forget_cum = draw_forget_cum(jax.random.fold_in(streams_of[14], 71), 0)
    out_lru = noise_with(streams_of[12], (LRU_W, D), (LRU_W + FOX_W) ** -0.5, 0.1875, ((0, 4),), (0, 1, 4, 2.0))
    out_fox = noise_with(streams_of[13], (FOX_W, D), (LRU_W + FOX_W) ** -0.5, 0.1875, ((0, 4),), (0, 1, 4, 2.0))
    return {"tokens": tokens, "lru_in": lru_in, "lru_gate_in": lru_gate_in, "query_w": query_w, "key_w": key_w, "value_w": value_w, "conv_weight": conv_weight, "recur_gate_w": recur_gate_w, "input_gate_w": input_gate_w, "rate_param": rate_param, "decay_extra": decay_extra, "forget_cum": forget_cum, "out_lru": out_lru, "out_fox": out_fox}


decay_sharpness = 8.0
epsilon_norm = 1e-06

def combine_pairs(earlier, later):
    decay_one, state_one = earlier
    decay_two, state_two = later
    return (decay_one * decay_two, decay_two * state_one + state_two)

def reference(tokens, lru_in, lru_gate_in, query_w, key_w, value_w, conv_weight, recur_gate_w, input_gate_w, rate_param, decay_extra, forget_cum, out_lru, out_fox):
    token_f32 = tokens.astype(jnp.float32)
    row_scale = lax.rsqrt(lax.optimization_barrier(jnp.mean(token_f32 * token_f32, axis=1, keepdims=True)) + epsilon_norm)

    def project(weight):
        return (jnp.dot(tokens, weight, preferred_element_type=jnp.float32) * row_scale).astype(jnp.bfloat16)
    lru_input = project(lru_in)
    gate_input = project(lru_gate_in)
    queries = project(query_w)
    keys_all = project(key_w)
    values_all = project(value_w)
    padded = jnp.pad(lru_input, ((CONV_W - 1, 0), (0, 0)))
    conv_sum = jnp.zeros((SEQUENCE_TOKENS, LRU_W), jnp.float32)
    for tap_idx in range(CONV_W):
        conv_sum = conv_sum + conv_weight[tap_idx].astype(jnp.float32)[None, :] * padded[tap_idx:tap_idx + SEQUENCE_TOKENS].astype(jnp.float32)
    conv_out = conv_sum.astype(jnp.bfloat16)
    blocked = conv_out.astype(jnp.float32).reshape(SEQUENCE_TOKENS, LRU_BLOCKS, BLOCK_W)
    recur_gate = jax.nn.sigmoid(jnp.einsum('tnc,ncd->tnd', blocked, recur_gate_w.astype(jnp.float32)).reshape(SEQUENCE_TOKENS, LRU_W))
    input_gate = jax.nn.sigmoid(jnp.einsum('tnc,ncd->tnd', blocked, input_gate_w.astype(jnp.float32)).reshape(SEQUENCE_TOKENS, LRU_W))
    log_decay = -decay_sharpness * jax.nn.softplus(-rate_param)[None, :] * recur_gate + decay_extra
    driven = jnp.sqrt(-jnp.expm1(2.0 * log_decay)) * input_gate * conv_out.astype(jnp.float32)
    unused_decay, states = lax.associative_scan(combine_pairs, (jnp.exp(log_decay), driven), axis=0)
    lru_out = (states * jax.nn.gelu(gate_input.astype(jnp.float32))).astype(jnp.bfloat16)
    block_len = math.gcd(SEQUENCE_TOKENS, 512)
    block_count = SEQUENCE_TOKENS // block_len
    positions = jnp.arange(SEQUENCE_TOKENS).astype(jnp.int32)
    score_scale = HEAD_DIM ** (-0.5)
    heads_q = queries.reshape(SEQUENCE_TOKENS, FOX_HEADS, HEAD_DIM).transpose(1, 0, 2)
    heads_k = keys_all.reshape(SEQUENCE_TOKENS, FOX_HEADS, HEAD_DIM).transpose(1, 0, 2)
    heads_v = values_all.reshape(SEQUENCE_TOKENS, FOX_HEADS, HEAD_DIM).transpose(1, 0, 2)
    heads_c = forget_cum.T

    def one_head(entries):
        head_q, head_k, head_v, head_c = entries
        query_blocks = head_q.reshape(block_count, block_len, HEAD_DIM)
        cum_blocks = head_c.reshape(block_count, block_len)
        pos_blocks = positions.reshape(block_count, block_len)

        def one_block(block_entries):
            block_q, block_c, block_pos = block_entries
            scores = jnp.dot(block_q, head_k.T, preferred_element_type=jnp.float32) * score_scale
            scores = scores + block_c[:, None] - head_c[None, :]
            causal = block_pos[:, None] >= positions[None, :]
            scores = jnp.where(causal, scores, -jnp.inf)
            maxima = lax.optimization_barrier(jnp.max(scores, axis=1, keepdims=True))
            probs = jnp.where(causal, jnp.exp(scores - maxima), 0.0)
            totals = lax.optimization_barrier(jnp.sum(probs, axis=1, keepdims=True))
            weighted = jnp.dot(probs.astype(jnp.bfloat16), head_v, preferred_element_type=jnp.float32)
            return (weighted / totals).astype(jnp.bfloat16)
        return lax.map(one_block, (query_blocks, cum_blocks, pos_blocks)).reshape(SEQUENCE_TOKENS, HEAD_DIM)
    fox_heads = lax.map(one_head, (heads_q, heads_k, heads_v, heads_c))
    fox_out = fox_heads.transpose(1, 0, 2).reshape(SEQUENCE_TOKENS, FOX_W)
    mixed_out = jnp.dot(lru_out, out_lru, preferred_element_type=jnp.float32) + jnp.dot(fox_out, out_fox, preferred_element_type=jnp.float32)
    return mixed_out.astype(jnp.bfloat16)
```

```python
import functools

import jax
import jax.numpy as jnp
from jax import lax
from jax.experimental import pallas as pl
from jax.experimental.pallas import tpu as pltpu
from jax.sharding import PartitionSpec as P

HEAD_DIM = 128
decay_sharpness = 8.0
epsilon_norm = 1e-06
MESH = pl.DeviceIdType.MESH
F32 = jnp.float32
BF16 = jnp.bfloat16


def one_minus_exp(w):
    u = -w
    series = 1.0 - u / 9.0
    for n in range(8, 1, -1):
        series = 1.0 - u / n * series
    return jnp.where(u < 0.5, u * series, 1.0 - jnp.exp(w))


def remote(src, dst, send_sem, recv_sem, device):
    return pltpu.make_async_remote_copy(
        src_ref=src,
        dst_ref=dst,
        send_sem=send_sem,
        recv_sem=recv_sem,
        device_id=device,
        device_id_type=MESH,
    )


def kernel(
    SP,
    TP,
    X,
    tokens,
    lru_in,
    gate_in,
    query_w,
    key_w,
    value_w,
    conv_w,
    rg_w,
    ig_w,
    rate,
    decay_extra,
    forget,
    out_lru,
    out_fox,
    out,
    tok_buf,
    w_buf,
    acc,
    sq,
    lru_ref,
    halo,
    pad,
    bd_r,
    bd_i,
    gate_ref,
    q_ref,
    decay_buf,
    prefix_ref,
    local_ref,
    ends,
    incoming,
    kv_buf,
    cum_buf,
    cum_pad,
    wide,
    fcol,
    m_ref,
    l_ref,
    o_ref,
    q_far,
    m_far,
    l_far,
    o_far,
    part_out,
    stat_out,
    part_in,
    stat_in,
    wl_buf,
    wf_buf,
    br_lru,
    br_fox,
    oacc,
    load_sem,
    tsend,
    tfwd,
    trecv,
    hsend,
    hrecv,
    esend,
    erecv,
    zsend,
    xsend,
    kvrecv,
    wsend,
    wrecv,
    lsend,
    lrecv,
    fsend,
    ffwd,
    frecv,
    lfwd,
    qsend,
    qrecv,
    osend,
    orecv,
):
    rows, dcols = tokens.shape
    D, lw = lru_in.shape
    fw = query_w.shape[1]
    H = fw // HEAD_DIM
    oc = out.shape[1]
    Y = TP // 2
    Z = SP // X
    CH = tsend.shape[1]
    rc = rows // CH
    sp = lax.axis_index("sp")
    tp = lax.axis_index("tp")
    z = lax.div(sp, X)
    x = lax.rem(sp, X)
    partner = tp + 1 - 2 * lax.rem(tp, 2)
    far = [lax.rem(tp + 2 * k, TP) for k in range(Y)]
    pfar = [lax.rem(partner + 2 * k, TP) for k in range(Y)]
    offs = [0, lw, lw + fw, lw + 2 * fw, 2 * lw + 2 * fw, 2 * lw + 3 * fw]

    barrier = pltpu.get_barrier_semaphore()
    for k in range(1, SP):
        pl.semaphore_signal(
            barrier, inc=1, device_id={"sp": lax.rem(sp + k, SP)}, device_id_type=MESH
        )
    for k in range(1, TP):
        pl.semaphore_signal(
            barrier, inc=1, device_id={"tp": lax.rem(tp + k, TP)}, device_id_type=MESH
        )
    loads = []
    for i, w in enumerate((lru_in, key_w, value_w, gate_in, query_w)):
        c = pltpu.make_async_copy(w, w_buf.at[:, offs[i] : offs[i + 1]], load_sem.at[i])
        c.start()
        loads.append(c)
    mine = pl.ds(pl.multiple_of(tp * oc, 128), oc)
    own_loads = [
        pltpu.make_async_copy(decay_extra, decay_buf, load_sem.at[5]),
        pltpu.make_async_copy(out_lru.at[:, mine], wl_buf.at[tp], load_sem.at[6]),
        pltpu.make_async_copy(out_fox.at[:, mine], wf_buf.at[tp], load_sem.at[7]),
    ]
    for c in own_loads:
        c.start()
    pl.semaphore_wait(barrier, SP - 1 + TP - 1)

    pending = []

    def chunk(c):
        return pl.ds(c * rc, rc)

    for c in range(CH):
        for k in range(1, Y):
            s = remote(
                tokens.at[chunk(c)],
                tok_buf.at[tp, chunk(c)],
                tsend.at[k, c],
                trecv.at[tp, c],
                {"tp": far[k]},
            )
            s.start()
            pending.append(s)
    for c in range(CH):
        s = remote(
            tokens.at[chunk(c)],
            tok_buf.at[tp, chunk(c)],
            tsend.at[0, c],
            trecv.at[tp, c],
            {"tp": partner},
        )
        s.start()
        pending.append(s)

    bw = rg_w.shape[1]
    nb = lw // bw
    bd_r[...] = jnp.zeros_like(bd_r)
    bd_i[...] = jnp.zeros_like(bd_i)
    for n in range(nb):
        sl = pl.ds(n * bw, bw)
        bd_r[sl, sl] = rg_w[tp * nb + n]
        bd_i[sl, sl] = ig_w[tp * nb + n]
    cum_pad[...] = jnp.zeros_like(cum_pad)
    wide[...] = jnp.zeros_like(wide)
    wide[0:H, :] = forget[...]
    fcol[...] = wide[...].T
    cum_buf[sp] = wide[0:8, :]

    for c in loads:
        c.wait()

    def project(val, src, r, first=False):
        w_rows = pl.ds(pl.multiple_of(src * dcols, dcols), dcols)
        v32 = val.astype(F32)
        part = jnp.sum(v32 * v32, axis=1, keepdims=True)
        dot = jnp.dot(val, w_buf[w_rows, :], preferred_element_type=F32)
        if first:
            sq[r, :] = part
            acc[r, :] = dot
        else:
            sq[r, :] += part
            acc[r, :] += dot

    def tok_wait(src, c):
        ref = tok_buf.at[src, chunk(c)]
        remote(ref, ref, tsend.at[0, c], trecv.at[src, c], {"tp": partner}).wait_recv()

    for c in range(CH):
        project(tokens[chunk(c), :], tp, chunk(c), True)
    for c in range(CH):
        tok_wait(partner, c)
        project(tok_buf[partner, chunk(c), :], partner, chunk(c))
    for c in range(CH):
        for k in range(1, Y):
            tok_wait(far[k], c)
            ref = tok_buf.at[far[k], chunk(c)]
            s = remote(ref, ref, tfwd.at[k, c], trecv.at[far[k], c], {"tp": partner})
            s.start()
            pending.append(s)
            project(tok_buf[far[k], chunk(c), :], far[k], chunk(c))
        for k in range(1, Y):
            tok_wait(pfar[k], c)
            project(tok_buf[pfar[k], chunk(c), :], pfar[k], chunk(c))

    row_scale = lax.rsqrt(sq[...] / D + epsilon_norm)

    def scaled(i, n=1):
        return (acc[:, offs[i] : offs[i + n]] * row_scale).astype(BF16)

    lru_ref[...] = scaled(0)
    hb = halo.shape[0]
    halo_copy = remote(
        lru_ref.at[pl.ds(rows - hb, hb)],
        halo,
        hsend.at[0],
        hrecv.at[0],
        {"sp": lax.rem(sp + 1, SP)},
    )

    @pl.when(sp < SP - 1)
    def _():
        halo_copy.start()

    kv_buf[sp] = scaled(1, 2)

    paired = Z in (3, 4)
    helper = jnp.logical_and(z <= Z - 3, paired)
    helped = jnp.logical_and(z >= 2, paired)

    def block_copies(j, a, send_sem, device):
        return (
            remote(kv_buf.at[j], kv_buf.at[j], send_sem.at[a, 0], kvrecv.at[j, 0], device),
            remote(cum_buf.at[j], cum_buf.at[j], send_sem.at[a, 1], kvrecv.at[j, 1], device),
        )

    def z_copies(dz):
        j = (z - dz) * X + x
        return block_copies(j, dz, zsend, {"sp": lax.rem(sp + X, SP)})

    def x_copies(dz, dx):
        j = (z - dz) * X + x
        xo = lax.rem(x + dx, X)
        return block_copies(j, dz, xsend.at[dx - 1], {"sp": z * X + xo})

    def for_sends(dz, own, act):
        if own or not paired:

            @pl.when(z < Z - 1)
            def _():
                for c in z_copies(dz):
                    act(c)

        for dx in range(1, X):
            if own:

                @pl.when(jnp.logical_or(lax.rem(x + dx, X) > x, helper))
                def _():
                    for c in x_copies(dz, dx):
                        act(c)
            else:
                for c in x_copies(dz, dx):
                    act(c)

    def kv_wait(j):
        for c in block_copies(j, 0, zsend, {"sp": lax.rem(sp + X, SP)}):
            c.wait_recv()

    for_sends(0, True, lambda c: c.start())

    q_ref[...] = scaled(4)
    q_copy = remote(
        q_ref, q_far, qsend.at[0], qrecv.at[0], {"sp": lax.rem(sp + SP - 2 * X, SP)}
    )

    @pl.when(helped)
    def _():
        q_copy.start()

    for i, (w, buf) in enumerate(((out_lru, wl_buf), (out_fox, wf_buf))):
        for k in range(1, TP):
            t = lax.rem(tp + k, TP)
            cols = pl.ds(pl.multiple_of(t * oc, 128), oc)
            s = remote(w.at[:, cols], buf.at[tp], wsend.at[i, k], wrecv.at[i, tp], {"tp": t})
            s.start()
            pending.append(s)

    gate_ref[...] = scaled(3)

    @pl.when(sp == 0)
    def _():
        pad[0:8, :] = jnp.zeros((8, lw), F32)

    @pl.when(sp > 0)
    def _():
        halo_copy.wait_recv()
        pad[0:8, :] = halo[...].astype(F32)[hb - 8 : hb, :]

    pad[8 : 8 + rows, :] = lru_ref[...].astype(F32)
    chans = pl.ds(pl.multiple_of(tp * lw, 128), lw)
    taps = conv_w.shape[0]
    taps_f32 = conv_w[:, chans].astype(F32)
    conv = jnp.zeros((rows, lw), F32)
    for j in range(taps):
        conv = conv + taps_f32[j : j + 1, :] * pad[8 - (taps - 1) + j : 8 - (taps - 1) + j + rows, :]
    conv_b = conv.astype(BF16)

    def sigmoid(v):
        return 1.0 / (1.0 + jnp.exp(-v))

    recur_gate = sigmoid(jnp.dot(conv_b, bd_r[...], preferred_element_type=F32))
    input_gate = sigmoid(jnp.dot(conv_b, bd_i[...], preferred_element_type=F32))
    own_rate = rate[:, chans]
    softplus = jnp.maximum(-own_rate, 0.0) + jnp.log1p(jnp.exp(-jnp.abs(own_rate)))
    for c in own_loads:
        c.wait()
    log_decay = -decay_sharpness * softplus * recur_gate + decay_buf[...]
    prefix_ref[...] = jnp.exp(log_decay)
    local_ref[...] = jnp.sqrt(one_minus_exp(2.0 * log_decay)) * input_gate * conv_b.astype(F32)
    row_id = lax.broadcasted_iota(jnp.int32, (rows, lw), 0)
    step = 1
    while step < rows:
        a = prefix_ref[...]
        b = local_ref[...]
        keep = row_id >= step
        a_prev = jnp.where(keep, pltpu.roll(a, step, 0), 1.0)
        b_prev = jnp.where(keep, pltpu.roll(b, step, 0), 0.0)
        local_ref[...] = b + a * b_prev
        prefix_ref[...] = a * a_prev
        step *= 2
    ends[sp, 0:1, :] = prefix_ref[rows - 1 : rows, :]
    ends[sp, 1:2, :] = local_ref[rows - 1 : rows, :]

    def end_copy(k):
        return remote(
            ends.at[sp], ends.at[sp], esend.at[k], erecv.at[sp], {"sp": lax.rem(sp + k, SP)}
        )

    for k in range(1, SP):

        @pl.when(sp + k < SP)
        def _():
            end_copy(k).start()

    score_scale = HEAD_DIM ** (-0.5)
    qc = rows // 2

    def attend(j, diagonal, far_first=None):
        other = far_first is not None
        first = diagonal or far_first
        qs, ms, ls, os = (q_far, m_far, l_far, o_far) if other else (q_ref, m_ref, l_ref, o_ref)

        def some(i, carry):
            r = pl.ds(pl.multiple_of(i * qc, qc), qc)
            for h in range(H):
                hs = slice(h * HEAD_DIM, (h + 1) * HEAD_DIM)
                vs = slice(fw + h * HEAD_DIM, fw + (h + 1) * HEAD_DIM)
                s = lax.dot_general(
                    qs[r, hs],
                    kv_buf[j, :, hs],
                    (((1,), (1,)), ((), ())),
                    preferred_element_type=F32,
                )
                s = s * score_scale
                if not other:
                    s = s + fcol[r, h : h + 1]
                s = s - cum_buf[j, h : h + 1, :]
                if diagonal:
                    causal = (
                        lax.broadcasted_iota(jnp.int32, (qc, rows), 0) + i * qc
                        >= lax.broadcasted_iota(jnp.int32, (qc, rows), 1)
                    )
                    s = jnp.where(causal, s, -1e30)
                top = jnp.max(s, axis=1, keepdims=True)
                if first:
                    p = jnp.exp(s - top)
                    ms[h, r, :] = top
                    ls[h, r, :] = jnp.sum(p, axis=1, keepdims=True)
                    os[h, r, :] = jnp.dot(
                        p.astype(BF16), kv_buf[j, :, vs], preferred_element_type=F32
                    )
                else:
                    old = ms[h, r, :]
                    new = jnp.maximum(old, top)
                    p = jnp.exp(s - new)
                    fade = jnp.exp(old - new)
                    ms[h, r, :] = new
                    ls[h, r, :] = ls[h, r, :] * fade + jnp.sum(p, axis=1, keepdims=True)
                    os[h, r, :] = os[h, r, :] * fade + jnp.dot(
                        p.astype(BF16), kv_buf[j, :, vs], preferred_element_type=F32
                    )
            return carry

        lax.fori_loop(0, rows // qc, some, 0)

    attend(sp, True)

    def row_blocks(dz):
        for dx in range(1, X):
            xo = lax.rem(x + dx, X)

            @pl.when(jnp.logical_or(dz > 0, xo < x))
            def _():
                j = (z - dz) * X + xo
                kv_wait(j)
                attend(j, False)

    def finish_lru():
        incoming[...] = jnp.zeros_like(incoming)
        for j in range(SP - 1):

            @pl.when(j < sp)
            def _():
                remote(
                    ends.at[j], ends.at[j], esend.at[0], erecv.at[j], {"sp": lax.rem(sp + 1, SP)}
                ).wait_recv()
                incoming[...] = ends[j, 0:1, :] * incoming[...] + ends[j, 1:2, :]

        states = local_ref[...] + prefix_ref[...] * incoming[...]
        g = gate_ref[...].astype(F32)
        gelu = 0.5 * g * (1.0 + jnp.tanh(0.7978845608028654 * (g + 0.044715 * (g * g * g))))
        br_lru[tp] = (states * gelu).astype(BF16)
        for k in range(Y - 1, -1, -1):
            lru_copy(k).start()

    def lru_copy(k):
        to = far[k] if k else partner
        return remote(br_lru.at[tp], br_lru.at[tp], lsend.at[k], lrecv.at[tp], {"tp": to})

    lru_step = min(2, Z - 1)
    if Z == 1:
        finish_lru()

    def hop(dz, carry):
        @pl.when(dz <= z)
        def _():
            j = (z - dz) * X + x
            kv_wait(j)
            for_sends(dz, False, lambda c: c.start())
            row_blocks(dz - 1)
            attend(j, False)

        @pl.when(dz == lru_step)
        def _():
            finish_lru()

        return carry

    up = {"sp": lax.rem(sp + 2 * X, SP)}
    part_copies = (
        remote(part_out, part_in, osend.at[0], orecv.at[0], up),
        remote(stat_out, stat_in, osend.at[1], orecv.at[1], up),
    )

    def send_partial():
        for h in range(H):
            part_out[:, h * HEAD_DIM : (h + 1) * HEAD_DIM] = o_far[h].astype(BF16)
            cum_pad[:, h : h + 1] = m_far[h]
            cum_pad[:, H + h : H + h + 1] = l_far[h]
        stat_out[...] = cum_pad[...].T[0:8, :]
        for c in part_copies:
            c.start()

    if paired:
        below = (z - 1) * X

        @pl.when(helper)
        def _():
            q_copy.wait_recv()
            attend(sp, False, True)

        @pl.when(z >= 1)
        def _():
            kv_wait(below + x)
            for_sends(1, False, lambda c: c.start())

        for dx in range(1, X):
            xo = lax.rem(x + dx, X)

            @pl.when(jnp.logical_or(xo < x, helper))
            def _():
                kv_wait(z * X + xo)

            @pl.when(helper)
            def _():
                attend(z * X + xo, False, False)

        @pl.when(jnp.logical_and(helper, z == 0))
        def _():
            send_partial()

        for dx in range(1, X):
            xo = lax.rem(x + dx, X)

            @pl.when(xo < x)
            def _():
                attend(z * X + xo, False)

        finish_lru()

        @pl.when(jnp.logical_and(helper, z >= 1))
        def _():
            attend(below + x, False, False)

        @pl.when(z >= 1)
        def _():
            attend(below + x, False)
            for dx in range(1, X):
                j = below + lax.rem(x + dx, X)
                kv_wait(j)

                @pl.when(helper)
                def _():
                    attend(j, False, False)

            @pl.when(helper)
            def _():
                send_partial()

            for dx in range(1, X):
                attend(below + lax.rem(x + dx, X), False)

    else:
        lax.fori_loop(1, Z, hop, 0)

    def lru_wait(t):
        remote(br_lru.at[t], br_lru.at[t], lsend.at[0], lrecv.at[t], {"tp": partner}).wait_recv()

    def lru_dot(t):
        return jnp.dot(br_lru[t], wl_buf[t], preferred_element_type=F32)

    oacc[...] = lru_dot(tp)
    for k in range(1, TP):
        t = lax.rem(tp + k, TP)
        for i, buf in enumerate((wl_buf, wf_buf)):
            remote(buf.at[t], buf.at[t], wsend.at[i, k], wrecv.at[i, t], {"tp": t}).wait_recv()
    for k in range(1, Y):
        lru_wait(far[k])
        ref = br_lru.at[far[k]]
        s = remote(ref, ref, lfwd.at[k], lrecv.at[far[k]], {"tp": partner})
        s.start()
        pending.append(s)
    lru_wait(partner)
    oacc[...] += lru_dot(partner)
    for k in range(1, Y):
        oacc[...] += lru_dot(far[k])
        lru_wait(pfar[k])
        oacc[...] += lru_dot(pfar[k])

    if paired:

        @pl.when(helped)
        def _():
            for c in part_copies:
                c.wait_recv()
            wide[0:8, :] = stat_in[...]
            stats = wide[...].T
            for h in range(H):
                m_in = stats[:, h : h + 1] + fcol[:, h : h + 1]
                l_in = stats[:, H + h : H + h + 1]
                part = part_in[:, h * HEAD_DIM : (h + 1) * HEAD_DIM].astype(F32)
                new = jnp.maximum(m_ref[h], m_in)
                fade = jnp.exp(m_ref[h] - new)
                grow = jnp.exp(m_in - new)
                l_ref[h] = l_ref[h] * fade + l_in * grow
                o_ref[h] = o_ref[h] * fade + part * grow

    else:
        row_blocks(z)

    for c in range(CH):
        r = chunk(c)
        for h in range(H):
            br_fox[tp, r, h * HEAD_DIM : (h + 1) * HEAD_DIM] = (
                o_ref[h, r, :] / l_ref[h, r, :]
            ).astype(BF16)
        ref = br_fox.at[tp, r]
        for k in list(range(1, Y)) + [0]:
            to = far[k] if k else partner
            s = remote(ref, ref, fsend.at[k, c], frecv.at[tp, c], {"tp": to})
            s.start()
            pending.append(s)

    def fox_wait(src, c):
        ref = br_fox.at[src, chunk(c)]
        remote(ref, ref, fsend.at[0, c], frecv.at[src, c], {"tp": partner}).wait_recv()

    def fox_dot(src, r):
        return jnp.dot(br_fox[src, r, :], wf_buf[src], preferred_element_type=F32)

    for c in range(CH):
        fox_wait(partner, c)
        oacc[chunk(c), :] += fox_dot(tp, chunk(c)) + fox_dot(partner, chunk(c))
    for c in range(CH):
        r = chunk(c)
        for k in range(1, Y):
            fox_wait(far[k], c)
            ref = br_fox.at[far[k], r]
            s = remote(ref, ref, ffwd.at[k, c], frecv.at[far[k], c], {"tp": partner})
            s.start()
            pending.append(s)
            oacc[r, :] += fox_dot(far[k], r)
        for k in range(1, Y):
            fox_wait(pfar[k], c)
            oacc[r, :] += fox_dot(pfar[k], r)
        out[r, :] = oacc[r, :].astype(out.dtype)

    for s in pending:
        s.wait_send()
    for k in range(Y):
        lru_copy(k).wait_send()

    @pl.when(helped)
    def _():
        q_copy.wait_send()

    @pl.when(helper)
    def _():
        for c in part_copies:
            c.wait_send()

    @pl.when(sp < SP - 1)
    def _():
        halo_copy.wait_send()

    for k in range(1, SP):

        @pl.when(sp + k < SP)
        def _():
            end_copy(k).wait_send()

    for_sends(0, True, lambda c: c.wait_send())

    def drain(dz, carry):
        @pl.when(dz <= z)
        def _():
            for_sends(dz, False, lambda c: c.wait_send())

        return carry

    if paired:

        @pl.when(z >= 1)
        def _():
            for_sends(1, False, lambda c: c.wait_send())

    else:
        lax.fori_loop(1, Z, drain, 0)


def shards(SP, TP, X, *args):
    tokens, lru_in, gate_in, query_w = args[:4]
    (conv_weight, rg_w, ig_w, rate, decay_extra, forget, out_lru, out_fox) = args[6:]
    rows, dcols = tokens.shape
    D, lw = lru_in.shape
    fw = query_w.shape[1]
    oc = out_lru.shape[1] // TP
    tot = 2 * lw + 3 * fw
    H = fw // HEAD_DIM
    Y = TP // 2
    Z = SP // X
    CH = 4
    vm = pl.BlockSpec(memory_space=pltpu.VMEM)
    hbm = pl.BlockSpec(memory_space=pl.ANY)
    dma = pltpu.SemaphoreType.DMA
    V = pltpu.VMEM
    scratch = [
        V((TP, rows, dcols), BF16),
        V((D, tot), BF16),
        V((rows, tot), F32),
        V((rows, 1), F32),
        V((rows, lw), BF16),
        V((16, lw), BF16),
        V((rows + 8, lw), F32),
        V((lw, lw), BF16),
        V((lw, lw), BF16),
        V((rows, lw), BF16),
        V((rows, fw), BF16),
        V((rows, lw), F32),
        V((rows, lw), F32),
        V((rows, lw), F32),
        V((SP, 8, lw), F32),
        V((1, lw), F32),
        V((SP, rows, 2 * fw), BF16),
        V((SP, 8, rows), F32),
        V((rows, 128), F32),
        V((128, rows), F32),
        V((rows, 128), F32),
        V((H, rows, 1), F32),
        V((H, rows, 1), F32),
        V((H, rows, HEAD_DIM), F32),
        V((rows, fw), BF16),
        V((H, rows, 1), F32),
        V((H, rows, 1), F32),
        V((H, rows, HEAD_DIM), F32),
        V((rows, fw), BF16),
        V((8, rows), F32),
        V((rows, fw), BF16),
        V((8, rows), F32),
        V((TP, lw, oc), BF16),
        V((TP, fw, oc), BF16),
        V((TP, rows, lw), BF16),
        V((TP, rows, fw), BF16),
        V((rows, oc), F32),
        dma((8,)),
        dma((Y, CH)),
        dma((Y, CH)),
        dma((TP, CH)),
        dma((1,)),
        dma((1,)),
        dma((SP,)),
        dma((SP,)),
        dma((Z, 2)),
        dma((max(X - 1, 1), Z, 2)),
        dma((SP, 2)),
        dma((2, TP)),
        dma((2, TP)),
        dma((TP,)),
        dma((TP,)),
        dma((Y, CH)),
        dma((Y, CH)),
        dma((TP, CH)),
        dma((Y,)),
        dma((1,)),
        dma((1,)),
        dma((2,)),
        dma((2,)),
    ]
    return pl.pallas_call(
        functools.partial(kernel, SP, TP, X),
        out_shape=jax.ShapeDtypeStruct((rows, oc), BF16),
        in_specs=[vm] + [hbm] * 5 + [vm] * 4 + [hbm, vm, hbm, hbm],
        out_specs=vm,
        scratch_shapes=scratch,
        compiler_params=pltpu.CompilerParams(
            collective_id=0, has_side_effects=True, vmem_limit_bytes=60 * 1024 * 1024
        ),
    )(*args[:9], rate.reshape(1, -1), decay_extra, forget.T, out_lru, out_fox)


LOG2E = 1.4426950408889634


def block_kernel(
    SP,
    TP,
    X,
    CH,
    tokens,
    lru_in,
    gate_in,
    query_w,
    key_w,
    value_w,
    conv_w,
    rg_w,
    ig_w,
    rate,
    decay_extra,
    forget,
    out_lru,
    out_fox,
    out,
    tok_buf,
    w_buf,
    acc,
    sq,
    lru_ref,
    halo,
    pad,
    conv_v,
    rg_v,
    ig_v,
    rate_v,
    forget_v,
    bd_r,
    bd_i,
    gate_ref,
    q_ref,
    decay_buf,
    prefix_ref,
    local_ref,
    seg_a,
    seg_b,
    carry_ref,
    ends,
    kv_buf,
    cum_buf,
    m_ref,
    o_ref,
    q_far,
    m_far,
    o_far,
    part_out,
    stat_out,
    part_in,
    stat_in,
    wl_buf,
    wf_buf,
    br_lru,
    br_fox,
    oacc,
    obuf,
    load_sem,
    out_sem,
    tsend,
    tfwd,
    trecv,
    hsend,
    hrecv,
    esend,
    erecv,
    csend,
    crecv,
    zsend,
    xsend,
    zfwd,
    xfwd,
    kvrecv,
    wsend,
    wfwd,
    wrecv,
    lsend,
    lrecv,
    fsend,
    ffwd,
    frecv,
    lfwd,
    qsend,
    qrecv,
    osend,
    orecv,
):
    rows, dcols = tokens.shape
    D, lw = lru_in.shape
    fw = query_w.shape[1]
    H = fw // HEAD_DIM
    oc = out.shape[1]
    Z = SP // X
    rc = rows // CH
    half = rows // 2
    wh = out_lru.shape[0] // X
    sp = lax.axis_index("sp")
    tp = lax.axis_index("tp")
    z = lax.div(sp, X)
    x = lax.rem(sp, X)
    xo = 1 - x
    y = lax.div(tp, 2)
    partner = tp + 1 - 2 * lax.rem(tp, 2)
    far = lax.rem(tp + 2, TP)
    pfar = lax.rem(partner + 2, TP)
    j_xo = z * X + xo
    to_xo = {"sp": j_xo}
    to_up = {"sp": lax.rem(sp + X, SP)}
    j_b = lax.rem(sp + SP - X, SP)
    j_bo = lax.rem(j_xo + SP - X, SP)
    helper = z <= Z - 3
    helped = z >= 2
    not_top = z < Z - 1
    above0 = z >= 1
    order = list(range(CH - 1, -1, -1))
    via_z = order[0::2]
    via_x = order[1::2]
    score_k = HEAD_DIM ** (-0.5) * LOG2E

    def chunk(c):
        return pl.ds(c * rc, rc)

    barrier = pltpu.get_barrier_semaphore()
    for k in range(1, SP):
        pl.semaphore_signal(
            barrier, inc=1, device_id={"sp": lax.rem(sp + k, SP)}, device_id_type=MESH
        )
    for k in range(1, TP):
        pl.semaphore_signal(
            barrier, inc=1, device_id={"tp": lax.rem(tp + k, TP)}, device_id_type=MESH
        )

    def load(i, src, dst):
        c = pltpu.make_async_copy(src, dst, load_sem.at[i])
        c.start()
        return c

    tok_load = load(0, tokens, tok_buf.at[tp])
    cols = (0, fw, 2 * fw, 2 * fw + lw, 3 * fw + lw, 3 * fw + 2 * lw)
    w_loads = [
        load(1 + i, w, w_buf.at[:, cols[i] : cols[i + 1]])
        for i, w in enumerate((key_w, value_w, lru_in, query_w, gate_in))
    ]
    mine = pl.ds(pl.multiple_of(tp * oc, 128), oc)
    bw = rg_w.shape[1]
    nb = lw // bw
    gates = pl.ds(tp * nb, nb)
    forget_load = load(6, forget, forget_v)
    small_loads = [
        load(7, conv_w, conv_v),
        load(8, rg_w.at[gates], rg_v),
        load(9, ig_w.at[gates], ig_v),
        load(10, rate, rate_v),
        load(11, decay_extra, decay_buf),
    ]
    own_loads = [
        load(12, out_lru.at[:, mine], wl_buf.at[tp]),
        load(13, out_fox.at[:, mine], wf_buf.at[tp]),
    ]
    tok_load.wait()
    pl.semaphore_wait(barrier, SP - 1 + TP - 1)

    pending = []

    def send(src, dst, send_sem, recv_sem, device):
        s = remote(src, dst, send_sem, recv_sem, device)
        s.start()
        pending.append(s)

    for c in order:
        ref = tok_buf.at[tp, chunk(c)]
        send(ref, ref, tsend.at[1, c], trecv.at[tp, c], {"tp": far})
        send(ref, ref, tsend.at[0, c], trecv.at[tp, c], {"tp": partner})

    forget_load.wait()
    cum_buf[sp] = jnp.zeros_like(cum_buf[sp])
    cum_buf[sp, 0:H, :] = forget_v[...] * LOG2E
    own_cum = cum_buf.at[sp]
    send(own_cum, own_cum, csend.at[0], crecv.at[sp], to_xo)
    cum_up = (
        remote(own_cum, own_cum, csend.at[1], crecv.at[sp], to_up),
        remote(own_cum, own_cum, csend.at[2], crecv.at[sp], {"sp": lax.rem(j_xo + X, SP)}),
    )

    @pl.when(not_top)
    def _():
        for c in cum_up:
            c.start()

    for c in small_loads:
        c.wait()
    bd_r[...] = jnp.zeros_like(bd_r)
    bd_i[...] = jnp.zeros_like(bd_i)
    for n in range(nb):
        sl = pl.ds(n * bw, bw)
        bd_r[sl, sl] = rg_v[n]
        bd_i[sl, sl] = ig_v[n]
    for c in w_loads:
        c.wait()

    def tok_wait(src, c):
        ref = tok_buf.at[src, chunk(c)]
        remote(ref, ref, tsend.at[0, c], trecv.at[src, c], {"tp": partner}).wait_recv()

    def features(side, c):
        first = 2 * side
        return jnp.concatenate([tok_buf[first, chunk(c), :], tok_buf[first + 1, chunk(c), :]], axis=1)

    def w_rows(side):
        return pl.ds(pl.multiple_of(side * 2 * dcols, 2 * dcols), 2 * dcols)

    def squares(v):
        v32 = v.astype(F32)
        return jnp.sum(v32 * v32, axis=1, keepdims=True)

    def near_part(c, slot):
        tok_wait(partner, c)
        v = features(y, c)
        sq[slot] = squares(v)
        acc[slot] = jnp.dot(v, w_buf[w_rows(y), :], preferred_element_type=F32)

    halo_copy = remote(
        lru_ref.at[pl.ds(rows - halo.shape[0], halo.shape[0])],
        halo,
        hsend.at[0],
        hrecv.at[0],
        {"sp": lax.rem(sp + 1, SP)},
    )

    def kv_copy(j, c, send_sem, device):
        ref = kv_buf.at[j, chunk(c)]
        return remote(ref, ref, send_sem.at[c], kvrecv.at[j, c], device)

    def kv_wait(j, c):
        kv_copy(j, c, zsend, to_up).wait_recv()

    def across(c):
        return jnp.logical_or(x == 0, z <= (Z - 2 if c in via_z else Z - 3))

    def from_across(c):
        return jnp.logical_or(x == 1, z <= (Z - 2 if c in via_z else Z - 3))

    def q_copy(c):
        return remote(
            q_ref.at[chunk(c)],
            q_far.at[chunk(c)],
            qsend.at[c],
            qrecv.at[c],
            {"sp": lax.rem(sp + SP - 2 * X, SP)},
        )

    def far_part(i, c, slot):
        tok_wait(far, c)
        ref = tok_buf.at[far, chunk(c)]
        send(ref, ref, tfwd.at[c], trecv.at[far, c], {"tp": partner})
        if i + 1 < CH:
            near_part(order[i + 1], 1 - slot)
        tok_wait(pfar, c)
        v = features(1 - y, c)
        row_scale = lax.rsqrt((sq[slot] + squares(v)) / D + epsilon_norm)

        def part(a, b):
            w = w_buf[w_rows(1 - y), cols[a] : cols[b]]
            both = acc[slot, :, cols[a] : cols[b]] + jnp.dot(v, w, preferred_element_type=F32)
            return (both * row_scale).astype(BF16)

        kv_buf[sp, chunk(c), :] = part(0, 2)

        @pl.when(across(c))
        def _():
            kv_copy(sp, c, xsend, to_xo).start()

        @pl.when(not_top)
        def _():
            kv_copy(sp, c, zsend, to_up).start()

        rest = part(2, 5)
        lru_ref[chunk(c), :] = rest[:, 0:lw]
        q_ref[chunk(c), :] = rest[:, lw : lw + fw]
        gate_ref[chunk(c), :] = rest[:, lw + fw :]

        @pl.when(helped)
        def _():
            q_copy(c).start()

        if i == 0:

            @pl.when(sp < SP - 1)
            def _():
                halo_copy.start()

    def weight_copy(i, w, buf, t, k):
        r = pl.ds(x * wh, wh)
        c = pl.ds(pl.multiple_of(t * oc, 128), oc)
        return remote(w.at[r, c], buf.at[tp, r], wsend.at[i, k], wrecv.at[i, tp, x], {"tp": t})

    near_part(order[0], 0)
    for i, c in enumerate(order):
        far_part(i, c, i % 2)
        if i == CH - 2:
            for n, (w, buf) in enumerate(((out_lru, wl_buf), (out_fox, wf_buf))):
                for k, t in enumerate((far, pfar)):
                    s = weight_copy(n, w, buf, t, k)
                    s.start()
                    pending.append(s)
            for n, (w, buf) in enumerate(((out_lru, wl_buf), (out_fox, wf_buf))):
                c2 = pl.ds(pl.multiple_of(partner * oc, 128), oc)
                for k in range(X):
                    r = pl.ds(k * wh, wh)
                    send(
                        w.at[r, c2],
                        buf.at[tp, r],
                        wsend.at[n, 2 + k],
                        wrecv.at[n, tp, k],
                        {"tp": partner},
                    )

    def weight_pass(n, t):
        buf = (wl_buf, wf_buf)[n]
        ref = buf.at[t, pl.ds(x * wh, wh)]
        remote(ref, ref, wsend.at[n, 0], wrecv.at[n, t, x], {"tp": t}).wait_recv()
        send(ref, ref, wfwd.at[n, 0 if t is far else 1], wrecv.at[n, t, x], to_xo)

    def weight_wait(n, t, k):
        ref = (wl_buf, wf_buf)[n].at[t, pl.ds(k * wh, wh)]
        remote(ref, ref, wsend.at[n, 0], wrecv.at[n, t, k], to_xo).wait_recv()

    def pass_up(c):
        @pl.when(from_across(c))
        def _():
            kv_wait(j_xo, c)

        @pl.when(not_top)
        def _():
            kv_copy(j_xo, c, zfwd, to_up).start()

    def pass_across(c):
        @pl.when(above0)
        def _():
            kv_wait(j_b, c)
            kv_copy(j_b, c, xfwd, to_xo).start()

    pass_up(via_z[0])
    pass_across(via_x[0])

    @pl.when(sp == 0)
    def _():
        pad[0:8, :] = jnp.zeros((8, lw), F32)

    @pl.when(sp > 0)
    def _():
        halo_copy.wait_recv()
        hb = halo.shape[0]
        pad[0:8, :] = halo[...].astype(F32)[hb - 8 : hb, :]

    pad[8 : 8 + rows, :] = lru_ref[...].astype(F32)
    chans = pl.ds(pl.multiple_of(tp * lw, 128), lw)
    taps = conv_w.shape[0]
    taps_f32 = conv_v[:, chans].astype(F32)
    conv = jnp.zeros((rows, lw), F32)
    for j in range(taps):
        conv = conv + taps_f32[j : j + 1, :] * pad[8 - (taps - 1) + j : 8 - (taps - 1) + j + rows, :]
    conv_b = conv.astype(BF16)

    def sigmoid(v):
        return 1.0 / (1.0 + jnp.exp(-v))

    recur_gate = sigmoid(jnp.dot(conv_b, bd_r[...], preferred_element_type=F32))
    input_gate = sigmoid(jnp.dot(conv_b, bd_i[...], preferred_element_type=F32))
    own_rate = rate_v[:, chans]
    softplus = jnp.maximum(-own_rate, 0.0) + jnp.log1p(jnp.exp(-jnp.abs(own_rate)))
    log_decay = -decay_sharpness * softplus * recur_gate + decay_buf[...]
    decay = jnp.exp(log_decay)
    driven = jnp.sqrt(one_minus_exp(2.0 * log_decay)) * input_gate * conv_b.astype(F32)
    for n in range(lw // 128):
        prefix_ref[n] = decay[:, n * 128 : (n + 1) * 128]
        local_ref[n] = driven[:, n * 128 : (n + 1) * 128]

    segs = 8
    seg_len = rows // segs
    run_a = jnp.ones((segs, lw), F32)
    run_b = jnp.zeros((segs, lw), F32)
    for i in range(seg_len):
        at = pl.ds(i, segs, stride=seg_len)
        a = [prefix_ref[n, at, :] for n in range(lw // 128)]
        b = [local_ref[n, at, :] for n in range(lw // 128)]
        a = jnp.concatenate(a, axis=1)
        b = jnp.concatenate(b, axis=1)
        run_a = run_a * a
        run_b = a * run_b + b
        for n in range(lw // 128):
            prefix_ref[n, at, :] = run_a[:, n * 128 : (n + 1) * 128]
            local_ref[n, at, :] = run_b[:, n * 128 : (n + 1) * 128]
    seg_a[...] = run_a
    seg_b[...] = run_b
    end_a = seg_a[0:1, :]
    end_b = seg_b[0:1, :]
    for i in range(1, segs):
        end_b = seg_a[i : i + 1, :] * end_b + seg_b[i : i + 1, :]
        end_a = end_a * seg_a[i : i + 1, :]
    ends[sp, 0:1, :] = end_a
    ends[sp, 1:2, :] = end_b

    def end_copy(k):
        return remote(
            ends.at[sp], ends.at[sp], esend.at[k], erecv.at[sp], {"sp": lax.rem(sp + k, SP)}
        )

    for k in range(1, SP):

        @pl.when(sp + k < SP)
        def _():
            end_copy(k).start()

    for c in via_z[1:]:
        pass_up(c)

    def attend(qs, st, j, lo, hi, first=False, diagonal=False, qc=half, after=None):
        ms, os = st
        items = [(i, h) for i in range(rows // qc) for h in range(H)]

        def width(i):
            return (lo, (i + 1) * qc) if diagonal else (lo, hi)

        def scores(i, h):
            a, b = width(i)
            hs = slice(h * HEAD_DIM, (h + 1) * HEAD_DIM)
            s = lax.dot_general(
                qs[i * qc : (i + 1) * qc, hs],
                kv_buf[j, a:b, hs],
                (((1,), (1,)), ((), ())),
                preferred_element_type=F32,
            )
            s = s * score_k - cum_buf[j, h : h + 1, a:b]
            if diagonal:
                causal = (
                    lax.broadcasted_iota(jnp.int32, (qc, b - a), 0) + (i * qc - a)
                    >= lax.broadcasted_iota(jnp.int32, (qc, b - a), 1)
                )
                s = jnp.where(causal, s, -1e30)
            return s

        def update(i, h, s):
            a, b = width(i)
            r = slice(i * qc, (i + 1) * qc)
            top = jnp.max(s, axis=1, keepdims=True)
            if first:
                new = jnp.broadcast_to(top, (qc, 128))
            else:
                old = ms[h, r, :]
                new = jnp.maximum(old, top)
            ms[h, r, :] = new
            p = jnp.exp2(s - jnp.concatenate([new] * ((b - a) // 128), axis=1)).astype(BF16)
            v = kv_buf[j, a:b, fw + h * HEAD_DIM : fw + (h + 1) * HEAD_DIM]
            v1 = jnp.concatenate([v, jnp.ones((b - a, 128), BF16)], axis=1)
            pv = jnp.dot(p, v1, preferred_element_type=F32)
            if first:
                os[h, r, :] = pv
            else:
                fade = jnp.exp2(old - new)
                os[h, r, :] = os[h, r, :] * jnp.concatenate([fade, fade], axis=1) + pv

        s = scores(*items[0])
        for n, (i, h) in enumerate(items):
            nxt = scores(*items[n + 1]) if n + 1 < len(items) else None
            update(i, h, s)
            s = nxt
            if after is not None and h == H - 1:
                after(i)

    own_st = (m_ref, o_ref)
    far_st = (m_far, o_far)
    up2 = {"sp": lax.rem(sp + 2 * X, SP)}

    def part_copies(c):
        return (
            remote(part_out.at[chunk(c)], part_in.at[chunk(c)], osend.at[c, 0], orecv.at[c, 0], up2),
            remote(stat_out.at[c], stat_in.at[c], osend.at[c, 1], orecv.at[c, 1], up2),
        )

    def send_partial(c):
        r = slice(c * rc, (c + 1) * rc)
        lane = lax.broadcasted_iota(jnp.int32, (rc, 128), 1)
        stats = jnp.zeros((rc, 128), F32)
        for h in range(H):
            part_out[r, h * HEAD_DIM : (h + 1) * HEAD_DIM] = o_far[h, r, 0:HEAD_DIM].astype(BF16)
            stats = jnp.where(lane == h, m_far[h, r, :], stats)
            stats = jnp.where(lane == H + h, o_far[h, r, HEAD_DIM:], stats)
        stat_out[c] = stats.T[0:8, :]
        for s in part_copies(c):
            s.start()

    attend(q_ref, own_st, sp, 0, rows, True, True)

    for c in via_x[1:]:
        pass_across(c)

    remote(own_cum, cum_buf.at[j_xo], csend.at[0], crecv.at[j_xo], to_xo).wait_recv()

    @pl.when(helper)
    def _():
        for c in order:
            q_copy(c).wait_recv()
        attend(q_far, far_st, sp, 0, rows, True)

    for c in via_x:

        @pl.when(from_across(c))
        def _():
            kv_wait(j_xo, c)

    @pl.when(helper)
    def _():
        attend(q_far, far_st, j_xo, 0, rows)

    @pl.when(jnp.logical_and(helper, z == 0))
    def _():
        for c in range(CH):
            send_partial(c)

    weight_pass(0, far)
    weight_pass(0, pfar)

    @pl.when(x == 1)
    def _():
        attend(q_ref, own_st, j_xo, 0, rows)

    @pl.when(above0)
    def _():
        for c in via_z:
            kv_wait(j_b, c)
        for j in (j_b, j_bo):
            ref = cum_buf.at[j]
            remote(ref, ref, csend.at[0], crecv.at[j], to_xo).wait_recv()

        @pl.when(helper)
        def _():
            attend(q_far, far_st, j_b, 0, rows)

        attend(q_ref, own_st, j_b, 0, rows)

    carry_ref[0:1, :] = jnp.zeros((1, lw), F32)
    for j in range(SP - 1):

        @pl.when(j < sp)
        def _():
            remote(
                ends.at[j], ends.at[j], esend.at[0], erecv.at[j], {"sp": lax.rem(sp + 1, SP)}
            ).wait_recv()
            carry_ref[0:1, :] = ends[j, 0:1, :] * carry_ref[0:1, :] + ends[j, 1:2, :]

    carry = carry_ref[0:1, :]
    for i in range(segs):
        r = slice(i * seg_len, (i + 1) * seg_len)
        g = gate_ref[r, :].astype(F32)
        gelu = 0.5 * g * (1.0 + jnp.tanh(0.7978845608028654 * (g + 0.044715 * (g * g * g))))
        for n in range(lw // 128):
            cs = slice(n * 128, (n + 1) * 128)
            states = local_ref[n, r, :] + prefix_ref[n, r, :] * carry[:, cs]
            br_lru[tp, r, cs] = (states * gelu[:, cs]).astype(BF16)
        if i + 1 < segs:
            carry = seg_a[i : i + 1, :] * carry + seg_b[i : i + 1, :]
    own_lru = br_lru.at[tp]
    send(own_lru, own_lru, lsend.at[1], lrecv.at[tp], {"tp": far})
    send(own_lru, own_lru, lsend.at[0], lrecv.at[tp], {"tp": partner})
    weight_pass(1, far)

    @pl.when(above0)
    def _():
        for c in order[0:2]:
            kv_wait(j_bo, c)

        @pl.when(helper)
        def _():
            attend(q_far, far_st, j_bo, half, rows)

        attend(q_ref, own_st, j_bo, half, rows)
        for c in order[2:]:
            kv_wait(j_bo, c)

        @pl.when(helper)
        def _():
            attend(q_far, far_st, j_bo, 0, half, qc=rc, after=send_partial)

        attend(q_ref, own_st, j_bo, 0, half)

    weight_pass(1, pfar)

    def lru_wait(t):
        ref = br_lru.at[t]
        remote(ref, ref, lsend.at[0], lrecv.at[t], {"tp": partner}).wait_recv()

    def pair_dot(br, buf, side, r):
        first = 2 * side
        return jnp.dot(br[first, r, :], buf[first], preferred_element_type=F32) + jnp.dot(
            br[first + 1, r, :], buf[first + 1], preferred_element_type=F32
        )

    for c in own_loads:
        c.wait()
    for k in range(X):
        weight_wait(0, partner, k)
        weight_wait(1, partner, k)
    lru_wait(partner)
    for c in range(CH):
        oacc[chunk(c), :] = pair_dot(br_lru, wl_buf, y, chunk(c))

    for c in range(CH):
        r = slice(c * rc, (c + 1) * rc)

        @pl.when(helped)
        def _():
            for s in part_copies(c):
                s.wait_recv()
            stats = jnp.concatenate([stat_in[c], jnp.zeros((120, rc), F32)], axis=0).T
            for h in range(H):
                hs = slice(h * HEAD_DIM, (h + 1) * HEAD_DIM)
                m_in = stats[:, h : h + 1]
                l_in = stats[:, H + h : H + h + 1]
                part = part_in[r, hs].astype(F32)
                old = m_ref[h, r, :]
                new = jnp.maximum(old, m_in)
                fade = jnp.exp2(old - new)
                grow = jnp.exp2(m_in - new)
                total = o_ref[h, r, HEAD_DIM:] * fade + l_in * grow
                br_fox[tp, r, hs] = (
                    (o_ref[h, r, 0:HEAD_DIM] * fade + part * grow) / total
                ).astype(BF16)

        @pl.when(jnp.logical_not(helped))
        def _():
            for h in range(H):
                hs = slice(h * HEAD_DIM, (h + 1) * HEAD_DIM)
                br_fox[tp, r, hs] = (o_ref[h, r, 0:HEAD_DIM] / o_ref[h, r, HEAD_DIM:]).astype(BF16)

        ref = br_fox.at[tp, chunk(c)]
        send(ref, ref, fsend.at[1, c], frecv.at[tp, c], {"tp": far})
        send(ref, ref, fsend.at[0, c], frecv.at[tp, c], {"tp": partner})

    lru_wait(far)
    ref = br_lru.at[far]
    send(ref, ref, lfwd.at[0], lrecv.at[far], {"tp": partner})
    for t in (far, pfar):
        weight_wait(0, t, xo)
    lru_wait(pfar)
    for c in range(CH):
        oacc[chunk(c), :] += pair_dot(br_lru, wl_buf, 1 - y, chunk(c))
    for t in (far, pfar):
        weight_wait(1, t, xo)

    def fox_wait(src, c):
        ref = br_fox.at[src, chunk(c)]
        remote(ref, ref, fsend.at[0, c], frecv.at[src, c], {"tp": partner}).wait_recv()

    out_copies = []
    for c in range(CH):
        r = chunk(c)
        fox_wait(far, c)
        ref = br_fox.at[far, r]
        send(ref, ref, ffwd.at[c], frecv.at[far, c], {"tp": partner})
        fox_wait(partner, c)
        near = oacc[r, :] + pair_dot(br_fox, wf_buf, y, r)
        fox_wait(pfar, c)
        obuf[r, :] = (near + pair_dot(br_fox, wf_buf, 1 - y, r)).astype(out.dtype)
        o = pltpu.make_async_copy(obuf.at[r], out.at[r], out_sem.at[c])
        o.start()
        out_copies.append(o)

    for s in pending:
        s.wait_send()
    for c in range(CH):

        @pl.when(across(c))
        def _():
            kv_copy(sp, c, xsend, to_xo).wait_send()

        @pl.when(not_top)
        def _():
            kv_copy(sp, c, zsend, to_up).wait_send()

        @pl.when(helped)
        def _():
            q_copy(c).wait_send()

        @pl.when(helper)
        def _():
            for s in part_copies(c):
                s.wait_send()

    for c in via_z:

        @pl.when(not_top)
        def _():
            kv_copy(j_xo, c, zfwd, to_up).wait_send()

    for c in via_x:

        @pl.when(above0)
        def _():
            kv_copy(j_b, c, xfwd, to_xo).wait_send()

    @pl.when(not_top)
    def _():
        for c in cum_up:
            c.wait_send()

    @pl.when(sp < SP - 1)
    def _():
        halo_copy.wait_send()

    for k in range(1, SP):

        @pl.when(sp + k < SP)
        def _():
            end_copy(k).wait_send()

    for o in out_copies:
        o.wait()


def block_shards(SP, TP, X, *args):
    tokens, lru_in, gate_in, query_w = args[:4]
    (conv_weight, rg_w, ig_w, rate, decay_extra, forget, out_lru, out_fox) = args[6:]
    rows, dcols = tokens.shape
    D, lw = lru_in.shape
    fw = query_w.shape[1]
    oc = out_lru.shape[1] // TP
    tot = 2 * lw + 3 * fw
    H = fw // HEAD_DIM
    CH = 4
    rc = rows // CH
    bw = rg_w.shape[1]
    hbm = pl.BlockSpec(memory_space=pl.ANY)
    dma = pltpu.SemaphoreType.DMA
    V = pltpu.VMEM
    scratch = [
        V((TP, rows, dcols), BF16),
        V((D, tot), BF16),
        V((2, rc, tot), F32),
        V((2, rc, 1), F32),
        V((rows, lw), BF16),
        V((16, lw), BF16),
        V((rows + 8, lw), F32),
        V(conv_weight.shape, BF16),
        V((lw // bw, bw, bw), BF16),
        V((lw // bw, bw, bw), BF16),
        V((1, rate.shape[0]), F32),
        V((H, rows), F32),
        V((lw, lw), BF16),
        V((lw, lw), BF16),
        V((rows, lw), BF16),
        V((rows, fw), BF16),
        V((rows, lw), F32),
        V((lw // 128, rows, 128), F32),
        V((lw // 128, rows, 128), F32),
        V((8, lw), F32),
        V((8, lw), F32),
        V((8, lw), F32),
        V((SP, 8, lw), F32),
        V((SP, rows, 2 * fw), BF16),
        V((SP, 8, rows), F32),
        V((H, rows, 128), F32),
        V((H, rows, 2 * HEAD_DIM), F32),
        V((rows, fw), BF16),
        V((H, rows, 128), F32),
        V((H, rows, 2 * HEAD_DIM), F32),
        V((rows, fw), BF16),
        V((CH, 8, rc), F32),
        V((rows, fw), BF16),
        V((CH, 8, rc), F32),
        V((TP, lw, oc), BF16),
        V((TP, fw, oc), BF16),
        V((TP, rows, lw), BF16),
        V((TP, rows, fw), BF16),
        V((rows, oc), F32),
        V((rows, oc), BF16),
        dma((14,)),
        dma((CH,)),
        dma((2, CH)),
        dma((CH,)),
        dma((TP, CH)),
        dma((1,)),
        dma((1,)),
        dma((SP,)),
        dma((SP,)),
        dma((3,)),
        dma((SP,)),
        dma((CH,)),
        dma((CH,)),
        dma((CH,)),
        dma((CH,)),
        dma((SP, CH)),
        dma((2, 4)),
        dma((2, 2)),
        dma((2, TP, X)),
        dma((2,)),
        dma((TP,)),
        dma((2, CH)),
        dma((CH,)),
        dma((TP, CH)),
        dma((1,)),
        dma((CH,)),
        dma((CH,)),
        dma((CH, 2)),
        dma((CH, 2)),
    ]
    return pl.pallas_call(
        functools.partial(block_kernel, SP, TP, X, CH),
        out_shape=jax.ShapeDtypeStruct((rows, oc), BF16),
        in_specs=[hbm] * 14,
        out_specs=hbm,
        scratch_shapes=scratch,
        compiler_params=pltpu.CompilerParams(
            collective_id=1, has_side_effects=True, vmem_limit_bytes=60 * 1024 * 1024
        ),
    )(*args[:9], rate.reshape(1, -1), decay_extra, forget.T, out_lru, out_fox)


def columns_of(mesh):
    SP = mesh.shape["sp"]
    try:
        X = len({d.coords[0] for d in mesh.devices.flat})
    except AttributeError:
        X = 2
    return X if SP % X == 0 else 1


def solution(mesh):
    placed = (
        P("sp", "tp"),
        P(None, "tp"),
        P(None, "tp"),
        P(None, "tp"),
        P(None, "tp"),
        P(None, "tp"),
        P(),
        P(),
        P(),
        P(),
        P("sp", "tp"),
        P("sp", "tp"),
        P("tp", None),
        P("tp", None),
    )
    SP, TP, X = mesh.shape["sp"], mesh.shape["tp"], columns_of(mesh)
    small = X == 2 and TP == 4 and SP // X in (3, 4)
    body = functools.partial(block_shards if small else shards, SP, TP, X)
    return jax.shard_map(
        body, mesh=mesh, in_specs=placed, out_specs=P("sp", "tp"), check_vma=False
    )
```

```python
import functools

import jax
import jax.numpy as jnp
from jax import lax
from jax.experimental import pallas as pl
from jax.experimental.pallas import tpu as pltpu
from jax.sharding import PartitionSpec as P

HEAD_DIM = 128
decay_sharpness = 8.0
epsilon_norm = 1e-06
MESH = pl.DeviceIdType.MESH
F32 = jnp.float32
BF16 = jnp.bfloat16


def one_minus_exp(w):
    u = -w
    series = 1.0 - u / 9.0
    for n in range(8, 1, -1):
        series = 1.0 - u / n * series
    return jnp.where(u < 0.5, u * series, 1.0 - jnp.exp(w))


def remote(src, dst, send_sem, recv_sem, device):
    return pltpu.make_async_remote_copy(
        src_ref=src,
        dst_ref=dst,
        send_sem=send_sem,
        recv_sem=recv_sem,
        device_id=device,
        device_id_type=MESH,
    )


def kernel(
    SP,
    TP,
    X,
    tokens,
    lru_in,
    gate_in,
    query_w,
    key_w,
    value_w,
    conv_w,
    rg_w,
    ig_w,
    rate,
    decay_extra,
    forget,
    out_lru,
    out_fox,
    out,
    tok_buf,
    w_buf,
    acc,
    sq,
    lru_ref,
    halo,
    pad,
    bd_r,
    bd_i,
    gate_ref,
    q_ref,
    decay_buf,
    prefix_ref,
    local_ref,
    ends,
    incoming,
    kv_buf,
    cum_buf,
    cum_pad,
    wide,
    fcol,
    m_ref,
    l_ref,
    o_ref,
    q_far,
    m_far,
    l_far,
    o_far,
    part_out,
    stat_out,
    part_in,
    stat_in,
    wl_buf,
    wf_buf,
    br_lru,
    br_fox,
    oacc,
    load_sem,
    tsend,
    tfwd,
    trecv,
    hsend,
    hrecv,
    esend,
    erecv,
    zsend,
    xsend,
    kvrecv,
    wsend,
    wrecv,
    lsend,
    lrecv,
    fsend,
    ffwd,
    frecv,
    lfwd,
    qsend,
    qrecv,
    osend,
    orecv,
):
    rows, dcols = tokens.shape
    D, lw = lru_in.shape
    fw = query_w.shape[1]
    H = fw // HEAD_DIM
    oc = out.shape[1]
    Y = TP // 2
    Z = SP // X
    CH = tsend.shape[1]
    rc = rows // CH
    sp = lax.axis_index("sp")
    tp = lax.axis_index("tp")
    z = lax.div(sp, X)
    x = lax.rem(sp, X)
    partner = tp + 1 - 2 * lax.rem(tp, 2)
    far = [lax.rem(tp + 2 * k, TP) for k in range(Y)]
    pfar = [lax.rem(partner + 2 * k, TP) for k in range(Y)]
    offs = [0, lw, lw + fw, lw + 2 * fw, 2 * lw + 2 * fw, 2 * lw + 3 * fw]

    barrier = pltpu.get_barrier_semaphore()
    for k in range(1, SP):
        pl.semaphore_signal(
            barrier, inc=1, device_id={"sp": lax.rem(sp + k, SP)}, device_id_type=MESH
        )
    for k in range(1, TP):
        pl.semaphore_signal(
            barrier, inc=1, device_id={"tp": lax.rem(tp + k, TP)}, device_id_type=MESH
        )
    loads = []
    for i, w in enumerate((lru_in, key_w, value_w, gate_in, query_w)):
        c = pltpu.make_async_copy(w, w_buf.at[:, offs[i] : offs[i + 1]], load_sem.at[i])
        c.start()
        loads.append(c)
    mine = pl.ds(pl.multiple_of(tp * oc, 128), oc)
    own_loads = [
        pltpu.make_async_copy(decay_extra, decay_buf, load_sem.at[5]),
        pltpu.make_async_copy(out_lru.at[:, mine], wl_buf.at[tp], load_sem.at[6]),
        pltpu.make_async_copy(out_fox.at[:, mine], wf_buf.at[tp], load_sem.at[7]),
    ]
    for c in own_loads:
        c.start()
    pl.semaphore_wait(barrier, SP - 1 + TP - 1)

    pending = []

    def chunk(c):
        return pl.ds(c * rc, rc)

    for c in range(CH):
        for k in range(1, Y):
            s = remote(
                tokens.at[chunk(c)],
                tok_buf.at[tp, chunk(c)],
                tsend.at[k, c],
                trecv.at[tp, c],
                {"tp": far[k]},
            )
            s.start()
            pending.append(s)
    for c in range(CH):
        s = remote(
            tokens.at[chunk(c)],
            tok_buf.at[tp, chunk(c)],
            tsend.at[0, c],
            trecv.at[tp, c],
            {"tp": partner},
        )
        s.start()
        pending.append(s)

    bw = rg_w.shape[1]
    nb = lw // bw
    bd_r[...] = jnp.zeros_like(bd_r)
    bd_i[...] = jnp.zeros_like(bd_i)
    for n in range(nb):
        sl = pl.ds(n * bw, bw)
        bd_r[sl, sl] = rg_w[tp * nb + n]
        bd_i[sl, sl] = ig_w[tp * nb + n]
    cum_pad[...] = jnp.zeros_like(cum_pad)
    wide[...] = jnp.zeros_like(wide)
    wide[0:H, :] = forget[...]
    fcol[...] = wide[...].T
    cum_buf[sp] = wide[0:8, :]

    for c in loads:
        c.wait()

    def project(val, src, r, first=False):
        w_rows = pl.ds(pl.multiple_of(src * dcols, dcols), dcols)
        v32 = val.astype(F32)
        part = jnp.sum(v32 * v32, axis=1, keepdims=True)
        dot = jnp.dot(val, w_buf[w_rows, :], preferred_element_type=F32)
        if first:
            sq[r, :] = part
            acc[r, :] = dot
        else:
            sq[r, :] += part
            acc[r, :] += dot

    def tok_wait(src, c):
        ref = tok_buf.at[src, chunk(c)]
        remote(ref, ref, tsend.at[0, c], trecv.at[src, c], {"tp": partner}).wait_recv()

    for c in range(CH):
        project(tokens[chunk(c), :], tp, chunk(c), True)
    for c in range(CH):
        tok_wait(partner, c)
        project(tok_buf[partner, chunk(c), :], partner, chunk(c))
    for c in range(CH):
        for k in range(1, Y):
            tok_wait(far[k], c)
            ref = tok_buf.at[far[k], chunk(c)]
            s = remote(ref, ref, tfwd.at[k, c], trecv.at[far[k], c], {"tp": partner})
            s.start()
            pending.append(s)
            project(tok_buf[far[k], chunk(c), :], far[k], chunk(c))
        for k in range(1, Y):
            tok_wait(pfar[k], c)
            project(tok_buf[pfar[k], chunk(c), :], pfar[k], chunk(c))

    row_scale = lax.rsqrt(sq[...] / D + epsilon_norm)

    def scaled(i, n=1):
        return (acc[:, offs[i] : offs[i + n]] * row_scale).astype(BF16)

    lru_ref[...] = scaled(0)
    hb = halo.shape[0]
    halo_copy = remote(
        lru_ref.at[pl.ds(rows - hb, hb)],
        halo,
        hsend.at[0],
        hrecv.at[0],
        {"sp": lax.rem(sp + 1, SP)},
    )

    @pl.when(sp < SP - 1)
    def _():
        halo_copy.start()

    kv_buf[sp] = scaled(1, 2)

    paired = Z in (3, 4)
    helper = jnp.logical_and(z <= Z - 3, paired)
    helped = jnp.logical_and(z >= 2, paired)

    def block_copies(j, a, send_sem, device):
        return (
            remote(kv_buf.at[j], kv_buf.at[j], send_sem.at[a, 0], kvrecv.at[j, 0], device),
            remote(cum_buf.at[j], cum_buf.at[j], send_sem.at[a, 1], kvrecv.at[j, 1], device),
        )

    def z_copies(dz):
        j = (z - dz) * X + x
        return block_copies(j, dz, zsend, {"sp": lax.rem(sp + X, SP)})

    def x_copies(dz, dx):
        j = (z - dz) * X + x
        xo = lax.rem(x + dx, X)
        return block_copies(j, dz, xsend.at[dx - 1], {"sp": z * X + xo})

    def for_sends(dz, own, act):
        if own or not paired:

            @pl.when(z < Z - 1)
            def _():
                for c in z_copies(dz):
                    act(c)

        for dx in range(1, X):
            if own:

                @pl.when(jnp.logical_or(lax.rem(x + dx, X) > x, helper))
                def _():
                    for c in x_copies(dz, dx):
                        act(c)
            else:
                for c in x_copies(dz, dx):
                    act(c)

    def kv_wait(j):
        for c in block_copies(j, 0, zsend, {"sp": lax.rem(sp + X, SP)}):
            c.wait_recv()

    for_sends(0, True, lambda c: c.start())

    q_ref[...] = scaled(4)
    q_copy = remote(
        q_ref, q_far, qsend.at[0], qrecv.at[0], {"sp": lax.rem(sp + SP - 2 * X, SP)}
    )

    @pl.when(helped)
    def _():
        q_copy.start()

    for i, (w, buf) in enumerate(((out_lru, wl_buf), (out_fox, wf_buf))):
        for k in range(1, TP):
            t = lax.rem(tp + k, TP)
            cols = pl.ds(pl.multiple_of(t * oc, 128), oc)
            s = remote(w.at[:, cols], buf.at[tp], wsend.at[i, k], wrecv.at[i, tp], {"tp": t})
            s.start()
            pending.append(s)

    gate_ref[...] = scaled(3)

    @pl.when(sp == 0)
    def _():
        pad[0:8, :] = jnp.zeros((8, lw), F32)

    @pl.when(sp > 0)
    def _():
        halo_copy.wait_recv()
        pad[0:8, :] = halo[...].astype(F32)[hb - 8 : hb, :]

    pad[8 : 8 + rows, :] = lru_ref[...].astype(F32)
    chans = pl.ds(pl.multiple_of(tp * lw, 128), lw)
    taps = conv_w.shape[0]
    taps_f32 = conv_w[:, chans].astype(F32)
    conv = jnp.zeros((rows, lw), F32)
    for j in range(taps):
        conv = conv + taps_f32[j : j + 1, :] * pad[8 - (taps - 1) + j : 8 - (taps - 1) + j + rows, :]
    conv_b = conv.astype(BF16)

    def sigmoid(v):
        return 1.0 / (1.0 + jnp.exp(-v))

    recur_gate = sigmoid(jnp.dot(conv_b, bd_r[...], preferred_element_type=F32))
    input_gate = sigmoid(jnp.dot(conv_b, bd_i[...], preferred_element_type=F32))
    own_rate = rate[:, chans]
    softplus = jnp.maximum(-own_rate, 0.0) + jnp.log1p(jnp.exp(-jnp.abs(own_rate)))
    for c in own_loads:
        c.wait()
    log_decay = -decay_sharpness * softplus * recur_gate + decay_buf[...]
    prefix_ref[...] = jnp.exp(log_decay)
    local_ref[...] = jnp.sqrt(one_minus_exp(2.0 * log_decay)) * input_gate * conv_b.astype(F32)
    row_id = lax.broadcasted_iota(jnp.int32, (rows, lw), 0)
    step = 1
    while step < rows:
        a = prefix_ref[...]
        b = local_ref[...]
        keep = row_id >= step
        a_prev = jnp.where(keep, pltpu.roll(a, step, 0), 1.0)
        b_prev = jnp.where(keep, pltpu.roll(b, step, 0), 0.0)
        local_ref[...] = b + a * b_prev
        prefix_ref[...] = a * a_prev
        step *= 2
    ends[sp, 0:1, :] = prefix_ref[rows - 1 : rows, :]
    ends[sp, 1:2, :] = local_ref[rows - 1 : rows, :]

    def end_copy(k):
        return remote(
            ends.at[sp], ends.at[sp], esend.at[k], erecv.at[sp], {"sp": lax.rem(sp + k, SP)}
        )

    for k in range(1, SP):

        @pl.when(sp + k < SP)
        def _():
            end_copy(k).start()

    score_scale = HEAD_DIM ** (-0.5)
    qc = rows // 2

    def attend(j, diagonal, far_first=None):
        other = far_first is not None
        first = diagonal or far_first
        qs, ms, ls, os = (q_far, m_far, l_far, o_far) if other else (q_ref, m_ref, l_ref, o_ref)

        def some(i, carry):
            r = pl.ds(pl.multiple_of(i * qc, qc), qc)
            for h in range(H):
                hs = slice(h * HEAD_DIM, (h + 1) * HEAD_DIM)
                vs = slice(fw + h * HEAD_DIM, fw + (h + 1) * HEAD_DIM)
                s = lax.dot_general(
                    qs[r, hs],
                    kv_buf[j, :, hs],
                    (((1,), (1,)), ((), ())),
                    preferred_element_type=F32,
                )
                s = s * score_scale
                if not other:
                    s = s + fcol[r, h : h + 1]
                s = s - cum_buf[j, h : h + 1, :]
                if diagonal:
                    causal = (
                        lax.broadcasted_iota(jnp.int32, (qc, rows), 0) + i * qc
                        >= lax.broadcasted_iota(jnp.int32, (qc, rows), 1)
                    )
                    s = jnp.where(causal, s, -1e30)
                top = jnp.max(s, axis=1, keepdims=True)
                if first:
                    p = jnp.exp(s - top)
                    ms[h, r, :] = top
                    ls[h, r, :] = jnp.sum(p, axis=1, keepdims=True)
                    os[h, r, :] = jnp.dot(
                        p.astype(BF16), kv_buf[j, :, vs], preferred_element_type=F32
                    )
                else:
                    old = ms[h, r, :]
                    new = jnp.maximum(old, top)
                    p = jnp.exp(s - new)
                    fade = jnp.exp(old - new)
                    ms[h, r, :] = new
                    ls[h, r, :] = ls[h, r, :] * fade + jnp.sum(p, axis=1, keepdims=True)
                    os[h, r, :] = os[h, r, :] * fade + jnp.dot(
                        p.astype(BF16), kv_buf[j, :, vs], preferred_element_type=F32
                    )
            return carry

        lax.fori_loop(0, rows // qc, some, 0)

    attend(sp, True)

    def row_blocks(dz):
        for dx in range(1, X):
            xo = lax.rem(x + dx, X)

            @pl.when(jnp.logical_or(dz > 0, xo < x))
            def _():
                j = (z - dz) * X + xo
                kv_wait(j)
                attend(j, False)

    def finish_lru():
        incoming[...] = jnp.zeros_like(incoming)
        for j in range(SP - 1):

            @pl.when(j < sp)
            def _():
                remote(
                    ends.at[j], ends.at[j], esend.at[0], erecv.at[j], {"sp": lax.rem(sp + 1, SP)}
                ).wait_recv()
                incoming[...] = ends[j, 0:1, :] * incoming[...] + ends[j, 1:2, :]

        states = local_ref[...] + prefix_ref[...] * incoming[...]
        g = gate_ref[...].astype(F32)
        gelu = 0.5 * g * (1.0 + jnp.tanh(0.7978845608028654 * (g + 0.044715 * (g * g * g))))
        br_lru[tp] = (states * gelu).astype(BF16)
        for k in range(Y - 1, -1, -1):
            lru_copy(k).start()

    def lru_copy(k):
        to = far[k] if k else partner
        return remote(br_lru.at[tp], br_lru.at[tp], lsend.at[k], lrecv.at[tp], {"tp": to})

    lru_step = min(2, Z - 1)
    if Z == 1:
        finish_lru()

    def hop(dz, carry):
        @pl.when(dz <= z)
        def _():
            j = (z - dz) * X + x
            kv_wait(j)
            for_sends(dz, False, lambda c: c.start())
            row_blocks(dz - 1)
            attend(j, False)

        @pl.when(dz == lru_step)
        def _():
            finish_lru()

        return carry

    up = {"sp": lax.rem(sp + 2 * X, SP)}
    part_copies = (
        remote(part_out, part_in, osend.at[0], orecv.at[0], up),
        remote(stat_out, stat_in, osend.at[1], orecv.at[1], up),
    )

    def send_partial():
        for h in range(H):
            part_out[:, h * HEAD_DIM : (h + 1) * HEAD_DIM] = o_far[h].astype(BF16)
            cum_pad[:, h : h + 1] = m_far[h]
            cum_pad[:, H + h : H + h + 1] = l_far[h]
        stat_out[...] = cum_pad[...].T[0:8, :]
        for c in part_copies:
            c.start()

    if paired:
        below = (z - 1) * X

        @pl.when(helper)
        def _():
            q_copy.wait_recv()
            attend(sp, False, True)

        @pl.when(z >= 1)
        def _():
            kv_wait(below + x)
            for_sends(1, False, lambda c: c.start())

        for dx in range(1, X):
            xo = lax.rem(x + dx, X)

            @pl.when(jnp.logical_or(xo < x, helper))
            def _():
                kv_wait(z * X + xo)

            @pl.when(helper)
            def _():
                attend(z * X + xo, False, False)

        @pl.when(jnp.logical_and(helper, z == 0))
        def _():
            send_partial()

        for dx in range(1, X):
            xo = lax.rem(x + dx, X)

            @pl.when(xo < x)
            def _():
                attend(z * X + xo, False)

        finish_lru()

        @pl.when(jnp.logical_and(helper, z >= 1))
        def _():
            attend(below + x, False, False)

        @pl.when(z >= 1)
        def _():
            attend(below + x, False)
            for dx in range(1, X):
                j = below + lax.rem(x + dx, X)
                kv_wait(j)

                @pl.when(helper)
                def _():
                    attend(j, False, False)

            @pl.when(helper)
            def _():
                send_partial()

            for dx in range(1, X):
                attend(below + lax.rem(x + dx, X), False)

    else:
        lax.fori_loop(1, Z, hop, 0)

    def lru_wait(t):
        remote(br_lru.at[t], br_lru.at[t], lsend.at[0], lrecv.at[t], {"tp": partner}).wait_recv()

    def lru_dot(t):
        return jnp.dot(br_lru[t], wl_buf[t], preferred_element_type=F32)

    oacc[...] = lru_dot(tp)
    for k in range(1, TP):
        t = lax.rem(tp + k, TP)
        for i, buf in enumerate((wl_buf, wf_buf)):
            remote(buf.at[t], buf.at[t], wsend.at[i, k], wrecv.at[i, t], {"tp": t}).wait_recv()
    for k in range(1, Y):
        lru_wait(far[k])
        ref = br_lru.at[far[k]]
        s = remote(ref, ref, lfwd.at[k], lrecv.at[far[k]], {"tp": partner})
        s.start()
        pending.append(s)
    lru_wait(partner)
    oacc[...] += lru_dot(partner)
    for k in range(1, Y):
        oacc[...] += lru_dot(far[k])
        lru_wait(pfar[k])
        oacc[...] += lru_dot(pfar[k])

    if paired:

        @pl.when(helped)
        def _():
            for c in part_copies:
                c.wait_recv()
            wide[0:8, :] = stat_in[...]
            stats = wide[...].T
            for h in range(H):
                m_in = stats[:, h : h + 1] + fcol[:, h : h + 1]
                l_in = stats[:, H + h : H + h + 1]
                part = part_in[:, h * HEAD_DIM : (h + 1) * HEAD_DIM].astype(F32)
                new = jnp.maximum(m_ref[h], m_in)
                fade = jnp.exp(m_ref[h] - new)
                grow = jnp.exp(m_in - new)
                l_ref[h] = l_ref[h] * fade + l_in * grow
                o_ref[h] = o_ref[h] * fade + part * grow

    else:
        row_blocks(z)

    for c in range(CH):
        r = chunk(c)
        for h in range(H):
            br_fox[tp, r, h * HEAD_DIM : (h + 1) * HEAD_DIM] = (
                o_ref[h, r, :] / l_ref[h, r, :]
            ).astype(BF16)
        ref = br_fox.at[tp, r]
        for k in list(range(1, Y)) + [0]:
            to = far[k] if k else partner
            s = remote(ref, ref, fsend.at[k, c], frecv.at[tp, c], {"tp": to})
            s.start()
            pending.append(s)

    def fox_wait(src, c):
        ref = br_fox.at[src, chunk(c)]
        remote(ref, ref, fsend.at[0, c], frecv.at[src, c], {"tp": partner}).wait_recv()

    def fox_dot(src, r):
        return jnp.dot(br_fox[src, r, :], wf_buf[src], preferred_element_type=F32)

    for c in range(CH):
        fox_wait(partner, c)
        oacc[chunk(c), :] += fox_dot(tp, chunk(c)) + fox_dot(partner, chunk(c))
    for c in range(CH):
        r = chunk(c)
        for k in range(1, Y):
            fox_wait(far[k], c)
            ref = br_fox.at[far[k], r]
            s = remote(ref, ref, ffwd.at[k, c], frecv.at[far[k], c], {"tp": partner})
            s.start()
            pending.append(s)
            oacc[r, :] += fox_dot(far[k], r)
        for k in range(1, Y):
            fox_wait(pfar[k], c)
            oacc[r, :] += fox_dot(pfar[k], r)
        out[r, :] = oacc[r, :].astype(out.dtype)

    for s in pending:
        s.wait_send()
    for k in range(Y):
        lru_copy(k).wait_send()

    @pl.when(helped)
    def _():
        q_copy.wait_send()

    @pl.when(helper)
    def _():
        for c in part_copies:
            c.wait_send()

    @pl.when(sp < SP - 1)
    def _():
        halo_copy.wait_send()

    for k in range(1, SP):

        @pl.when(sp + k < SP)
        def _():
            end_copy(k).wait_send()

    for_sends(0, True, lambda c: c.wait_send())

    def drain(dz, carry):
        @pl.when(dz <= z)
        def _():
            for_sends(dz, False, lambda c: c.wait_send())

        return carry

    if paired:

        @pl.when(z >= 1)
        def _():
            for_sends(1, False, lambda c: c.wait_send())

    else:
        lax.fori_loop(1, Z, drain, 0)


def shards(SP, TP, X, *args):
    tokens, lru_in, gate_in, query_w = args[:4]
    (conv_weight, rg_w, ig_w, rate, decay_extra, forget, out_lru, out_fox) = args[6:]
    rows, dcols = tokens.shape
    D, lw = lru_in.shape
    fw = query_w.shape[1]
    oc = out_lru.shape[1] // TP
    tot = 2 * lw + 3 * fw
    H = fw // HEAD_DIM
    Y = TP // 2
    Z = SP // X
    CH = 4
    vm = pl.BlockSpec(memory_space=pltpu.VMEM)
    hbm = pl.BlockSpec(memory_space=pl.ANY)
    dma = pltpu.SemaphoreType.DMA
    V = pltpu.VMEM
    scratch = [
        V((TP, rows, dcols), BF16),
        V((D, tot), BF16),
        V((rows, tot), F32),
        V((rows, 1), F32),
        V((rows, lw), BF16),
        V((16, lw), BF16),
        V((rows + 8, lw), F32),
        V((lw, lw), BF16),
        V((lw, lw), BF16),
        V((rows, lw), BF16),
        V((rows, fw), BF16),
        V((rows, lw), F32),
        V((rows, lw), F32),
        V((rows, lw), F32),
        V((SP, 8, lw), F32),
        V((1, lw), F32),
        V((SP, rows, 2 * fw), BF16),
        V((SP, 8, rows), F32),
        V((rows, 128), F32),
        V((128, rows), F32),
        V((rows, 128), F32),
        V((H, rows, 1), F32),
        V((H, rows, 1), F32),
        V((H, rows, HEAD_DIM), F32),
        V((rows, fw), BF16),
        V((H, rows, 1), F32),
        V((H, rows, 1), F32),
        V((H, rows, HEAD_DIM), F32),
        V((rows, fw), BF16),
        V((8, rows), F32),
        V((rows, fw), BF16),
        V((8, rows), F32),
        V((TP, lw, oc), BF16),
        V((TP, fw, oc), BF16),
        V((TP, rows, lw), BF16),
        V((TP, rows, fw), BF16),
        V((rows, oc), F32),
        dma((8,)),
        dma((Y, CH)),
        dma((Y, CH)),
        dma((TP, CH)),
        dma((1,)),
        dma((1,)),
        dma((SP,)),
        dma((SP,)),
        dma((Z, 2)),
        dma((max(X - 1, 1), Z, 2)),
        dma((SP, 2)),
        dma((2, TP)),
        dma((2, TP)),
        dma((TP,)),
        dma((TP,)),
        dma((Y, CH)),
        dma((Y, CH)),
        dma((TP, CH)),
        dma((Y,)),
        dma((1,)),
        dma((1,)),
        dma((2,)),
        dma((2,)),
    ]
    return pl.pallas_call(
        functools.partial(kernel, SP, TP, X),
        out_shape=jax.ShapeDtypeStruct((rows, oc), BF16),
        in_specs=[vm] + [hbm] * 5 + [vm] * 4 + [hbm, vm, hbm, hbm],
        out_specs=vm,
        scratch_shapes=scratch,
        compiler_params=pltpu.CompilerParams(
            collective_id=0, has_side_effects=True, vmem_limit_bytes=60 * 1024 * 1024
        ),
    )(*args[:9], rate.reshape(1, -1), decay_extra, forget.T, out_lru, out_fox)


LOG2E = 1.4426950408889634


def block_kernel(
    SP,
    TP,
    X,
    CH,
    tokens,
    lru_in,
    gate_in,
    query_w,
    key_w,
    value_w,
    conv_w,
    rg_w,
    ig_w,
    rate,
    decay_extra,
    forget,
    out_lru,
    out_fox,
    out,
    tok_buf,
    w_buf,
    acc,
    sq,
    lru_ref,
    halo,
    pad,
    conv_v,
    rg_v,
    ig_v,
    rate_v,
    forget_v,
    bd_r,
    bd_i,
    gate_ref,
    q_ref,
    decay_buf,
    prefix_ref,
    local_ref,
    seg_a,
    seg_b,
    carry_ref,
    ends,
    kv_buf,
    cum_buf,
    m_ref,
    o_ref,
    q_far,
    m_far,
    o_far,
    part_out,
    stat_out,
    part_in,
    stat_in,
    wl_buf,
    wf_buf,
    br_lru,
    br_fox,
    oacc,
    load_sem,
    tsend,
    trecv,
    hsend,
    hrecv,
    esend,
    erecv,
    csend,
    crecv,
    zsend,
    xsend,
    zfwd,
    xfwd,
    kvrecv,
    wsend,
    wrecv_own,
    wrecv,
    lsend,
    lrecv,
    fsend,
    frecv,
    qsend,
    qrecv,
    osend,
    orecv,
):
    rows, dcols = tokens.shape
    D, lw = lru_in.shape
    fw = query_w.shape[1]
    H = fw // HEAD_DIM
    oc = out.shape[1]
    Z = SP // X
    rc = rows // CH
    half = rows // 2
    wh = out_lru.shape[0] // X
    sp = lax.axis_index("sp")
    tp = lax.axis_index("tp")
    z = lax.div(sp, X)
    x = lax.rem(sp, X)
    xo = 1 - x
    y = lax.div(tp, 2)
    partner = tp + 1 - 2 * lax.rem(tp, 2)
    far = lax.rem(tp + 2, TP)
    pfar = lax.rem(partner + 2, TP)
    j_xo = z * X + xo
    to_xo = {"sp": j_xo}
    to_up = {"sp": lax.rem(sp + X, SP)}
    j_b = lax.rem(sp + SP - X, SP)
    j_bo = lax.rem(j_xo + SP - X, SP)
    helper = z <= Z - 3
    helped = z >= 2
    not_top = z < Z - 1
    above0 = z >= 1
    order = list(range(CH - 1, -1, -1))
    via_x = order[0::2]
    via_z = order[1::2]
    goes_up = jnp.logical_and(not_top, z != Z - 3)
    all_over_x = z == Z - 2
    whalf = lax.rem(x + z, X)
    odd = lax.rem(z, 2) == 1
    PARTNER, FAR, PFAR = 0, 1, 2
    ACROSS, BELOW, DIAG = 0, 1, 2
    score_k = HEAD_DIM ** (-0.5) * LOG2E

    def chunk(c):
        return pl.ds(c * rc, rc)

    barrier = pltpu.get_barrier_semaphore()
    for k in range(1, SP):
        pl.semaphore_signal(
            barrier, inc=1, device_id={"sp": lax.rem(sp + k, SP)}, device_id_type=MESH
        )
    for k in range(1, TP):
        pl.semaphore_signal(
            barrier, inc=1, device_id={"tp": lax.rem(tp + k, TP)}, device_id_type=MESH
        )

    def load(i, src, dst):
        c = pltpu.make_async_copy(src, dst, load_sem.at[i])
        c.start()
        return c

    tok_loads = [
        load(n, tokens.at[chunk(c)], tok_buf.at[tp, chunk(c)]) for n, c in enumerate(order)
    ]
    cols = (0, fw, 2 * fw, 2 * fw + lw, 3 * fw + lw, 3 * fw + 2 * lw)
    for i, w in enumerate((key_w, value_w, lru_in, query_w, gate_in)):
        load(CH, w, w_buf.at[:, cols[i] : cols[i + 1]])
    mine = pl.ds(pl.multiple_of(tp * oc, 128), oc)
    bw = rg_w.shape[1]
    nb = lw // bw
    gates = pl.ds(tp * nb, nb)
    forget_load = load(CH + 1, forget, forget_v)
    small_loads = [
        load(CH + 2, conv_w, conv_v),
        load(CH + 3, rg_w.at[gates], rg_v),
        load(CH + 4, ig_w.at[gates], ig_v),
        load(CH + 5, rate, rate_v),
        load(CH + 6, decay_extra, decay_buf),
    ]
    own_loads = [
        load(CH + 7, out_lru.at[:, mine], wl_buf.at[tp]),
        load(CH + 8, out_fox.at[:, mine], wf_buf.at[tp]),
    ]
    pl.semaphore_wait(barrier, SP - 1 + TP - 1)

    def send(ref, send_sem, recv_sem, device):
        remote(ref, ref, send_sem, recv_sem, device).start()

    def arrived(ref, recv_sem):
        remote(ref, ref, recv_sem, recv_sem, to_xo).wait_recv()

    def sent(ref, send_sem):
        remote(ref, ref, send_sem, send_sem, to_xo).wait_send()

    for n, c in enumerate(order):
        tok_loads[n].wait()
        ref = tok_buf.at[tp, chunk(c)]
        send(ref, tsend.at[0], trecv.at[FAR, c], {"tp": far})
        send(ref, tsend.at[1], trecv.at[PARTNER, c], {"tp": partner})

    forget_load.wait()
    cum_buf[sp] = jnp.zeros_like(cum_buf[sp])
    cum_buf[sp, 0:H, :] = forget_v[...] * LOG2E
    own_cum = cum_buf.at[sp]
    send(own_cum, csend.at[0], crecv.at[ACROSS], to_xo)

    @pl.when(not_top)
    def _():
        send(own_cum, csend.at[1], crecv.at[BELOW], to_up)
        send(own_cum, csend.at[1], crecv.at[DIAG], {"sp": lax.rem(j_xo + X, SP)})

    for c in small_loads:
        c.wait()
    bd_r[...] = jnp.zeros_like(bd_r)
    bd_i[...] = jnp.zeros_like(bd_i)
    for n in range(nb):
        sl = pl.ds(n * bw, bw)
        bd_r[sl, sl] = rg_v[n]
        bd_i[sl, sl] = ig_v[n]
    pltpu.make_async_copy(w_buf, w_buf, load_sem.at[CH]).wait()

    def tok_wait(src, role, c):
        arrived(tok_buf.at[src, chunk(c)], trecv.at[role, c])

    def features(side, c):
        first = 2 * side
        return jnp.concatenate([tok_buf[first, chunk(c), :], tok_buf[first + 1, chunk(c), :]], axis=1)

    def w_rows(side):
        return pl.ds(pl.multiple_of(side * 2 * dcols, 2 * dcols), 2 * dcols)

    def squares(v):
        v32 = v.astype(F32)
        return jnp.sum(v32 * v32, axis=1, keepdims=True)

    def near_part(c, slot):
        tok_wait(partner, PARTNER, c)
        v = features(y, c)
        sq[slot] = squares(v)
        acc[slot] = jnp.dot(v, w_buf[w_rows(y), :], preferred_element_type=F32)

    halo_copy = remote(
        lru_ref.at[pl.ds(rows - halo.shape[0], halo.shape[0])],
        halo,
        hsend.at[0],
        hrecv.at[0],
        {"sp": lax.rem(sp + 1, SP)},
    )

    def kv_send(j, c, send_sem, role, device):
        send(kv_buf.at[j, chunk(c)], send_sem.at[0], kvrecv.at[role, c], device)

    def kv_wait(j, c, role):
        arrived(kv_buf.at[j, chunk(c)], kvrecv.at[role, c])

    def all_across(own_x):
        return jnp.logical_or(own_x, helper)

    def across(own_x, c):
        need = all_across(own_x)
        return jnp.logical_or(need, goes_up) if c in via_z else need

    def q_copy(c):
        return remote(
            q_ref.at[chunk(c)],
            q_far.at[chunk(c)],
            qsend.at[0],
            qrecv.at[0],
            {"sp": lax.rem(sp + SP - 2 * X, SP)},
        )

    def far_part(i, c, slot):
        tok_wait(far, FAR, c)
        send(tok_buf.at[far, chunk(c)], tsend.at[2], trecv.at[PFAR, c], {"tp": partner})
        if i + 1 < CH:
            near_part(order[i + 1], 1 - slot)
        tok_wait(pfar, PFAR, c)
        if i == CH - 1:
            send_weights()
        v = features(1 - y, c)
        row_scale = lax.rsqrt((sq[slot] + squares(v)) / D + epsilon_norm)

        def part(a, b):
            w = w_buf[w_rows(1 - y), cols[a] : cols[b]]
            both = acc[slot, :, cols[a] : cols[b]] + jnp.dot(v, w, preferred_element_type=F32)
            return (both * row_scale).astype(BF16)

        kv_buf[sp, chunk(c), :] = part(0, 2)

        @pl.when(across(x == 0, c))
        def _():
            kv_send(sp, c, xsend, ACROSS, to_xo)

        @pl.when(not_top)
        def _():
            kv_send(sp, c, zsend, BELOW, to_up)

        rest = part(2, 5)
        lru_ref[chunk(c), :] = rest[:, 0:lw]
        q_ref[chunk(c), :] = rest[:, lw : lw + fw]
        gate_ref[chunk(c), :] = rest[:, lw + fw :]

        @pl.when(helped)
        def _():
            q_copy(c).start()

        if i == 0:

            @pl.when(sp < SP - 1)
            def _():
                halo_copy.start()

    banks = ((out_lru, wl_buf), (out_fox, wf_buf))

    def send_weights():
        r = pl.ds(pl.multiple_of(whalf * wh, wh), wh)
        for n, (w, buf) in enumerate(banks):
            for role, t in ((FAR, far), (PFAR, pfar)):
                c = pl.ds(pl.multiple_of(t * oc, 128), oc)
                remote(
                    w.at[r, c], buf.at[tp, r], wsend.at[0], wrecv.at[n, role - 1, whalf], {"tp": t}
                ).start()
        c = pl.ds(pl.multiple_of(partner * oc, 128), oc)
        for n, (w, buf) in enumerate(banks):
            remote(w.at[:, c], buf.at[tp], wsend.at[1], wrecv_own.at[n], {"tp": partner}).start()

    def weight_part(n, role, k):
        t = far if role == FAR else pfar
        ref = banks[n][1].at[t, pl.ds(pl.multiple_of(k * wh, wh), wh)]
        return ref, wrecv.at[n, role - 1, k]

    def weight_pass(n, role):
        ref, sem = weight_part(n, role, whalf)
        arrived(ref, sem)

        @pl.when(odd)
        def _():
            send(ref, wsend.at[2], sem, to_xo)
            send(ref, wsend.at[3], sem, {"sp": lax.rem(sp + SP - X, SP)})

    def weight_wait(n, role):
        arrived(*weight_part(n, role, 1 - whalf))

    def pass_up(c):
        @pl.when(goes_up)
        def _():
            kv_wait(j_xo, c, ACROSS)
            kv_send(j_xo, c, zfwd, DIAG, to_up)

    def pass_across(c):
        @pl.when(above0 if c in via_x else all_over_x)
        def _():
            kv_wait(j_b, c, BELOW)
            kv_send(j_b, c, xfwd, DIAG, to_xo)

    near_part(order[0], 0)
    for i, c in enumerate(order):
        far_part(i, c, i % 2)
        if i == CH - 2:
            pass_across(order[0])

    pass_up(order[1])
    pass_across(order[1])

    @pl.when(sp == 0)
    def _():
        pad[0:8, :] = jnp.zeros((8, lw), F32)

    @pl.when(sp > 0)
    def _():
        halo_copy.wait_recv()
        hb = halo.shape[0]
        pad[0:8, :] = halo[...].astype(F32)[hb - 8 : hb, :]

    pad[8 : 8 + rows, :] = lru_ref[...].astype(F32)
    chans = pl.ds(pl.multiple_of(tp * lw, 128), lw)
    taps = conv_w.shape[0]
    taps_f32 = conv_v[:, chans].astype(F32)
    conv = jnp.zeros((rows, lw), F32)
    for j in range(taps):
        conv = conv + taps_f32[j : j + 1, :] * pad[8 - (taps - 1) + j : 8 - (taps - 1) + j + rows, :]
    conv_b = conv.astype(BF16)

    def sigmoid(v):
        return 1.0 / (1.0 + jnp.exp(-v))

    recur_gate = sigmoid(jnp.dot(conv_b, bd_r[...], preferred_element_type=F32))
    input_gate = sigmoid(jnp.dot(conv_b, bd_i[...], preferred_element_type=F32))
    own_rate = rate_v[:, chans]
    softplus = jnp.maximum(-own_rate, 0.0) + jnp.log1p(jnp.exp(-jnp.abs(own_rate)))
    log_decay = -decay_sharpness * softplus * recur_gate + decay_buf[...]
    decay = jnp.exp(log_decay)
    driven = jnp.sqrt(one_minus_exp(2.0 * log_decay)) * input_gate * conv_b.astype(F32)
    for n in range(lw // 128):
        prefix_ref[n] = decay[:, n * 128 : (n + 1) * 128]
        local_ref[n] = driven[:, n * 128 : (n + 1) * 128]

    segs = 8
    seg_len = rows // segs
    run_a = jnp.ones((segs, lw), F32)
    run_b = jnp.zeros((segs, lw), F32)
    for i in range(seg_len):
        at = pl.ds(i, segs, stride=seg_len)
        a = [prefix_ref[n, at, :] for n in range(lw // 128)]
        b = [local_ref[n, at, :] for n in range(lw // 128)]
        a = jnp.concatenate(a, axis=1)
        b = jnp.concatenate(b, axis=1)
        run_a = run_a * a
        run_b = a * run_b + b
        for n in range(lw // 128):
            prefix_ref[n, at, :] = run_a[:, n * 128 : (n + 1) * 128]
            local_ref[n, at, :] = run_b[:, n * 128 : (n + 1) * 128]
    seg_a[...] = run_a
    seg_b[...] = run_b
    end_a = seg_a[0:1, :]
    end_b = seg_b[0:1, :]
    for i in range(1, segs):
        end_b = seg_a[i : i + 1, :] * end_b + seg_b[i : i + 1, :]
        end_a = end_a * seg_a[i : i + 1, :]
    ends[sp, 0:1, :] = end_a
    ends[sp, 1:2, :] = end_b

    def end_copy(k):
        return remote(
            ends.at[sp],
            ends.at[sp],
            esend.at[k - 1],
            erecv.at[lax.rem(sp, SP - 1)],
            {"sp": lax.rem(sp + k, SP)},
        )

    for k in range(1, SP):

        @pl.when(sp + k < SP)
        def _():
            end_copy(k).start()

    pass_across(order[2])

    def attend(qs, st, j, lo, hi, first=False, diagonal=False, qc=half, after=None):
        ms, os = st
        items = [(i, h) for i in range(rows // qc) for h in range(H)]

        def width(i):
            return (lo, (i + 1) * qc) if diagonal else (lo, hi)

        def scores(i, h):
            a, b = width(i)
            hs = slice(h * HEAD_DIM, (h + 1) * HEAD_DIM)
            s = lax.dot_general(
                qs[i * qc : (i + 1) * qc, hs],
                kv_buf[j, a:b, hs],
                (((1,), (1,)), ((), ())),
                preferred_element_type=F32,
            )
            s = s * score_k - cum_buf[j, h : h + 1, a:b]
            if diagonal:
                causal = (
                    lax.broadcasted_iota(jnp.int32, (qc, b - a), 0) + (i * qc - a)
                    >= lax.broadcasted_iota(jnp.int32, (qc, b - a), 1)
                )
                s = jnp.where(causal, s, -1e30)
            return s

        def update(i, h, s):
            a, b = width(i)
            r = slice(i * qc, (i + 1) * qc)
            top = jnp.max(s, axis=1, keepdims=True)
            if first:
                new = jnp.broadcast_to(top, (qc, 128))
            else:
                old = ms[h, r, :]
                new = jnp.maximum(old, top)
            ms[h, r, :] = new
            p = jnp.exp2(s - jnp.concatenate([new] * ((b - a) // 128), axis=1)).astype(BF16)
            v = kv_buf[j, a:b, fw + h * HEAD_DIM : fw + (h + 1) * HEAD_DIM]
            v1 = jnp.concatenate([v, jnp.ones((b - a, 128), BF16)], axis=1)
            pv = jnp.dot(p, v1, preferred_element_type=F32)
            if first:
                os[h, r, :] = pv
            else:
                fade = jnp.exp2(old - new)
                os[h, r, :] = os[h, r, :] * jnp.concatenate([fade, fade], axis=1) + pv

        s = scores(*items[0])
        for n, (i, h) in enumerate(items):
            nxt = scores(*items[n + 1]) if n + 1 < len(items) else None
            update(i, h, s)
            s = nxt
            if after is not None and h == H - 1:
                after(i)

    own_st = (m_ref, o_ref)
    far_st = (m_far, o_far)
    up2 = {"sp": lax.rem(sp + 2 * X, SP)}

    def part_copies(c):
        return (
            remote(part_out.at[chunk(c)], part_in.at[chunk(c)], osend.at[0], orecv.at[c, 0], up2),
            remote(stat_out.at[c], stat_in.at[c], osend.at[1], orecv.at[c, 1], up2),
        )

    def send_partial(c):
        r = slice(c * rc, (c + 1) * rc)
        lane = lax.broadcasted_iota(jnp.int32, (rc, 128), 1)
        stats = jnp.zeros((rc, 128), F32)
        for h in range(H):
            part_out[r, h * HEAD_DIM : (h + 1) * HEAD_DIM] = o_far[h, r, 0:HEAD_DIM].astype(BF16)
            stats = jnp.where(lane == h, m_far[h, r, :], stats)
            stats = jnp.where(lane == H + h, o_far[h, r, HEAD_DIM:], stats)
        stat_out[c] = stats.T[0:8, :]
        for s in part_copies(c):
            s.start()

    attend(q_ref, own_st, sp, 0, rows, True, True)

    pass_up(order[3])
    pass_across(order[3])

    arrived(cum_buf.at[j_xo], crecv.at[ACROSS])

    @pl.when(helper)
    def _():
        arrived(q_far, qrecv.at[0])
        attend(q_far, far_st, sp, 0, rows, True)

    for c in order:
        need = all_across(x == 1)
        if c in via_z:
            need = jnp.logical_and(need, jnp.logical_not(goes_up))

        @pl.when(need)
        def _():
            kv_wait(j_xo, c, ACROSS)

    @pl.when(helper)
    def _():
        attend(q_far, far_st, j_xo, 0, rows)

    @pl.when(jnp.logical_and(helper, z == 0))
    def _():
        for c in range(CH):
            send_partial(c)

    @pl.when(above0)
    def _():
        for c in via_z:

            @pl.when(jnp.logical_not(all_over_x))
            def _():
                kv_wait(j_b, c, BELOW)

        arrived(cum_buf.at[j_b], crecv.at[BELOW])
        arrived(cum_buf.at[j_bo], crecv.at[DIAG])

    @pl.when(jnp.logical_and(helper, above0))
    def _():
        attend(q_far, far_st, j_b, 0, rows)

    weight_pass(0, FAR)
    weight_pass(0, PFAR)

    @pl.when(x == 1)
    def _():
        attend(q_ref, own_st, j_xo, 0, rows)

    @pl.when(above0)
    def _():
        attend(q_ref, own_st, j_b, 0, rows)

    carry_ref[0:1, :] = jnp.zeros((1, lw), F32)
    for j in range(SP - 1):

        @pl.when(j < sp)
        def _():
            arrived(ends.at[j], erecv.at[j])
            carry_ref[0:1, :] = ends[j, 0:1, :] * carry_ref[0:1, :] + ends[j, 1:2, :]

    carry = carry_ref[0:1, :]
    for i in range(segs):
        r = slice(i * seg_len, (i + 1) * seg_len)
        g = gate_ref[r, :].astype(F32)
        gelu = 0.5 * g * (1.0 + jnp.tanh(0.7978845608028654 * (g + 0.044715 * (g * g * g))))
        for n in range(lw // 128):
            cs = slice(n * 128, (n + 1) * 128)
            states = local_ref[n, r, :] + prefix_ref[n, r, :] * carry[:, cs]
            br_lru[tp, r, cs] = (states * gelu[:, cs]).astype(BF16)
        if i + 1 < segs:
            carry = seg_a[i : i + 1, :] * carry + seg_b[i : i + 1, :]
    own_lru = br_lru.at[tp]
    send(own_lru, lsend.at[0], lrecv.at[FAR], {"tp": far})
    send(own_lru, lsend.at[0], lrecv.at[PARTNER], {"tp": partner})
    weight_pass(1, FAR)

    @pl.when(above0)
    def _():
        for c in order[0:2]:
            kv_wait(j_bo, c, DIAG)

        @pl.when(helper)
        def _():
            attend(q_far, far_st, j_bo, half, rows)

        for c in order[2:]:
            kv_wait(j_bo, c, DIAG)

        @pl.when(helper)
        def _():
            attend(q_far, far_st, j_bo, 0, half, qc=rc, after=send_partial)

    weight_pass(1, PFAR)

    @pl.when(above0)
    def _():
        attend(q_ref, own_st, j_bo, 0, rows)

    def pair_dot(br, buf, side, r):
        first = 2 * side
        return jnp.dot(br[first, r, :], buf[first], preferred_element_type=F32) + jnp.dot(
            br[first + 1, r, :], buf[first + 1], preferred_element_type=F32
        )

    for c in own_loads:
        c.wait()
    for n in range(2):
        arrived(banks[n][1].at[partner], wrecv_own.at[n])
    arrived(br_lru.at[partner], lrecv.at[PARTNER])
    for c in range(CH):
        oacc[chunk(c), :] = pair_dot(br_lru, wl_buf, y, chunk(c))

    for c in range(CH):
        r = slice(c * rc, (c + 1) * rc)

        @pl.when(helped)
        def _():
            for s in part_copies(c):
                s.wait_recv()
            stats = jnp.concatenate([stat_in[c], jnp.zeros((120, rc), F32)], axis=0).T
            for h in range(H):
                hs = slice(h * HEAD_DIM, (h + 1) * HEAD_DIM)
                m_in = stats[:, h : h + 1]
                l_in = stats[:, H + h : H + h + 1]
                part = part_in[r, hs].astype(F32)
                old = m_ref[h, r, :]
                new = jnp.maximum(old, m_in)
                fade = jnp.exp2(old - new)
                grow = jnp.exp2(m_in - new)
                total = o_ref[h, r, HEAD_DIM:] * fade + l_in * grow
                br_fox[tp, r, hs] = (
                    (o_ref[h, r, 0:HEAD_DIM] * fade + part * grow) / total
                ).astype(BF16)

        @pl.when(jnp.logical_not(helped))
        def _():
            for h in range(H):
                hs = slice(h * HEAD_DIM, (h + 1) * HEAD_DIM)
                br_fox[tp, r, hs] = (o_ref[h, r, 0:HEAD_DIM] / o_ref[h, r, HEAD_DIM:]).astype(BF16)

        ref = br_fox.at[tp, chunk(c)]
        send(ref, fsend.at[0], frecv.at[FAR, c], {"tp": far})
        send(ref, fsend.at[1], frecv.at[PARTNER, c], {"tp": partner})

    arrived(br_lru.at[far], lrecv.at[FAR])
    send(br_lru.at[far], lsend.at[1], lrecv.at[PFAR], {"tp": partner})
    for role in (FAR, PFAR):
        weight_wait(0, role)
        weight_wait(1, role)
    arrived(br_lru.at[pfar], lrecv.at[PFAR])
    for c in range(CH):
        oacc[chunk(c), :] += pair_dot(br_lru, wl_buf, 1 - y, chunk(c))

    def fox_wait(src, role, c):
        arrived(br_fox.at[src, chunk(c)], frecv.at[role, c])

    def fox_pass(c):
        fox_wait(far, FAR, c)
        send(br_fox.at[far, chunk(c)], fsend.at[2], frecv.at[PFAR, c], {"tp": partner})

    fox_pass(0)
    for c in range(CH):
        r = chunk(c)
        if c + 1 < CH:
            fox_pass(c + 1)
        fox_wait(partner, PARTNER, c)
        oacc[r, :] += pair_dot(br_fox, wf_buf, y, r)
        fox_wait(pfar, PFAR, c)
        out[r, :] = (oacc[r, :] + pair_dot(br_fox, wf_buf, 1 - y, r)).astype(out.dtype)

    for k in range(3):
        sent(tok_buf.at[0], tsend.at[k])
        sent(br_fox.at[0], fsend.at[k])
    sent(br_lru.at[pl.ds(0, 2)], lsend.at[0])
    sent(br_lru.at[0], lsend.at[1])
    for k in range(2):
        sent(wl_buf.at[pl.ds(0, 2)], wsend.at[k])

    @pl.when(odd)
    def _():
        for k in range(2, 4):
            sent(wl_buf.at[pl.ds(0, 2)], wsend.at[k])

    sent(own_cum, csend.at[0])
    top_half = pl.ds(0, half)
    need = all_across(x == 0)

    @pl.when(need)
    def _():
        sent(kv_buf.at[0], xsend.at[0])

    @pl.when(jnp.logical_and(goes_up, jnp.logical_not(need)))
    def _():
        sent(kv_buf.at[0, top_half], xsend.at[0])

    @pl.when(goes_up)
    def _():
        sent(kv_buf.at[0, top_half], zfwd.at[0])

    @pl.when(all_over_x)
    def _():
        sent(kv_buf.at[0], xfwd.at[0])

    @pl.when(jnp.logical_and(above0, jnp.logical_not(all_over_x)))
    def _():
        sent(kv_buf.at[0, top_half], xfwd.at[0])

    @pl.when(not_top)
    def _():
        sent(kv_buf.at[0], zsend.at[0])
        sent(cum_buf.at[pl.ds(0, 2)], csend.at[1])

    @pl.when(helped)
    def _():
        sent(q_ref, qsend.at[0])

    @pl.when(helper)
    def _():
        sent(part_out, osend.at[0])
        sent(stat_out, osend.at[1])

    @pl.when(sp < SP - 1)
    def _():
        halo_copy.wait_send()

    for k in range(1, SP):

        @pl.when(sp + k < SP)
        def _():
            end_copy(k).wait_send()


def block_shards(SP, TP, X, *args):
    tokens, lru_in, gate_in, query_w = args[:4]
    (conv_weight, rg_w, ig_w, rate, decay_extra, forget, out_lru, out_fox) = args[6:]
    rows, dcols = tokens.shape
    D, lw = lru_in.shape
    fw = query_w.shape[1]
    oc = out_lru.shape[1] // TP
    tot = 2 * lw + 3 * fw
    H = fw // HEAD_DIM
    CH = 4
    rc = rows // CH
    bw = rg_w.shape[1]
    hbm = pl.BlockSpec(memory_space=pl.ANY)
    dma = pltpu.SemaphoreType.DMA
    V = pltpu.VMEM
    scratch = [
        V((TP, rows, dcols), BF16),
        V((D, tot), BF16),
        V((2, rc, tot), F32),
        V((2, rc, 1), F32),
        V((rows, lw), BF16),
        V((16, lw), BF16),
        V((rows + 8, lw), F32),
        V(conv_weight.shape, BF16),
        V((lw // bw, bw, bw), BF16),
        V((lw // bw, bw, bw), BF16),
        V((1, rate.shape[0]), F32),
        V((H, rows), F32),
        V((lw, lw), BF16),
        V((lw, lw), BF16),
        V((rows, lw), BF16),
        V((rows, fw), BF16),
        V((rows, lw), F32),
        V((lw // 128, rows, 128), F32),
        V((lw // 128, rows, 128), F32),
        V((8, lw), F32),
        V((8, lw), F32),
        V((8, lw), F32),
        V((SP, 8, lw), F32),
        V((SP, rows, 2 * fw), BF16),
        V((SP, 8, rows), F32),
        V((H, rows, 128), F32),
        V((H, rows, 2 * HEAD_DIM), F32),
        V((rows, fw), BF16),
        V((H, rows, 128), F32),
        V((H, rows, 2 * HEAD_DIM), F32),
        V((rows, fw), BF16),
        V((CH, 8, rc), F32),
        V((rows, fw), BF16),
        V((CH, 8, rc), F32),
        V((TP, lw, oc), BF16),
        V((TP, fw, oc), BF16),
        V((TP, rows, lw), BF16),
        V((TP, rows, fw), BF16),
        V((rows, oc), F32),
        dma((CH + 9,)),
        dma((3,)),
        dma((3, CH)),
        dma((1,)),
        dma((1,)),
        dma((SP - 1,)),
        dma((SP - 1,)),
        dma((2,)),
        dma((3,)),
        dma((1,)),
        dma((1,)),
        dma((1,)),
        dma((1,)),
        dma((3, CH)),
        dma((4,)),
        dma((2,)),
        dma((2, 2, X)),
        dma((2,)),
        dma((3,)),
        dma((3,)),
        dma((3, CH)),
        dma((1,)),
        dma((1,)),
        dma((2,)),
        dma((CH, 2)),
    ]
    return pl.pallas_call(
        functools.partial(block_kernel, SP, TP, X, CH),
        out_shape=pltpu.VMEM((rows, oc), BF16),
        in_specs=[hbm] * 14,
        out_specs=pl.BlockSpec(memory_space=pltpu.VMEM),
        scratch_shapes=scratch,
        compiler_params=pltpu.CompilerParams(
            collective_id=1, has_side_effects=True, vmem_limit_bytes=60 * 1024 * 1024
        ),
    )(*args[:9], rate.reshape(1, -1), decay_extra, forget.T, out_lru, out_fox)


def columns_of(mesh):
    SP = mesh.shape["sp"]
    try:
        X = len({d.coords[0] for d in mesh.devices.flat})
    except AttributeError:
        X = 2
    return X if SP % X == 0 else 1


def solution(mesh):
    placed = (
        P("sp", "tp"),
        P(None, "tp"),
        P(None, "tp"),
        P(None, "tp"),
        P(None, "tp"),
        P(None, "tp"),
        P(),
        P(),
        P(),
        P(),
        P("sp", "tp"),
        P("sp", "tp"),
        P("tp", None),
        P("tp", None),
    )
    SP, TP, X = mesh.shape["sp"], mesh.shape["tp"], columns_of(mesh)
    small = X == 2 and TP == 4 and SP // X == 4
    body = functools.partial(block_shards if small else shards, SP, TP, X)
    return jax.shard_map(
        body, mesh=mesh, in_specs=placed, out_specs=P("sp", "tp"), check_vma=False
    )
```

```python
import functools

import jax
import jax.numpy as jnp
from jax import lax
from jax.experimental import pallas as pl
from jax.experimental.pallas import tpu as pltpu
from jax.sharding import PartitionSpec as P

HEAD_DIM = 128
decay_sharpness = 8.0
epsilon_norm = 1e-06
MESH = pl.DeviceIdType.MESH
F32 = jnp.float32
BF16 = jnp.bfloat16


def one_minus_exp(w):
    u = -w
    series = 1.0 - u / 9.0
    for n in range(8, 1, -1):
        series = 1.0 - u / n * series
    return jnp.where(u < 0.5, u * series, 1.0 - jnp.exp(w))


def remote(src, dst, send_sem, recv_sem, device):
    return pltpu.make_async_remote_copy(
        src_ref=src,
        dst_ref=dst,
        send_sem=send_sem,
        recv_sem=recv_sem,
        device_id=device,
        device_id_type=MESH,
    )


def kernel(
    SP,
    TP,
    X,
    tokens,
    lru_in,
    gate_in,
    query_w,
    key_w,
    value_w,
    conv_w,
    rg_w,
    ig_w,
    rate,
    decay_extra,
    forget,
    out_lru,
    out_fox,
    out,
    tok_buf,
    w_buf,
    acc,
    sq,
    lru_ref,
    halo,
    pad,
    bd_r,
    bd_i,
    gate_ref,
    q_ref,
    decay_buf,
    prefix_ref,
    local_ref,
    ends,
    incoming,
    kv_buf,
    cum_buf,
    cum_pad,
    wide,
    fcol,
    m_ref,
    l_ref,
    o_ref,
    q_far,
    m_far,
    l_far,
    o_far,
    part_out,
    stat_out,
    part_in,
    stat_in,
    wl_buf,
    wf_buf,
    br_lru,
    br_fox,
    oacc,
    load_sem,
    tsend,
    tfwd,
    trecv,
    hsend,
    hrecv,
    esend,
    erecv,
    zsend,
    xsend,
    kvrecv,
    wsend,
    wrecv,
    lsend,
    lrecv,
    fsend,
    ffwd,
    frecv,
    lfwd,
    qsend,
    qrecv,
    osend,
    orecv,
):
    rows, dcols = tokens.shape
    D, lw = lru_in.shape
    fw = query_w.shape[1]
    H = fw // HEAD_DIM
    oc = out.shape[1]
    Y = TP // 2
    Z = SP // X
    CH = tsend.shape[1]
    rc = rows // CH
    sp = lax.axis_index("sp")
    tp = lax.axis_index("tp")
    z = lax.div(sp, X)
    x = lax.rem(sp, X)
    partner = tp + 1 - 2 * lax.rem(tp, 2)
    far = [lax.rem(tp + 2 * k, TP) for k in range(Y)]
    pfar = [lax.rem(partner + 2 * k, TP) for k in range(Y)]
    offs = [0, lw, lw + fw, lw + 2 * fw, 2 * lw + 2 * fw, 2 * lw + 3 * fw]

    barrier = pltpu.get_barrier_semaphore()
    for k in range(1, SP):
        pl.semaphore_signal(
            barrier, inc=1, device_id={"sp": lax.rem(sp + k, SP)}, device_id_type=MESH
        )
    for k in range(1, TP):
        pl.semaphore_signal(
            barrier, inc=1, device_id={"tp": lax.rem(tp + k, TP)}, device_id_type=MESH
        )
    loads = []
    for i, w in enumerate((lru_in, key_w, value_w, gate_in, query_w)):
        c = pltpu.make_async_copy(w, w_buf.at[:, offs[i] : offs[i + 1]], load_sem.at[i])
        c.start()
        loads.append(c)
    mine = pl.ds(pl.multiple_of(tp * oc, 128), oc)
    own_loads = [
        pltpu.make_async_copy(decay_extra, decay_buf, load_sem.at[5]),
        pltpu.make_async_copy(out_lru.at[:, mine], wl_buf.at[tp], load_sem.at[6]),
        pltpu.make_async_copy(out_fox.at[:, mine], wf_buf.at[tp], load_sem.at[7]),
    ]
    for c in own_loads:
        c.start()
    pl.semaphore_wait(barrier, SP - 1 + TP - 1)

    pending = []

    def chunk(c):
        return pl.ds(c * rc, rc)

    for c in range(CH):
        for k in range(1, Y):
            s = remote(
                tokens.at[chunk(c)],
                tok_buf.at[tp, chunk(c)],
                tsend.at[k, c],
                trecv.at[tp, c],
                {"tp": far[k]},
            )
            s.start()
            pending.append(s)
    for c in range(CH):
        s = remote(
            tokens.at[chunk(c)],
            tok_buf.at[tp, chunk(c)],
            tsend.at[0, c],
            trecv.at[tp, c],
            {"tp": partner},
        )
        s.start()
        pending.append(s)

    bw = rg_w.shape[1]
    nb = lw // bw
    bd_r[...] = jnp.zeros_like(bd_r)
    bd_i[...] = jnp.zeros_like(bd_i)
    for n in range(nb):
        sl = pl.ds(n * bw, bw)
        bd_r[sl, sl] = rg_w[tp * nb + n]
        bd_i[sl, sl] = ig_w[tp * nb + n]
    cum_pad[...] = jnp.zeros_like(cum_pad)
    wide[...] = jnp.zeros_like(wide)
    wide[0:H, :] = forget[...]
    fcol[...] = wide[...].T
    cum_buf[sp] = wide[0:8, :]

    for c in loads:
        c.wait()

    def project(val, src, r, first=False):
        w_rows = pl.ds(pl.multiple_of(src * dcols, dcols), dcols)
        v32 = val.astype(F32)
        part = jnp.sum(v32 * v32, axis=1, keepdims=True)
        dot = jnp.dot(val, w_buf[w_rows, :], preferred_element_type=F32)
        if first:
            sq[r, :] = part
            acc[r, :] = dot
        else:
            sq[r, :] += part
            acc[r, :] += dot

    def tok_wait(src, c):
        ref = tok_buf.at[src, chunk(c)]
        remote(ref, ref, tsend.at[0, c], trecv.at[src, c], {"tp": partner}).wait_recv()

    for c in range(CH):
        project(tokens[chunk(c), :], tp, chunk(c), True)
    for c in range(CH):
        tok_wait(partner, c)
        project(tok_buf[partner, chunk(c), :], partner, chunk(c))
    for c in range(CH):
        for k in range(1, Y):
            tok_wait(far[k], c)
            ref = tok_buf.at[far[k], chunk(c)]
            s = remote(ref, ref, tfwd.at[k, c], trecv.at[far[k], c], {"tp": partner})
            s.start()
            pending.append(s)
            project(tok_buf[far[k], chunk(c), :], far[k], chunk(c))
        for k in range(1, Y):
            tok_wait(pfar[k], c)
            project(tok_buf[pfar[k], chunk(c), :], pfar[k], chunk(c))

    row_scale = lax.rsqrt(sq[...] / D + epsilon_norm)

    def scaled(i, n=1):
        return (acc[:, offs[i] : offs[i + n]] * row_scale).astype(BF16)

    lru_ref[...] = scaled(0)
    hb = halo.shape[0]
    halo_copy = remote(
        lru_ref.at[pl.ds(rows - hb, hb)],
        halo,
        hsend.at[0],
        hrecv.at[0],
        {"sp": lax.rem(sp + 1, SP)},
    )

    @pl.when(sp < SP - 1)
    def _():
        halo_copy.start()

    kv_buf[sp] = scaled(1, 2)

    paired = Z in (3, 4)
    helper = jnp.logical_and(z <= Z - 3, paired)
    helped = jnp.logical_and(z >= 2, paired)

    def block_copies(j, a, send_sem, device):
        return (
            remote(kv_buf.at[j], kv_buf.at[j], send_sem.at[a, 0], kvrecv.at[j, 0], device),
            remote(cum_buf.at[j], cum_buf.at[j], send_sem.at[a, 1], kvrecv.at[j, 1], device),
        )

    def z_copies(dz):
        j = (z - dz) * X + x
        return block_copies(j, dz, zsend, {"sp": lax.rem(sp + X, SP)})

    def x_copies(dz, dx):
        j = (z - dz) * X + x
        xo = lax.rem(x + dx, X)
        return block_copies(j, dz, xsend.at[dx - 1], {"sp": z * X + xo})

    def for_sends(dz, own, act):
        if own or not paired:

            @pl.when(z < Z - 1)
            def _():
                for c in z_copies(dz):
                    act(c)

        for dx in range(1, X):
            if own:

                @pl.when(jnp.logical_or(lax.rem(x + dx, X) > x, helper))
                def _():
                    for c in x_copies(dz, dx):
                        act(c)
            else:
                for c in x_copies(dz, dx):
                    act(c)

    def kv_wait(j):
        for c in block_copies(j, 0, zsend, {"sp": lax.rem(sp + X, SP)}):
            c.wait_recv()

    for_sends(0, True, lambda c: c.start())

    q_ref[...] = scaled(4)
    q_copy = remote(
        q_ref, q_far, qsend.at[0], qrecv.at[0], {"sp": lax.rem(sp + SP - 2 * X, SP)}
    )

    @pl.when(helped)
    def _():
        q_copy.start()

    for i, (w, buf) in enumerate(((out_lru, wl_buf), (out_fox, wf_buf))):
        for k in range(1, TP):
            t = lax.rem(tp + k, TP)
            cols = pl.ds(pl.multiple_of(t * oc, 128), oc)
            s = remote(w.at[:, cols], buf.at[tp], wsend.at[i, k], wrecv.at[i, tp], {"tp": t})
            s.start()
            pending.append(s)

    gate_ref[...] = scaled(3)

    @pl.when(sp == 0)
    def _():
        pad[0:8, :] = jnp.zeros((8, lw), F32)

    @pl.when(sp > 0)
    def _():
        halo_copy.wait_recv()
        pad[0:8, :] = halo[...].astype(F32)[hb - 8 : hb, :]

    pad[8 : 8 + rows, :] = lru_ref[...].astype(F32)
    chans = pl.ds(pl.multiple_of(tp * lw, 128), lw)
    taps = conv_w.shape[0]
    taps_f32 = conv_w[:, chans].astype(F32)
    conv = jnp.zeros((rows, lw), F32)
    for j in range(taps):
        conv = conv + taps_f32[j : j + 1, :] * pad[8 - (taps - 1) + j : 8 - (taps - 1) + j + rows, :]
    conv_b = conv.astype(BF16)

    def sigmoid(v):
        return 1.0 / (1.0 + jnp.exp(-v))

    recur_gate = sigmoid(jnp.dot(conv_b, bd_r[...], preferred_element_type=F32))
    input_gate = sigmoid(jnp.dot(conv_b, bd_i[...], preferred_element_type=F32))
    own_rate = rate[:, chans]
    softplus = jnp.maximum(-own_rate, 0.0) + jnp.log1p(jnp.exp(-jnp.abs(own_rate)))
    for c in own_loads:
        c.wait()
    log_decay = -decay_sharpness * softplus * recur_gate + decay_buf[...]
    prefix_ref[...] = jnp.exp(log_decay)
    local_ref[...] = jnp.sqrt(one_minus_exp(2.0 * log_decay)) * input_gate * conv_b.astype(F32)
    row_id = lax.broadcasted_iota(jnp.int32, (rows, lw), 0)
    step = 1
    while step < rows:
        a = prefix_ref[...]
        b = local_ref[...]
        keep = row_id >= step
        a_prev = jnp.where(keep, pltpu.roll(a, step, 0), 1.0)
        b_prev = jnp.where(keep, pltpu.roll(b, step, 0), 0.0)
        local_ref[...] = b + a * b_prev
        prefix_ref[...] = a * a_prev
        step *= 2
    ends[sp, 0:1, :] = prefix_ref[rows - 1 : rows, :]
    ends[sp, 1:2, :] = local_ref[rows - 1 : rows, :]

    def end_copy(k):
        return remote(
            ends.at[sp], ends.at[sp], esend.at[k], erecv.at[sp], {"sp": lax.rem(sp + k, SP)}
        )

    for k in range(1, SP):

        @pl.when(sp + k < SP)
        def _():
            end_copy(k).start()

    score_scale = HEAD_DIM ** (-0.5)
    qc = rows // 2

    def attend(j, diagonal, far_first=None):
        other = far_first is not None
        first = diagonal or far_first
        qs, ms, ls, os = (q_far, m_far, l_far, o_far) if other else (q_ref, m_ref, l_ref, o_ref)

        def some(i, carry):
            r = pl.ds(pl.multiple_of(i * qc, qc), qc)
            for h in range(H):
                hs = slice(h * HEAD_DIM, (h + 1) * HEAD_DIM)
                vs = slice(fw + h * HEAD_DIM, fw + (h + 1) * HEAD_DIM)
                s = lax.dot_general(
                    qs[r, hs],
                    kv_buf[j, :, hs],
                    (((1,), (1,)), ((), ())),
                    preferred_element_type=F32,
                )
                s = s * score_scale
                if not other:
                    s = s + fcol[r, h : h + 1]
                s = s - cum_buf[j, h : h + 1, :]
                if diagonal:
                    causal = (
                        lax.broadcasted_iota(jnp.int32, (qc, rows), 0) + i * qc
                        >= lax.broadcasted_iota(jnp.int32, (qc, rows), 1)
                    )
                    s = jnp.where(causal, s, -1e30)
                top = jnp.max(s, axis=1, keepdims=True)
                if first:
                    p = jnp.exp(s - top)
                    ms[h, r, :] = top
                    ls[h, r, :] = jnp.sum(p, axis=1, keepdims=True)
                    os[h, r, :] = jnp.dot(
                        p.astype(BF16), kv_buf[j, :, vs], preferred_element_type=F32
                    )
                else:
                    old = ms[h, r, :]
                    new = jnp.maximum(old, top)
                    p = jnp.exp(s - new)
                    fade = jnp.exp(old - new)
                    ms[h, r, :] = new
                    ls[h, r, :] = ls[h, r, :] * fade + jnp.sum(p, axis=1, keepdims=True)
                    os[h, r, :] = os[h, r, :] * fade + jnp.dot(
                        p.astype(BF16), kv_buf[j, :, vs], preferred_element_type=F32
                    )
            return carry

        lax.fori_loop(0, rows // qc, some, 0)

    attend(sp, True)

    def row_blocks(dz):
        for dx in range(1, X):
            xo = lax.rem(x + dx, X)

            @pl.when(jnp.logical_or(dz > 0, xo < x))
            def _():
                j = (z - dz) * X + xo
                kv_wait(j)
                attend(j, False)

    def finish_lru():
        incoming[...] = jnp.zeros_like(incoming)
        for j in range(SP - 1):

            @pl.when(j < sp)
            def _():
                remote(
                    ends.at[j], ends.at[j], esend.at[0], erecv.at[j], {"sp": lax.rem(sp + 1, SP)}
                ).wait_recv()
                incoming[...] = ends[j, 0:1, :] * incoming[...] + ends[j, 1:2, :]

        states = local_ref[...] + prefix_ref[...] * incoming[...]
        g = gate_ref[...].astype(F32)
        gelu = 0.5 * g * (1.0 + jnp.tanh(0.7978845608028654 * (g + 0.044715 * (g * g * g))))
        br_lru[tp] = (states * gelu).astype(BF16)
        for k in range(Y - 1, -1, -1):
            lru_copy(k).start()

    def lru_copy(k):
        to = far[k] if k else partner
        return remote(br_lru.at[tp], br_lru.at[tp], lsend.at[k], lrecv.at[tp], {"tp": to})

    lru_step = min(2, Z - 1)
    if Z == 1:
        finish_lru()

    def hop(dz, carry):
        @pl.when(dz <= z)
        def _():
            j = (z - dz) * X + x
            kv_wait(j)
            for_sends(dz, False, lambda c: c.start())
            row_blocks(dz - 1)
            attend(j, False)

        @pl.when(dz == lru_step)
        def _():
            finish_lru()

        return carry

    up = {"sp": lax.rem(sp + 2 * X, SP)}
    part_copies = (
        remote(part_out, part_in, osend.at[0], orecv.at[0], up),
        remote(stat_out, stat_in, osend.at[1], orecv.at[1], up),
    )

    def send_partial():
        for h in range(H):
            part_out[:, h * HEAD_DIM : (h + 1) * HEAD_DIM] = o_far[h].astype(BF16)
            cum_pad[:, h : h + 1] = m_far[h]
            cum_pad[:, H + h : H + h + 1] = l_far[h]
        stat_out[...] = cum_pad[...].T[0:8, :]
        for c in part_copies:
            c.start()

    if paired:
        below = (z - 1) * X

        @pl.when(helper)
        def _():
            q_copy.wait_recv()
            attend(sp, False, True)

        @pl.when(z >= 1)
        def _():
            kv_wait(below + x)
            for_sends(1, False, lambda c: c.start())

        for dx in range(1, X):
            xo = lax.rem(x + dx, X)

            @pl.when(jnp.logical_or(xo < x, helper))
            def _():
                kv_wait(z * X + xo)

            @pl.when(helper)
            def _():
                attend(z * X + xo, False, False)

        @pl.when(jnp.logical_and(helper, z == 0))
        def _():
            send_partial()

        for dx in range(1, X):
            xo = lax.rem(x + dx, X)

            @pl.when(xo < x)
            def _():
                attend(z * X + xo, False)

        finish_lru()

        @pl.when(jnp.logical_and(helper, z >= 1))
        def _():
            attend(below + x, False, False)

        @pl.when(z >= 1)
        def _():
            attend(below + x, False)
            for dx in range(1, X):
                j = below + lax.rem(x + dx, X)
                kv_wait(j)

                @pl.when(helper)
                def _():
                    attend(j, False, False)

            @pl.when(helper)
            def _():
                send_partial()

            for dx in range(1, X):
                attend(below + lax.rem(x + dx, X), False)

    else:
        lax.fori_loop(1, Z, hop, 0)

    def lru_wait(t):
        remote(br_lru.at[t], br_lru.at[t], lsend.at[0], lrecv.at[t], {"tp": partner}).wait_recv()

    def lru_dot(t):
        return jnp.dot(br_lru[t], wl_buf[t], preferred_element_type=F32)

    oacc[...] = lru_dot(tp)
    for k in range(1, TP):
        t = lax.rem(tp + k, TP)
        for i, buf in enumerate((wl_buf, wf_buf)):
            remote(buf.at[t], buf.at[t], wsend.at[i, k], wrecv.at[i, t], {"tp": t}).wait_recv()
    for k in range(1, Y):
        lru_wait(far[k])
        ref = br_lru.at[far[k]]
        s = remote(ref, ref, lfwd.at[k], lrecv.at[far[k]], {"tp": partner})
        s.start()
        pending.append(s)
    lru_wait(partner)
    oacc[...] += lru_dot(partner)
    for k in range(1, Y):
        oacc[...] += lru_dot(far[k])
        lru_wait(pfar[k])
        oacc[...] += lru_dot(pfar[k])

    if paired:

        @pl.when(helped)
        def _():
            for c in part_copies:
                c.wait_recv()
            wide[0:8, :] = stat_in[...]
            stats = wide[...].T
            for h in range(H):
                m_in = stats[:, h : h + 1] + fcol[:, h : h + 1]
                l_in = stats[:, H + h : H + h + 1]
                part = part_in[:, h * HEAD_DIM : (h + 1) * HEAD_DIM].astype(F32)
                new = jnp.maximum(m_ref[h], m_in)
                fade = jnp.exp(m_ref[h] - new)
                grow = jnp.exp(m_in - new)
                l_ref[h] = l_ref[h] * fade + l_in * grow
                o_ref[h] = o_ref[h] * fade + part * grow

    else:
        row_blocks(z)

    for c in range(CH):
        r = chunk(c)
        for h in range(H):
            br_fox[tp, r, h * HEAD_DIM : (h + 1) * HEAD_DIM] = (
                o_ref[h, r, :] / l_ref[h, r, :]
            ).astype(BF16)
        ref = br_fox.at[tp, r]
        for k in list(range(1, Y)) + [0]:
            to = far[k] if k else partner
            s = remote(ref, ref, fsend.at[k, c], frecv.at[tp, c], {"tp": to})
            s.start()
            pending.append(s)

    def fox_wait(src, c):
        ref = br_fox.at[src, chunk(c)]
        remote(ref, ref, fsend.at[0, c], frecv.at[src, c], {"tp": partner}).wait_recv()

    def fox_dot(src, r):
        return jnp.dot(br_fox[src, r, :], wf_buf[src], preferred_element_type=F32)

    for c in range(CH):
        fox_wait(partner, c)
        oacc[chunk(c), :] += fox_dot(tp, chunk(c)) + fox_dot(partner, chunk(c))
    for c in range(CH):
        r = chunk(c)
        for k in range(1, Y):
            fox_wait(far[k], c)
            ref = br_fox.at[far[k], r]
            s = remote(ref, ref, ffwd.at[k, c], frecv.at[far[k], c], {"tp": partner})
            s.start()
            pending.append(s)
            oacc[r, :] += fox_dot(far[k], r)
        for k in range(1, Y):
            fox_wait(pfar[k], c)
            oacc[r, :] += fox_dot(pfar[k], r)
        out[r, :] = oacc[r, :].astype(out.dtype)

    for s in pending:
        s.wait_send()
    for k in range(Y):
        lru_copy(k).wait_send()

    @pl.when(helped)
    def _():
        q_copy.wait_send()

    @pl.when(helper)
    def _():
        for c in part_copies:
            c.wait_send()

    @pl.when(sp < SP - 1)
    def _():
        halo_copy.wait_send()

    for k in range(1, SP):

        @pl.when(sp + k < SP)
        def _():
            end_copy(k).wait_send()

    for_sends(0, True, lambda c: c.wait_send())

    def drain(dz, carry):
        @pl.when(dz <= z)
        def _():
            for_sends(dz, False, lambda c: c.wait_send())

        return carry

    if paired:

        @pl.when(z >= 1)
        def _():
            for_sends(1, False, lambda c: c.wait_send())

    else:
        lax.fori_loop(1, Z, drain, 0)


def shards(SP, TP, X, *args):
    tokens, lru_in, gate_in, query_w = args[:4]
    (conv_weight, rg_w, ig_w, rate, decay_extra, forget, out_lru, out_fox) = args[6:]
    rows, dcols = tokens.shape
    D, lw = lru_in.shape
    fw = query_w.shape[1]
    oc = out_lru.shape[1] // TP
    tot = 2 * lw + 3 * fw
    H = fw // HEAD_DIM
    Y = TP // 2
    Z = SP // X
    CH = 4
    vm = pl.BlockSpec(memory_space=pltpu.VMEM)
    hbm = pl.BlockSpec(memory_space=pl.ANY)
    dma = pltpu.SemaphoreType.DMA
    V = pltpu.VMEM
    scratch = [
        V((TP, rows, dcols), BF16),
        V((D, tot), BF16),
        V((rows, tot), F32),
        V((rows, 1), F32),
        V((rows, lw), BF16),
        V((16, lw), BF16),
        V((rows + 8, lw), F32),
        V((lw, lw), BF16),
        V((lw, lw), BF16),
        V((rows, lw), BF16),
        V((rows, fw), BF16),
        V((rows, lw), F32),
        V((rows, lw), F32),
        V((rows, lw), F32),
        V((SP, 8, lw), F32),
        V((1, lw), F32),
        V((SP, rows, 2 * fw), BF16),
        V((SP, 8, rows), F32),
        V((rows, 128), F32),
        V((128, rows), F32),
        V((rows, 128), F32),
        V((H, rows, 1), F32),
        V((H, rows, 1), F32),
        V((H, rows, HEAD_DIM), F32),
        V((rows, fw), BF16),
        V((H, rows, 1), F32),
        V((H, rows, 1), F32),
        V((H, rows, HEAD_DIM), F32),
        V((rows, fw), BF16),
        V((8, rows), F32),
        V((rows, fw), BF16),
        V((8, rows), F32),
        V((TP, lw, oc), BF16),
        V((TP, fw, oc), BF16),
        V((TP, rows, lw), BF16),
        V((TP, rows, fw), BF16),
        V((rows, oc), F32),
        dma((8,)),
        dma((Y, CH)),
        dma((Y, CH)),
        dma((TP, CH)),
        dma((1,)),
        dma((1,)),
        dma((SP,)),
        dma((SP,)),
        dma((Z, 2)),
        dma((max(X - 1, 1), Z, 2)),
        dma((SP, 2)),
        dma((2, TP)),
        dma((2, TP)),
        dma((TP,)),
        dma((TP,)),
        dma((Y, CH)),
        dma((Y, CH)),
        dma((TP, CH)),
        dma((Y,)),
        dma((1,)),
        dma((1,)),
        dma((2,)),
        dma((2,)),
    ]
    return pl.pallas_call(
        functools.partial(kernel, SP, TP, X),
        out_shape=jax.ShapeDtypeStruct((rows, oc), BF16),
        in_specs=[vm] + [hbm] * 5 + [vm] * 4 + [hbm, vm, hbm, hbm],
        out_specs=vm,
        scratch_shapes=scratch,
        compiler_params=pltpu.CompilerParams(
            collective_id=0, has_side_effects=True, vmem_limit_bytes=60 * 1024 * 1024
        ),
    )(*args[:9], rate.reshape(1, -1), decay_extra, forget.T, out_lru, out_fox)


LOG2E = 1.4426950408889634


def block_kernel(
    SP,
    TP,
    X,
    CH,
    tokens,
    lru_in,
    gate_in,
    query_w,
    key_w,
    value_w,
    conv_w,
    rg_w,
    ig_w,
    rate,
    decay_extra,
    forget,
    out_lru,
    out_fox,
    out,
    tok_buf,
    w_buf,
    acc,
    sq,
    lru_ref,
    halo,
    pad,
    conv_v,
    rg_v,
    ig_v,
    rate_v,
    forget_v,
    bd_r,
    bd_i,
    gate_ref,
    q_ref,
    decay_buf,
    prefix_ref,
    local_ref,
    seg_a,
    seg_b,
    carry_ref,
    ends,
    kv_buf,
    cum_buf,
    m_ref,
    o_ref,
    q_far,
    m_far,
    o_far,
    part_out,
    stat_out,
    part_in,
    stat_in,
    wl_buf,
    wf_buf,
    br_lru,
    br_fox,
    oacc,
    load_sem,
    tsend,
    trecv,
    hsend,
    hrecv,
    esend,
    erecv,
    csend,
    crecv,
    zsend,
    xsend,
    zfwd,
    xfwd,
    kvrecv,
    wsend,
    wrecv_own,
    wrecv,
    lsend,
    lrecv,
    fsend,
    frecv,
    qsend,
    qrecv,
    osend,
    orecv,
):
    rows, dcols = tokens.shape
    D, lw = lru_in.shape
    fw = query_w.shape[1]
    H = fw // HEAD_DIM
    oc = out.shape[1]
    Z = SP // X
    rc = rows // CH
    half = rows // 2
    wh = out_lru.shape[0] // X
    sp = lax.axis_index("sp")
    tp = lax.axis_index("tp")
    z = lax.div(sp, X)
    x = lax.rem(sp, X)
    xo = 1 - x
    y = lax.div(tp, 2)
    partner = tp + 1 - 2 * lax.rem(tp, 2)
    far = lax.rem(tp + 2, TP)
    pfar = lax.rem(partner + 2, TP)
    j_xo = z * X + xo
    to_xo = {"sp": j_xo}
    to_up = {"sp": lax.rem(sp + X, SP)}
    j_b = lax.rem(sp + SP - X, SP)
    j_bo = lax.rem(j_xo + SP - X, SP)
    helper = z <= Z - 3
    helped = z >= 2
    not_top = z < Z - 1
    above0 = z >= 1
    order = list(range(CH - 1, -1, -1))
    second_top = z == Z - 2
    climbs = {order[1]: not_top, order[3]: second_top}
    crosses = {
        order[0]: above0,
        order[2]: above0,
        order[3]: jnp.logical_and(above0, not_top),
    }
    whalf = lax.rem(x + z, X)
    top = z == Z - 1
    first_core = lax.rem(tp, 2) == 0
    PARTNER, FAR, PFAR = 0, 1, 2
    ACROSS, BELOW, DIAG = 0, 1, 2
    score_k = HEAD_DIM ** (-0.5) * LOG2E

    def chunk(c):
        return pl.ds(c * rc, rc)

    barrier = pltpu.get_barrier_semaphore()
    for k in range(1, SP):
        pl.semaphore_signal(
            barrier, inc=1, device_id={"sp": lax.rem(sp + k, SP)}, device_id_type=MESH
        )
    for k in range(1, TP):
        pl.semaphore_signal(
            barrier, inc=1, device_id={"tp": lax.rem(tp + k, TP)}, device_id_type=MESH
        )

    def load(i, src, dst):
        c = pltpu.make_async_copy(src, dst, load_sem.at[i])
        c.start()
        return c

    tok_loads = [
        load(n, tokens.at[chunk(c)], tok_buf.at[tp, chunk(c)]) for n, c in enumerate(order)
    ]
    cols = (0, fw, 2 * fw, 2 * fw + lw, 3 * fw + lw, 3 * fw + 2 * lw)
    for i, w in enumerate((key_w, value_w, lru_in, query_w, gate_in)):
        load(CH, w, w_buf.at[:, cols[i] : cols[i + 1]])
    mine = pl.ds(pl.multiple_of(tp * oc, 128), oc)
    bw = rg_w.shape[1]
    nb = lw // bw
    gates = pl.ds(tp * nb, nb)
    forget_load = load(CH + 1, forget, forget_v)
    small_loads = [
        load(CH + 2, conv_w, conv_v),
        load(CH + 3, rg_w.at[gates], rg_v),
        load(CH + 4, ig_w.at[gates], ig_v),
        load(CH + 5, rate, rate_v),
        load(CH + 6, decay_extra, decay_buf),
    ]
    own_loads = [
        load(CH + 7, out_lru.at[:, mine], wl_buf.at[tp]),
        load(CH + 8, out_fox.at[:, mine], wf_buf.at[tp]),
    ]
    pl.semaphore_wait(barrier, SP - 1 + TP - 1)

    def send(ref, send_sem, recv_sem, device):
        remote(ref, ref, send_sem, recv_sem, device).start()

    def arrived(ref, recv_sem):
        remote(ref, ref, recv_sem, recv_sem, to_xo).wait_recv()

    def sent(ref, send_sem):
        remote(ref, ref, send_sem, send_sem, to_xo).wait_send()

    for n, c in enumerate(order):
        tok_loads[n].wait()
        ref = tok_buf.at[tp, chunk(c)]
        send(ref, tsend.at[0], trecv.at[FAR, c], {"tp": far})
        send(ref, tsend.at[1], trecv.at[PARTNER, c], {"tp": partner})

    forget_load.wait()
    cum_buf[sp] = forget_v[...] * LOG2E
    own_cum = cum_buf.at[sp]
    send(own_cum, csend.at[0], crecv.at[ACROSS], to_xo)

    @pl.when(not_top)
    def _():
        send(own_cum, csend.at[1], crecv.at[BELOW], to_up)
        send(own_cum, csend.at[1], crecv.at[DIAG], {"sp": lax.rem(j_xo + X, SP)})

    for c in small_loads:
        c.wait()
    bd_r[...] = jnp.zeros_like(bd_r)
    bd_i[...] = jnp.zeros_like(bd_i)
    for n in range(nb):
        sl = pl.ds(n * bw, bw)
        bd_r[sl, sl] = rg_v[n]
        bd_i[sl, sl] = ig_v[n]
    pltpu.make_async_copy(w_buf, w_buf, load_sem.at[CH]).wait()

    def tok_wait(src, role, c):
        arrived(tok_buf.at[src, chunk(c)], trecv.at[role, c])

    def features(side, c):
        first = 2 * side
        return jnp.concatenate([tok_buf[first, chunk(c), :], tok_buf[first + 1, chunk(c), :]], axis=1)

    def w_rows(side):
        return pl.ds(pl.multiple_of(side * 2 * dcols, 2 * dcols), 2 * dcols)

    def squares(v):
        v32 = v.astype(F32)
        return jnp.sum(v32 * v32, axis=1, keepdims=True)

    def near_part(c, slot):
        tok_wait(partner, PARTNER, c)
        v = features(y, c)
        sq[slot] = squares(v)
        acc[slot] = jnp.dot(v, w_buf[w_rows(y), :], preferred_element_type=F32)

    halo_copy = remote(
        lru_ref.at[pl.ds(rows - halo.shape[0], halo.shape[0])],
        halo,
        hsend.at[0],
        hrecv.at[0],
        {"sp": lax.rem(sp + 1, SP)},
    )

    def kv_send(j, c, send_sem, role, device):
        send(kv_buf.at[j, chunk(c)], send_sem.at[0], kvrecv.at[role, c], device)

    def kv_wait(j, c, role):
        arrived(kv_buf.at[j, chunk(c)], kvrecv.at[role, c])

    def all_across(own_x):
        return jnp.logical_or(own_x, helper)

    def across(own_x, c):
        need = all_across(own_x)
        return jnp.logical_or(need, climbs[c]) if c in climbs else need

    def q_copy(c):
        return remote(
            q_ref.at[chunk(c)],
            q_far.at[chunk(c)],
            qsend.at[0],
            qrecv.at[0 if c in order[0:2] else 1],
            {"sp": lax.rem(sp + SP - 2 * X, SP)},
        )

    def far_part(i, c, slot):
        tok_wait(far, FAR, c)
        send(tok_buf.at[far, chunk(c)], tsend.at[2], trecv.at[PFAR, c], {"tp": partner})
        if i + 1 < CH:
            near_part(order[i + 1], 1 - slot)
        tok_wait(pfar, PFAR, c)
        if i == CH - 1:
            send_weights()
        v = features(1 - y, c)
        row_scale = lax.rsqrt((sq[slot] + squares(v)) / D + epsilon_norm)

        def part(a, b):
            w = w_buf[w_rows(1 - y), cols[a] : cols[b]]
            both = acc[slot, :, cols[a] : cols[b]] + jnp.dot(v, w, preferred_element_type=F32)
            return (both * row_scale).astype(BF16)

        kv_buf[sp, chunk(c), :] = part(0, 2)

        @pl.when(across(x == 0, c))
        def _():
            kv_send(sp, c, xsend, ACROSS, to_xo)

        @pl.when(not_top)
        def _():
            kv_send(sp, c, zsend, BELOW, to_up)

        rest = part(2, 5)
        lru_ref[chunk(c), :] = rest[:, 0:lw]
        q_ref[chunk(c), :] = rest[:, lw : lw + fw]
        gate_ref[chunk(c), :] = rest[:, lw + fw :]

        @pl.when(helped)
        def _():
            q_copy(c).start()

        if i == 0:

            @pl.when(sp < SP - 1)
            def _():
                halo_copy.start()

    banks = ((out_lru, wl_buf), (out_fox, wf_buf))

    def send_weights():
        r = pl.ds(pl.multiple_of(whalf * wh, wh), wh)

        def over_y(n):
            w, buf = banks[n]
            for role, t in ((FAR, far), (PFAR, pfar)):
                c = pl.ds(pl.multiple_of(t * oc, 128), oc)
                remote(
                    w.at[r, c], buf.at[tp, r], wsend.at[n], wrecv.at[n, role - 1, whalf], {"tp": t}
                ).start()

        pl.when(above0)(lambda: over_y(0))
        over_y(1)
        c = pl.ds(pl.multiple_of(partner * oc, 128), oc)
        for n, (w, buf) in enumerate(banks):
            remote(w.at[:, c], buf.at[tp], wsend.at[2], wrecv_own.at[n], {"tp": partner}).start()

    def weight_part(n, role, k):
        t = far if role == FAR else pfar
        ref = banks[n][1].at[t, pl.ds(pl.multiple_of(k * wh, wh), wh)]
        return ref, wrecv.at[n, role - 1, k]

    def weight_pass(n, role):
        ref, sem = weight_part(n, role, whalf)

        def take():
            arrived(ref, sem)

        if n == 0:
            pl.when(above0)(take)
        else:
            take()

        @pl.when(above0)
        def _():
            send(ref, wsend.at[3], sem, {"sp": lax.rem(sp + SP - X, SP)})

        @pl.when(top)
        def _():
            send(ref, wsend.at[4], sem, to_xo)

    def weight_pass_bottom(role):
        @pl.when(z == 0)
        def _():
            ref, sem = weight_part(0, role, 1 - whalf)
            arrived(ref, sem)
            send(ref, wsend.at[4], sem, to_xo)

    def weight_wait(n, role):
        k = 1 - whalf
        if n == 0:
            k = jnp.where(z == 0, whalf, k)
        arrived(*weight_part(n, role, k))

    def pass_up(c):
        @pl.when(climbs[c])
        def _():
            kv_wait(j_xo, c, ACROSS)
            kv_send(j_xo, c, zfwd, DIAG, to_up)

    def pass_across(c):
        @pl.when(crosses[c])
        def _():
            kv_wait(j_b, c, BELOW)
            kv_send(j_b, c, xfwd, DIAG, to_xo)

    near_part(order[0], 0)
    for i, c in enumerate(order):
        far_part(i, c, i % 2)

    pass_across(order[0])
    pass_up(order[1])

    @pl.when(sp == 0)
    def _():
        pad[0:8, :] = jnp.zeros((8, lw), F32)

    @pl.when(sp > 0)
    def _():
        halo_copy.wait_recv()
        hb = halo.shape[0]
        pad[0:8, :] = halo[...].astype(F32)[hb - 8 : hb, :]

    pad[8 : 8 + rows, :] = lru_ref[...].astype(F32)
    chans = pl.ds(pl.multiple_of(tp * lw, 128), lw)
    taps = conv_w.shape[0]
    taps_f32 = conv_v[:, chans].astype(F32)
    conv = jnp.zeros((rows, lw), F32)
    for j in range(taps):
        conv = conv + taps_f32[j : j + 1, :] * pad[8 - (taps - 1) + j : 8 - (taps - 1) + j + rows, :]
    conv_b = conv.astype(BF16)

    def sigmoid(v):
        return 1.0 / (1.0 + jnp.exp(-v))

    recur_gate = sigmoid(jnp.dot(conv_b, bd_r[...], preferred_element_type=F32))
    input_gate = sigmoid(jnp.dot(conv_b, bd_i[...], preferred_element_type=F32))
    own_rate = rate_v[:, chans]
    softplus = jnp.maximum(-own_rate, 0.0) + jnp.log1p(jnp.exp(-jnp.abs(own_rate)))
    log_decay = -decay_sharpness * softplus * recur_gate + decay_buf[...]
    decay = jnp.exp(log_decay)
    driven = jnp.sqrt(one_minus_exp(2.0 * log_decay)) * input_gate * conv_b.astype(F32)
    for n in range(lw // 128):
        prefix_ref[n] = decay[:, n * 128 : (n + 1) * 128]
        local_ref[n] = driven[:, n * 128 : (n + 1) * 128]

    segs = 8
    seg_len = rows // segs
    run_a = jnp.ones((segs, lw), F32)
    run_b = jnp.zeros((segs, lw), F32)
    for i in range(seg_len):
        at = pl.ds(i, segs, stride=seg_len)
        a = [prefix_ref[n, at, :] for n in range(lw // 128)]
        b = [local_ref[n, at, :] for n in range(lw // 128)]
        a = jnp.concatenate(a, axis=1)
        b = jnp.concatenate(b, axis=1)
        run_a = run_a * a
        run_b = a * run_b + b
        for n in range(lw // 128):
            prefix_ref[n, at, :] = run_a[:, n * 128 : (n + 1) * 128]
            local_ref[n, at, :] = run_b[:, n * 128 : (n + 1) * 128]
    seg_a[...] = run_a
    seg_b[...] = run_b
    end_a = seg_a[0:1, :]
    end_b = seg_b[0:1, :]
    for i in range(1, segs):
        end_b = seg_a[i : i + 1, :] * end_b + seg_b[i : i + 1, :]
        end_a = end_a * seg_a[i : i + 1, :]
    ends[sp, 0:1, :] = end_a
    ends[sp, 1:2, :] = end_b

    def end_copy(k):
        return remote(
            ends.at[sp],
            ends.at[sp],
            esend.at[k - 1],
            erecv.at[lax.rem(sp, SP - 1)],
            {"sp": lax.rem(sp + k, SP)},
        )

    def send_ends(core):
        for k in range(1, SP):

            @pl.when(jnp.logical_and(core, sp + k < SP))
            def _():
                end_copy(k).start()

    send_ends(first_core)
    pass_across(order[2])

    def attend(qs, st, j, lo, hi, first=False, diagonal=False, qc=half, after=None, parts=None):
        ms, os = st
        items = [(i, h) for i in (parts or range(rows // qc)) for h in range(H)]

        def width(i):
            return (lo, (i + 1) * qc) if diagonal else (lo, hi)

        def scores(i, h):
            a, b = width(i)
            hs = slice(h * HEAD_DIM, (h + 1) * HEAD_DIM)
            s = lax.dot_general(
                qs[i * qc : (i + 1) * qc, hs],
                kv_buf[j, a:b, hs],
                (((1,), (1,)), ((), ())),
                preferred_element_type=F32,
            )
            s = s * score_k - cum_buf[j, h : h + 1, a:b]
            if diagonal:
                causal = (
                    lax.broadcasted_iota(jnp.int32, (qc, b - a), 0) + (i * qc - a)
                    >= lax.broadcasted_iota(jnp.int32, (qc, b - a), 1)
                )
                s = jnp.where(causal, s, -1e30)
            return s

        def update(i, h, s):
            a, b = width(i)
            r = slice(i * qc, (i + 1) * qc)
            top = jnp.max(s, axis=1, keepdims=True)
            if first:
                new = jnp.broadcast_to(top, (qc, 128))
            else:
                old = ms[h, r, :]
                new = jnp.maximum(old, top)
            ms[h, r, :] = new
            p = jnp.exp2(s - jnp.concatenate([new] * ((b - a) // 128), axis=1)).astype(BF16)
            v = kv_buf[j, a:b, fw + h * HEAD_DIM : fw + (h + 1) * HEAD_DIM]
            v1 = jnp.concatenate([v, jnp.ones((b - a, 128), BF16)], axis=1)
            pv = jnp.dot(p, v1, preferred_element_type=F32)
            if first:
                os[h, r, :] = pv
            else:
                fade = jnp.exp2(old - new)
                os[h, r, :] = os[h, r, :] * jnp.concatenate([fade, fade], axis=1) + pv

        s = scores(*items[0])
        for n, (i, h) in enumerate(items):
            nxt = scores(*items[n + 1]) if n + 1 < len(items) else None
            update(i, h, s)
            s = nxt
            if after is not None and h == H - 1:
                after(i)

    own_st = (m_ref, o_ref)
    far_st = (m_far, o_far)
    up2 = {"sp": lax.rem(sp + 2 * X, SP)}

    def part_copies(c):
        return (
            remote(part_out.at[chunk(c)], part_in.at[chunk(c)], osend.at[0], orecv.at[c, 0], up2),
            remote(stat_out.at[c], stat_in.at[c], osend.at[1], orecv.at[c, 1], up2),
        )

    def send_partial(c):
        r = slice(c * rc, (c + 1) * rc)
        lane = lax.broadcasted_iota(jnp.int32, (rc, 128), 1)
        stats = jnp.zeros((rc, 128), F32)
        for h in range(H):
            part_out[r, h * HEAD_DIM : (h + 1) * HEAD_DIM] = o_far[h, r, 0:HEAD_DIM].astype(BF16)
            stats = jnp.where(lane == h, m_far[h, r, :], stats)
            stats = jnp.where(lane == H + h, o_far[h, r, HEAD_DIM:], stats)
        stat_out[c] = stats.T[0 : 2 * H, :]
        part, stat = part_copies(c)

        @pl.when(first_core)
        def _():
            stat.start()

        part.start()

        @pl.when(jnp.logical_not(first_core))
        def _():
            stat.start()

    attend(q_ref, own_st, sp, 0, rows, True, True)

    @pl.when(helper)
    def _():
        arrived(q_far.at[pl.ds(half, half)], qrecv.at[0])
        attend(q_far, far_st, sp, 0, rows, True, parts=(1,))

    pass_up(order[3])
    pass_across(order[3])
    send_ends(jnp.logical_not(first_core))

    weight_pass(0, FAR)
    arrived(cum_buf.at[j_xo], crecv.at[ACROSS])

    @pl.when(helper)
    def _():
        arrived(q_far.at[pl.ds(0, half)], qrecv.at[1])
        attend(q_far, far_st, sp, 0, rows, True, parts=(0,))

    for c in order:
        need = all_across(x == 1)
        if c in climbs:
            need = jnp.logical_and(need, jnp.logical_not(climbs[c]))

        @pl.when(need)
        def _():
            kv_wait(j_xo, c, ACROSS)

    @pl.when(jnp.logical_and(helper, z == 0))
    def _():
        attend(q_far, far_st, j_xo, 0, rows, qc=rc, after=send_partial)

    @pl.when(jnp.logical_and(helper, above0))
    def _():
        attend(q_far, far_st, j_xo, 0, rows)

    weight_pass(0, PFAR)

    @pl.when(above0)
    def _():
        for c in climbs:

            @pl.when(jnp.logical_not(crosses.get(c, False)))
            def _():
                kv_wait(j_b, c, BELOW)

        arrived(cum_buf.at[j_b], crecv.at[BELOW])
        arrived(cum_buf.at[j_bo], crecv.at[DIAG])

    @pl.when(jnp.logical_and(helper, above0))
    def _():
        attend(q_far, far_st, j_b, 0, rows)

    @pl.when(above0)
    def _():
        attend(q_ref, own_st, j_b, 0, rows)

    weight_pass(1, FAR)

    @pl.when(jnp.logical_and(helper, above0))
    def _():
        for c in order[0:2]:
            kv_wait(j_bo, c, DIAG)
        attend(q_far, far_st, j_bo, half, rows)

    @pl.when(x == 1)
    def _():
        attend(q_ref, own_st, j_xo, 0, rows)

    carry_ref[0:1, :] = jnp.zeros((1, lw), F32)
    for j in range(SP - 1):

        @pl.when(j < sp)
        def _():
            arrived(ends.at[j], erecv.at[j])
            carry_ref[0:1, :] = ends[j, 0:1, :] * carry_ref[0:1, :] + ends[j, 1:2, :]

    carry = carry_ref[0:1, :]
    for i in range(segs):
        r = slice(i * seg_len, (i + 1) * seg_len)
        g = gate_ref[r, :].astype(F32)
        gelu = 0.5 * g * (1.0 + jnp.tanh(0.7978845608028654 * (g + 0.044715 * (g * g * g))))
        for n in range(lw // 128):
            cs = slice(n * 128, (n + 1) * 128)
            states = local_ref[n, r, :] + prefix_ref[n, r, :] * carry[:, cs]
            br_lru[tp, r, cs] = (states * gelu[:, cs]).astype(BF16)
        if i + 1 < segs:
            carry = seg_a[i : i + 1, :] * carry + seg_b[i : i + 1, :]
    own_lru = br_lru.at[tp]
    send(own_lru, lsend.at[0], lrecv.at[FAR], {"tp": far})
    send(own_lru, lsend.at[0], lrecv.at[PARTNER], {"tp": partner})
    weight_pass(1, PFAR)

    upper = jnp.logical_and(above0, jnp.logical_not(helper))
    middle = jnp.logical_and(above0, helper)

    @pl.when(upper)
    def _():
        for c in order[0:2]:
            kv_wait(j_bo, c, DIAG)
        attend(q_ref, own_st, j_bo, half, rows)

    @pl.when(above0)
    def _():
        for c in order[2:]:
            kv_wait(j_bo, c, DIAG)

    @pl.when(middle)
    def _():
        attend(q_far, far_st, j_bo, 0, half, qc=rc, after=send_partial)
        attend(q_ref, own_st, j_bo, 0, rows)

    @pl.when(upper)
    def _():
        attend(q_ref, own_st, j_bo, 0, half)

    def pair_dot(br, buf, side, r):
        first = 2 * side
        return jnp.dot(br[first, r, :], buf[first], preferred_element_type=F32) + jnp.dot(
            br[first + 1, r, :], buf[first + 1], preferred_element_type=F32
        )

    for c in range(CH):
        r = slice(c * rc, (c + 1) * rc)

        @pl.when(helped)
        def _():
            for s in part_copies(c):
                s.wait_recv()
            stats = jnp.concatenate([stat_in[c], jnp.zeros((128 - 2 * H, rc), F32)], axis=0).T
            for h in range(H):
                hs = slice(h * HEAD_DIM, (h + 1) * HEAD_DIM)
                m_in = stats[:, h : h + 1]
                l_in = stats[:, H + h : H + h + 1]
                part = part_in[r, hs].astype(F32)
                old = m_ref[h, r, :]
                new = jnp.maximum(old, m_in)
                fade = jnp.exp2(old - new)
                grow = jnp.exp2(m_in - new)
                total = o_ref[h, r, HEAD_DIM:] * fade + l_in * grow
                br_fox[tp, r, hs] = (
                    (o_ref[h, r, 0:HEAD_DIM] * fade + part * grow) / total
                ).astype(BF16)

        @pl.when(jnp.logical_not(helped))
        def _():
            for h in range(H):
                hs = slice(h * HEAD_DIM, (h + 1) * HEAD_DIM)
                br_fox[tp, r, hs] = (o_ref[h, r, 0:HEAD_DIM] / o_ref[h, r, HEAD_DIM:]).astype(BF16)

        ref = br_fox.at[tp, chunk(c)]
        send(ref, fsend.at[0], frecv.at[FAR, c], {"tp": far})
        send(ref, fsend.at[1], frecv.at[PARTNER, c], {"tp": partner})

    weight_pass_bottom(FAR)
    weight_pass_bottom(PFAR)
    for c in own_loads:
        c.wait()
    for n in range(2):
        arrived(banks[n][1].at[partner], wrecv_own.at[n])
    arrived(br_lru.at[partner], lrecv.at[PARTNER])
    for c in range(CH):
        oacc[chunk(c), :] = pair_dot(br_lru, wl_buf, y, chunk(c))

    arrived(br_lru.at[far], lrecv.at[FAR])
    send(br_lru.at[far], lsend.at[1], lrecv.at[PFAR], {"tp": partner})
    for role in (FAR, PFAR):
        weight_wait(0, role)
        weight_wait(1, role)
    arrived(br_lru.at[pfar], lrecv.at[PFAR])
    for c in range(CH):
        oacc[chunk(c), :] += pair_dot(br_lru, wl_buf, 1 - y, chunk(c))

    def fox_wait(src, role, c):
        arrived(br_fox.at[src, chunk(c)], frecv.at[role, c])

    def fox_pass(c):
        fox_wait(far, FAR, c)
        send(br_fox.at[far, chunk(c)], fsend.at[2], frecv.at[PFAR, c], {"tp": partner})

    fox_pass(0)
    for c in range(CH):
        r = chunk(c)
        if c + 1 < CH:
            fox_pass(c + 1)
        fox_wait(partner, PARTNER, c)
        oacc[r, :] += pair_dot(br_fox, wf_buf, y, r)
        fox_wait(pfar, PFAR, c)
        out[r, :] = (oacc[r, :] + pair_dot(br_fox, wf_buf, 1 - y, r)).astype(out.dtype)

    for k in range(3):
        sent(tok_buf.at[0], tsend.at[k])
        sent(br_fox.at[0], fsend.at[k])
    sent(br_lru.at[pl.ds(0, 2)], lsend.at[0])
    sent(br_lru.at[0], lsend.at[1])
    sent(wl_buf.at[0], wsend.at[1])
    sent(wl_buf.at[pl.ds(0, 2)], wsend.at[2])

    @pl.when(above0)
    def _():
        sent(wl_buf.at[0], wsend.at[0])
        sent(wl_buf.at[pl.ds(0, 2)], wsend.at[3])

    @pl.when(top)
    def _():
        sent(wl_buf.at[pl.ds(0, 2)], wsend.at[4])

    @pl.when(z == 0)
    def _():
        sent(wl_buf.at[0], wsend.at[4])

    sent(own_cum, csend.at[0])
    top_half = pl.ds(0, half)
    need = all_across(x == 0)

    @pl.when(need)
    def _():
        sent(kv_buf.at[0], xsend.at[0])

    @pl.when(jnp.logical_and(second_top, jnp.logical_not(need)))
    def _():
        sent(kv_buf.at[0, top_half], xsend.at[0])

    for level in range(Z):

        @pl.when(z == level)
        def _():
            ups = (level < Z - 1) + (level == Z - 2)
            if ups:
                sent(kv_buf.at[0, pl.ds(0, ups * rc)], zfwd.at[0])
            overs = (2 if level else 0) + (0 < level < Z - 1)
            if overs:
                sent(kv_buf.at[0, pl.ds(0, overs * rc)], xfwd.at[0])

    @pl.when(not_top)
    def _():
        sent(kv_buf.at[0], zsend.at[0])
        sent(cum_buf.at[pl.ds(0, 2)], csend.at[1])

    @pl.when(helped)
    def _():
        sent(q_ref, qsend.at[0])

    @pl.when(helper)
    def _():
        sent(part_out, osend.at[0])
        sent(stat_out, osend.at[1])

    @pl.when(sp < SP - 1)
    def _():
        halo_copy.wait_send()

    for k in range(1, SP):

        @pl.when(sp + k < SP)
        def _():
            end_copy(k).wait_send()


def block_shards(SP, TP, X, *args):
    tokens, lru_in, gate_in, query_w = args[:4]
    (conv_weight, rg_w, ig_w, rate, decay_extra, forget, out_lru, out_fox) = args[6:]
    rows, dcols = tokens.shape
    D, lw = lru_in.shape
    fw = query_w.shape[1]
    oc = out_lru.shape[1] // TP
    tot = 2 * lw + 3 * fw
    H = fw // HEAD_DIM
    CH = 4
    rc = rows // CH
    bw = rg_w.shape[1]
    hbm = pl.BlockSpec(memory_space=pl.ANY)
    dma = pltpu.SemaphoreType.DMA
    V = pltpu.VMEM
    scratch = [
        V((TP, rows, dcols), BF16),
        V((D, tot), BF16),
        V((2, rc, tot), F32),
        V((2, rc, 1), F32),
        V((rows, lw), BF16),
        V((16, lw), BF16),
        V((rows + 8, lw), F32),
        V(conv_weight.shape, BF16),
        V((lw // bw, bw, bw), BF16),
        V((lw // bw, bw, bw), BF16),
        V((1, rate.shape[0]), F32),
        V((H, rows), F32),
        V((lw, lw), BF16),
        V((lw, lw), BF16),
        V((rows, lw), BF16),
        V((rows, fw), BF16),
        V((rows, lw), F32),
        V((lw // 128, rows, 128), F32),
        V((lw // 128, rows, 128), F32),
        V((8, lw), F32),
        V((8, lw), F32),
        V((8, lw), F32),
        V((SP, 2, lw), F32),
        V((SP, rows, 2 * fw), BF16),
        V((SP, H, rows), F32),
        V((H, rows, 128), F32),
        V((H, rows, 2 * HEAD_DIM), F32),
        V((rows, fw), BF16),
        V((H, rows, 128), F32),
        V((H, rows, 2 * HEAD_DIM), F32),
        V((rows, fw), BF16),
        V((CH, 2 * H, rc), F32),
        V((rows, fw), BF16),
        V((CH, 2 * H, rc), F32),
        V((TP, lw, oc), BF16),
        V((TP, fw, oc), BF16),
        V((TP, rows, lw), BF16),
        V((TP, rows, fw), BF16),
        V((rows, oc), F32),
        dma((CH + 9,)),
        dma((3,)),
        dma((3, CH)),
        dma((1,)),
        dma((1,)),
        dma((SP - 1,)),
        dma((SP - 1,)),
        dma((2,)),
        dma((3,)),
        dma((1,)),
        dma((1,)),
        dma((1,)),
        dma((1,)),
        dma((3, CH)),
        dma((5,)),
        dma((2,)),
        dma((2, 2, X)),
        dma((2,)),
        dma((3,)),
        dma((3,)),
        dma((3, CH)),
        dma((1,)),
        dma((2,)),
        dma((2,)),
        dma((CH, 2)),
    ]
    return pl.pallas_call(
        functools.partial(block_kernel, SP, TP, X, CH),
        out_shape=pltpu.VMEM((rows, oc), BF16),
        in_specs=[hbm] * 14,
        out_specs=pl.BlockSpec(memory_space=pltpu.VMEM),
        scratch_shapes=scratch,
        compiler_params=pltpu.CompilerParams(
            collective_id=1, has_side_effects=True, vmem_limit_bytes=60 * 1024 * 1024
        ),
    )(*args[:9], rate.reshape(1, -1), decay_extra, forget.T, out_lru, out_fox)


def columns_of(mesh):
    SP = mesh.shape["sp"]
    try:
        X = len({d.coords[0] for d in mesh.devices.flat})
    except AttributeError:
        X = 2
    return X if SP % X == 0 else 1


def solution(mesh):
    placed = (
        P("sp", "tp"),
        P(None, "tp"),
        P(None, "tp"),
        P(None, "tp"),
        P(None, "tp"),
        P(None, "tp"),
        P(),
        P(),
        P(),
        P(),
        P("sp", "tp"),
        P("sp", "tp"),
        P("tp", None),
        P("tp", None),
    )
    SP, TP, X = mesh.shape["sp"], mesh.shape["tp"], columns_of(mesh)
    small = X == 2 and TP == 4 and SP // X == 4
    body = functools.partial(block_shards if small else shards, SP, TP, X)
    return jax.shard_map(
        body, mesh=mesh, in_specs=placed, out_specs=P("sp", "tp"), check_vma=False
    )
```

```python
import functools

import jax
import jax.numpy as jnp
from jax import lax
from jax.experimental import pallas as pl
from jax.experimental.pallas import tpu as pltpu
from jax.sharding import PartitionSpec as P

HEAD_DIM = 128
decay_sharpness = 8.0
epsilon_norm = 1e-06
MESH = pl.DeviceIdType.MESH
F32 = jnp.float32
BF16 = jnp.bfloat16


def one_minus_exp(w):
    u = -w
    series = 1.0 - u / 9.0
    for n in range(8, 1, -1):
        series = 1.0 - u / n * series
    return jnp.where(u < 0.5, u * series, 1.0 - jnp.exp(w))


def remote(src, dst, send_sem, recv_sem, device):
    return pltpu.make_async_remote_copy(
        src_ref=src,
        dst_ref=dst,
        send_sem=send_sem,
        recv_sem=recv_sem,
        device_id=device,
        device_id_type=MESH,
    )


def kernel(
    SP,
    TP,
    X,
    tokens,
    lru_in,
    gate_in,
    query_w,
    key_w,
    value_w,
    conv_w,
    rg_w,
    ig_w,
    rate,
    decay_extra,
    forget,
    out_lru,
    out_fox,
    out,
    tok_buf,
    w_buf,
    acc,
    sq,
    lru_ref,
    halo,
    pad,
    bd_r,
    bd_i,
    gate_ref,
    q_ref,
    decay_buf,
    prefix_ref,
    local_ref,
    ends,
    incoming,
    kv_buf,
    cum_buf,
    cum_pad,
    wide,
    fcol,
    m_ref,
    l_ref,
    o_ref,
    q_far,
    m_far,
    l_far,
    o_far,
    part_out,
    stat_out,
    part_in,
    stat_in,
    wl_buf,
    wf_buf,
    br_lru,
    br_fox,
    oacc,
    load_sem,
    tsend,
    tfwd,
    trecv,
    hsend,
    hrecv,
    esend,
    erecv,
    zsend,
    xsend,
    kvrecv,
    wsend,
    wrecv,
    lsend,
    lrecv,
    fsend,
    ffwd,
    frecv,
    lfwd,
    qsend,
    qrecv,
    osend,
    orecv,
):
    rows, dcols = tokens.shape
    D, lw = lru_in.shape
    fw = query_w.shape[1]
    H = fw // HEAD_DIM
    oc = out.shape[1]
    Y = TP // 2
    Z = SP // X
    CH = tsend.shape[1]
    rc = rows // CH
    sp = lax.axis_index("sp")
    tp = lax.axis_index("tp")
    z = lax.div(sp, X)
    x = lax.rem(sp, X)
    partner = tp + 1 - 2 * lax.rem(tp, 2)
    far = [lax.rem(tp + 2 * k, TP) for k in range(Y)]
    pfar = [lax.rem(partner + 2 * k, TP) for k in range(Y)]
    offs = [0, lw, lw + fw, lw + 2 * fw, 2 * lw + 2 * fw, 2 * lw + 3 * fw]

    barrier = pltpu.get_barrier_semaphore()
    for k in range(1, SP):
        pl.semaphore_signal(
            barrier, inc=1, device_id={"sp": lax.rem(sp + k, SP)}, device_id_type=MESH
        )
    for k in range(1, TP):
        pl.semaphore_signal(
            barrier, inc=1, device_id={"tp": lax.rem(tp + k, TP)}, device_id_type=MESH
        )
    loads = []
    for i, w in enumerate((lru_in, key_w, value_w, gate_in, query_w)):
        c = pltpu.make_async_copy(w, w_buf.at[:, offs[i] : offs[i + 1]], load_sem.at[i])
        c.start()
        loads.append(c)
    mine = pl.ds(pl.multiple_of(tp * oc, 128), oc)
    own_loads = [
        pltpu.make_async_copy(decay_extra, decay_buf, load_sem.at[5]),
        pltpu.make_async_copy(out_lru.at[:, mine], wl_buf.at[tp], load_sem.at[6]),
        pltpu.make_async_copy(out_fox.at[:, mine], wf_buf.at[tp], load_sem.at[7]),
    ]
    for c in own_loads:
        c.start()
    pl.semaphore_wait(barrier, SP - 1 + TP - 1)

    pending = []

    def chunk(c):
        return pl.ds(c * rc, rc)

    for c in range(CH):
        for k in range(1, Y):
            s = remote(
                tokens.at[chunk(c)],
                tok_buf.at[tp, chunk(c)],
                tsend.at[k, c],
                trecv.at[tp, c],
                {"tp": far[k]},
            )
            s.start()
            pending.append(s)
    for c in range(CH):
        s = remote(
            tokens.at[chunk(c)],
            tok_buf.at[tp, chunk(c)],
            tsend.at[0, c],
            trecv.at[tp, c],
            {"tp": partner},
        )
        s.start()
        pending.append(s)

    bw = rg_w.shape[1]
    nb = lw // bw
    bd_r[...] = jnp.zeros_like(bd_r)
    bd_i[...] = jnp.zeros_like(bd_i)
    for n in range(nb):
        sl = pl.ds(n * bw, bw)
        bd_r[sl, sl] = rg_w[tp * nb + n]
        bd_i[sl, sl] = ig_w[tp * nb + n]
    cum_pad[...] = jnp.zeros_like(cum_pad)
    wide[...] = jnp.zeros_like(wide)
    wide[0:H, :] = forget[...]
    fcol[...] = wide[...].T
    cum_buf[sp] = wide[0:8, :]

    for c in loads:
        c.wait()

    def project(val, src, r, first=False):
        w_rows = pl.ds(pl.multiple_of(src * dcols, dcols), dcols)
        v32 = val.astype(F32)
        part = jnp.sum(v32 * v32, axis=1, keepdims=True)
        dot = jnp.dot(val, w_buf[w_rows, :], preferred_element_type=F32)
        if first:
            sq[r, :] = part
            acc[r, :] = dot
        else:
            sq[r, :] += part
            acc[r, :] += dot

    def tok_wait(src, c):
        ref = tok_buf.at[src, chunk(c)]
        remote(ref, ref, tsend.at[0, c], trecv.at[src, c], {"tp": partner}).wait_recv()

    for c in range(CH):
        project(tokens[chunk(c), :], tp, chunk(c), True)
    for c in range(CH):
        tok_wait(partner, c)
        project(tok_buf[partner, chunk(c), :], partner, chunk(c))
    for c in range(CH):
        for k in range(1, Y):
            tok_wait(far[k], c)
            ref = tok_buf.at[far[k], chunk(c)]
            s = remote(ref, ref, tfwd.at[k, c], trecv.at[far[k], c], {"tp": partner})
            s.start()
            pending.append(s)
            project(tok_buf[far[k], chunk(c), :], far[k], chunk(c))
        for k in range(1, Y):
            tok_wait(pfar[k], c)
            project(tok_buf[pfar[k], chunk(c), :], pfar[k], chunk(c))

    row_scale = lax.rsqrt(sq[...] / D + epsilon_norm)

    def scaled(i, n=1):
        return (acc[:, offs[i] : offs[i + n]] * row_scale).astype(BF16)

    lru_ref[...] = scaled(0)
    hb = halo.shape[0]
    halo_copy = remote(
        lru_ref.at[pl.ds(rows - hb, hb)],
        halo,
        hsend.at[0],
        hrecv.at[0],
        {"sp": lax.rem(sp + 1, SP)},
    )

    @pl.when(sp < SP - 1)
    def _():
        halo_copy.start()

    kv_buf[sp] = scaled(1, 2)

    paired = Z in (3, 4)
    helper = jnp.logical_and(z <= Z - 3, paired)
    helped = jnp.logical_and(z >= 2, paired)

    def block_copies(j, a, send_sem, device):
        return (
            remote(kv_buf.at[j], kv_buf.at[j], send_sem.at[a, 0], kvrecv.at[j, 0], device),
            remote(cum_buf.at[j], cum_buf.at[j], send_sem.at[a, 1], kvrecv.at[j, 1], device),
        )

    def z_copies(dz):
        j = (z - dz) * X + x
        return block_copies(j, dz, zsend, {"sp": lax.rem(sp + X, SP)})

    def x_copies(dz, dx):
        j = (z - dz) * X + x
        xo = lax.rem(x + dx, X)
        return block_copies(j, dz, xsend.at[dx - 1], {"sp": z * X + xo})

    def for_sends(dz, own, act):
        if own or not paired:

            @pl.when(z < Z - 1)
            def _():
                for c in z_copies(dz):
                    act(c)

        for dx in range(1, X):
            if own:

                @pl.when(jnp.logical_or(lax.rem(x + dx, X) > x, helper))
                def _():
                    for c in x_copies(dz, dx):
                        act(c)
            else:
                for c in x_copies(dz, dx):
                    act(c)

    def kv_wait(j):
        for c in block_copies(j, 0, zsend, {"sp": lax.rem(sp + X, SP)}):
            c.wait_recv()

    for_sends(0, True, lambda c: c.start())

    q_ref[...] = scaled(4)
    q_copy = remote(
        q_ref, q_far, qsend.at[0], qrecv.at[0], {"sp": lax.rem(sp + SP - 2 * X, SP)}
    )

    @pl.when(helped)
    def _():
        q_copy.start()

    for i, (w, buf) in enumerate(((out_lru, wl_buf), (out_fox, wf_buf))):
        for k in range(1, TP):
            t = lax.rem(tp + k, TP)
            cols = pl.ds(pl.multiple_of(t * oc, 128), oc)
            s = remote(w.at[:, cols], buf.at[tp], wsend.at[i, k], wrecv.at[i, tp], {"tp": t})
            s.start()
            pending.append(s)

    gate_ref[...] = scaled(3)

    @pl.when(sp == 0)
    def _():
        pad[0:8, :] = jnp.zeros((8, lw), F32)

    @pl.when(sp > 0)
    def _():
        halo_copy.wait_recv()
        pad[0:8, :] = halo[...].astype(F32)[hb - 8 : hb, :]

    pad[8 : 8 + rows, :] = lru_ref[...].astype(F32)
    chans = pl.ds(pl.multiple_of(tp * lw, 128), lw)
    taps = conv_w.shape[0]
    taps_f32 = conv_w[:, chans].astype(F32)
    conv = jnp.zeros((rows, lw), F32)
    for j in range(taps):
        conv = conv + taps_f32[j : j + 1, :] * pad[8 - (taps - 1) + j : 8 - (taps - 1) + j + rows, :]
    conv_b = conv.astype(BF16)

    def sigmoid(v):
        return 1.0 / (1.0 + jnp.exp(-v))

    recur_gate = sigmoid(jnp.dot(conv_b, bd_r[...], preferred_element_type=F32))
    input_gate = sigmoid(jnp.dot(conv_b, bd_i[...], preferred_element_type=F32))
    own_rate = rate[:, chans]
    softplus = jnp.maximum(-own_rate, 0.0) + jnp.log1p(jnp.exp(-jnp.abs(own_rate)))
    for c in own_loads:
        c.wait()
    log_decay = -decay_sharpness * softplus * recur_gate + decay_buf[...]
    prefix_ref[...] = jnp.exp(log_decay)
    local_ref[...] = jnp.sqrt(one_minus_exp(2.0 * log_decay)) * input_gate * conv_b.astype(F32)
    row_id = lax.broadcasted_iota(jnp.int32, (rows, lw), 0)
    step = 1
    while step < rows:
        a = prefix_ref[...]
        b = local_ref[...]
        keep = row_id >= step
        a_prev = jnp.where(keep, pltpu.roll(a, step, 0), 1.0)
        b_prev = jnp.where(keep, pltpu.roll(b, step, 0), 0.0)
        local_ref[...] = b + a * b_prev
        prefix_ref[...] = a * a_prev
        step *= 2
    ends[sp, 0:1, :] = prefix_ref[rows - 1 : rows, :]
    ends[sp, 1:2, :] = local_ref[rows - 1 : rows, :]

    def end_copy(k):
        return remote(
            ends.at[sp], ends.at[sp], esend.at[k], erecv.at[sp], {"sp": lax.rem(sp + k, SP)}
        )

    for k in range(1, SP):

        @pl.when(sp + k < SP)
        def _():
            end_copy(k).start()

    score_scale = HEAD_DIM ** (-0.5)
    qc = rows // 2

    def attend(j, diagonal, far_first=None):
        other = far_first is not None
        first = diagonal or far_first
        qs, ms, ls, os = (q_far, m_far, l_far, o_far) if other else (q_ref, m_ref, l_ref, o_ref)

        def some(i, carry):
            r = pl.ds(pl.multiple_of(i * qc, qc), qc)
            for h in range(H):
                hs = slice(h * HEAD_DIM, (h + 1) * HEAD_DIM)
                vs = slice(fw + h * HEAD_DIM, fw + (h + 1) * HEAD_DIM)
                s = lax.dot_general(
                    qs[r, hs],
                    kv_buf[j, :, hs],
                    (((1,), (1,)), ((), ())),
                    preferred_element_type=F32,
                )
                s = s * score_scale
                if not other:
                    s = s + fcol[r, h : h + 1]
                s = s - cum_buf[j, h : h + 1, :]
                if diagonal:
                    causal = (
                        lax.broadcasted_iota(jnp.int32, (qc, rows), 0) + i * qc
                        >= lax.broadcasted_iota(jnp.int32, (qc, rows), 1)
                    )
                    s = jnp.where(causal, s, -1e30)
                top = jnp.max(s, axis=1, keepdims=True)
                if first:
                    p = jnp.exp(s - top)
                    ms[h, r, :] = top
                    ls[h, r, :] = jnp.sum(p, axis=1, keepdims=True)
                    os[h, r, :] = jnp.dot(
                        p.astype(BF16), kv_buf[j, :, vs], preferred_element_type=F32
                    )
                else:
                    old = ms[h, r, :]
                    new = jnp.maximum(old, top)
                    p = jnp.exp(s - new)
                    fade = jnp.exp(old - new)
                    ms[h, r, :] = new
                    ls[h, r, :] = ls[h, r, :] * fade + jnp.sum(p, axis=1, keepdims=True)
                    os[h, r, :] = os[h, r, :] * fade + jnp.dot(
                        p.astype(BF16), kv_buf[j, :, vs], preferred_element_type=F32
                    )
            return carry

        lax.fori_loop(0, rows // qc, some, 0)

    attend(sp, True)

    def row_blocks(dz):
        for dx in range(1, X):
            xo = lax.rem(x + dx, X)

            @pl.when(jnp.logical_or(dz > 0, xo < x))
            def _():
                j = (z - dz) * X + xo
                kv_wait(j)
                attend(j, False)

    def finish_lru():
        incoming[...] = jnp.zeros_like(incoming)
        for j in range(SP - 1):

            @pl.when(j < sp)
            def _():
                remote(
                    ends.at[j], ends.at[j], esend.at[0], erecv.at[j], {"sp": lax.rem(sp + 1, SP)}
                ).wait_recv()
                incoming[...] = ends[j, 0:1, :] * incoming[...] + ends[j, 1:2, :]

        states = local_ref[...] + prefix_ref[...] * incoming[...]
        g = gate_ref[...].astype(F32)
        gelu = 0.5 * g * (1.0 + jnp.tanh(0.7978845608028654 * (g + 0.044715 * (g * g * g))))
        br_lru[tp] = (states * gelu).astype(BF16)
        for k in range(Y - 1, -1, -1):
            lru_copy(k).start()

    def lru_copy(k):
        to = far[k] if k else partner
        return remote(br_lru.at[tp], br_lru.at[tp], lsend.at[k], lrecv.at[tp], {"tp": to})

    lru_step = min(2, Z - 1)
    if Z == 1:
        finish_lru()

    def hop(dz, carry):
        @pl.when(dz <= z)
        def _():
            j = (z - dz) * X + x
            kv_wait(j)
            for_sends(dz, False, lambda c: c.start())
            row_blocks(dz - 1)
            attend(j, False)

        @pl.when(dz == lru_step)
        def _():
            finish_lru()

        return carry

    up = {"sp": lax.rem(sp + 2 * X, SP)}
    part_copies = (
        remote(part_out, part_in, osend.at[0], orecv.at[0], up),
        remote(stat_out, stat_in, osend.at[1], orecv.at[1], up),
    )

    def send_partial():
        for h in range(H):
            part_out[:, h * HEAD_DIM : (h + 1) * HEAD_DIM] = o_far[h].astype(BF16)
            cum_pad[:, h : h + 1] = m_far[h]
            cum_pad[:, H + h : H + h + 1] = l_far[h]
        stat_out[...] = cum_pad[...].T[0:8, :]
        for c in part_copies:
            c.start()

    if paired:
        below = (z - 1) * X

        @pl.when(helper)
        def _():
            q_copy.wait_recv()
            attend(sp, False, True)

        @pl.when(z >= 1)
        def _():
            kv_wait(below + x)
            for_sends(1, False, lambda c: c.start())

        for dx in range(1, X):
            xo = lax.rem(x + dx, X)

            @pl.when(jnp.logical_or(xo < x, helper))
            def _():
                kv_wait(z * X + xo)

            @pl.when(helper)
            def _():
                attend(z * X + xo, False, False)

        @pl.when(jnp.logical_and(helper, z == 0))
        def _():
            send_partial()

        for dx in range(1, X):
            xo = lax.rem(x + dx, X)

            @pl.when(xo < x)
            def _():
                attend(z * X + xo, False)

        finish_lru()

        @pl.when(jnp.logical_and(helper, z >= 1))
        def _():
            attend(below + x, False, False)

        @pl.when(z >= 1)
        def _():
            attend(below + x, False)
            for dx in range(1, X):
                j = below + lax.rem(x + dx, X)
                kv_wait(j)

                @pl.when(helper)
                def _():
                    attend(j, False, False)

            @pl.when(helper)
            def _():
                send_partial()

            for dx in range(1, X):
                attend(below + lax.rem(x + dx, X), False)

    else:
        lax.fori_loop(1, Z, hop, 0)

    def lru_wait(t):
        remote(br_lru.at[t], br_lru.at[t], lsend.at[0], lrecv.at[t], {"tp": partner}).wait_recv()

    def lru_dot(t):
        return jnp.dot(br_lru[t], wl_buf[t], preferred_element_type=F32)

    oacc[...] = lru_dot(tp)
    for k in range(1, TP):
        t = lax.rem(tp + k, TP)
        for i, buf in enumerate((wl_buf, wf_buf)):
            remote(buf.at[t], buf.at[t], wsend.at[i, k], wrecv.at[i, t], {"tp": t}).wait_recv()
    for k in range(1, Y):
        lru_wait(far[k])
        ref = br_lru.at[far[k]]
        s = remote(ref, ref, lfwd.at[k], lrecv.at[far[k]], {"tp": partner})
        s.start()
        pending.append(s)
    lru_wait(partner)
    oacc[...] += lru_dot(partner)
    for k in range(1, Y):
        oacc[...] += lru_dot(far[k])
        lru_wait(pfar[k])
        oacc[...] += lru_dot(pfar[k])

    if paired:

        @pl.when(helped)
        def _():
            for c in part_copies:
                c.wait_recv()
            wide[0:8, :] = stat_in[...]
            stats = wide[...].T
            for h in range(H):
                m_in = stats[:, h : h + 1] + fcol[:, h : h + 1]
                l_in = stats[:, H + h : H + h + 1]
                part = part_in[:, h * HEAD_DIM : (h + 1) * HEAD_DIM].astype(F32)
                new = jnp.maximum(m_ref[h], m_in)
                fade = jnp.exp(m_ref[h] - new)
                grow = jnp.exp(m_in - new)
                l_ref[h] = l_ref[h] * fade + l_in * grow
                o_ref[h] = o_ref[h] * fade + part * grow

    else:
        row_blocks(z)

    for c in range(CH):
        r = chunk(c)
        for h in range(H):
            br_fox[tp, r, h * HEAD_DIM : (h + 1) * HEAD_DIM] = (
                o_ref[h, r, :] / l_ref[h, r, :]
            ).astype(BF16)
        ref = br_fox.at[tp, r]
        for k in list(range(1, Y)) + [0]:
            to = far[k] if k else partner
            s = remote(ref, ref, fsend.at[k, c], frecv.at[tp, c], {"tp": to})
            s.start()
            pending.append(s)

    def fox_wait(src, c):
        ref = br_fox.at[src, chunk(c)]
        remote(ref, ref, fsend.at[0, c], frecv.at[src, c], {"tp": partner}).wait_recv()

    def fox_dot(src, r):
        return jnp.dot(br_fox[src, r, :], wf_buf[src], preferred_element_type=F32)

    for c in range(CH):
        fox_wait(partner, c)
        oacc[chunk(c), :] += fox_dot(tp, chunk(c)) + fox_dot(partner, chunk(c))
    for c in range(CH):
        r = chunk(c)
        for k in range(1, Y):
            fox_wait(far[k], c)
            ref = br_fox.at[far[k], r]
            s = remote(ref, ref, ffwd.at[k, c], frecv.at[far[k], c], {"tp": partner})
            s.start()
            pending.append(s)
            oacc[r, :] += fox_dot(far[k], r)
        for k in range(1, Y):
            fox_wait(pfar[k], c)
            oacc[r, :] += fox_dot(pfar[k], r)
        out[r, :] = oacc[r, :].astype(out.dtype)

    for s in pending:
        s.wait_send()
    for k in range(Y):
        lru_copy(k).wait_send()

    @pl.when(helped)
    def _():
        q_copy.wait_send()

    @pl.when(helper)
    def _():
        for c in part_copies:
            c.wait_send()

    @pl.when(sp < SP - 1)
    def _():
        halo_copy.wait_send()

    for k in range(1, SP):

        @pl.when(sp + k < SP)
        def _():
            end_copy(k).wait_send()

    for_sends(0, True, lambda c: c.wait_send())

    def drain(dz, carry):
        @pl.when(dz <= z)
        def _():
            for_sends(dz, False, lambda c: c.wait_send())

        return carry

    if paired:

        @pl.when(z >= 1)
        def _():
            for_sends(1, False, lambda c: c.wait_send())

    else:
        lax.fori_loop(1, Z, drain, 0)


def shards(SP, TP, X, *args):
    tokens, lru_in, gate_in, query_w = args[:4]
    (conv_weight, rg_w, ig_w, rate, decay_extra, forget, out_lru, out_fox) = args[6:]
    rows, dcols = tokens.shape
    D, lw = lru_in.shape
    fw = query_w.shape[1]
    oc = out_lru.shape[1] // TP
    tot = 2 * lw + 3 * fw
    H = fw // HEAD_DIM
    Y = TP // 2
    Z = SP // X
    CH = 4
    vm = pl.BlockSpec(memory_space=pltpu.VMEM)
    hbm = pl.BlockSpec(memory_space=pl.ANY)
    dma = pltpu.SemaphoreType.DMA
    V = pltpu.VMEM
    scratch = [
        V((TP, rows, dcols), BF16),
        V((D, tot), BF16),
        V((rows, tot), F32),
        V((rows, 1), F32),
        V((rows, lw), BF16),
        V((16, lw), BF16),
        V((rows + 8, lw), F32),
        V((lw, lw), BF16),
        V((lw, lw), BF16),
        V((rows, lw), BF16),
        V((rows, fw), BF16),
        V((rows, lw), F32),
        V((rows, lw), F32),
        V((rows, lw), F32),
        V((SP, 8, lw), F32),
        V((1, lw), F32),
        V((SP, rows, 2 * fw), BF16),
        V((SP, 8, rows), F32),
        V((rows, 128), F32),
        V((128, rows), F32),
        V((rows, 128), F32),
        V((H, rows, 1), F32),
        V((H, rows, 1), F32),
        V((H, rows, HEAD_DIM), F32),
        V((rows, fw), BF16),
        V((H, rows, 1), F32),
        V((H, rows, 1), F32),
        V((H, rows, HEAD_DIM), F32),
        V((rows, fw), BF16),
        V((8, rows), F32),
        V((rows, fw), BF16),
        V((8, rows), F32),
        V((TP, lw, oc), BF16),
        V((TP, fw, oc), BF16),
        V((TP, rows, lw), BF16),
        V((TP, rows, fw), BF16),
        V((rows, oc), F32),
        dma((8,)),
        dma((Y, CH)),
        dma((Y, CH)),
        dma((TP, CH)),
        dma((1,)),
        dma((1,)),
        dma((SP,)),
        dma((SP,)),
        dma((Z, 2)),
        dma((max(X - 1, 1), Z, 2)),
        dma((SP, 2)),
        dma((2, TP)),
        dma((2, TP)),
        dma((TP,)),
        dma((TP,)),
        dma((Y, CH)),
        dma((Y, CH)),
        dma((TP, CH)),
        dma((Y,)),
        dma((1,)),
        dma((1,)),
        dma((2,)),
        dma((2,)),
    ]
    return pl.pallas_call(
        functools.partial(kernel, SP, TP, X),
        out_shape=jax.ShapeDtypeStruct((rows, oc), BF16),
        in_specs=[vm] + [hbm] * 5 + [vm] * 4 + [hbm, vm, hbm, hbm],
        out_specs=vm,
        scratch_shapes=scratch,
        compiler_params=pltpu.CompilerParams(
            collective_id=0, has_side_effects=True, vmem_limit_bytes=60 * 1024 * 1024
        ),
    )(*args[:9], rate.reshape(1, -1), decay_extra, forget.T, out_lru, out_fox)


LOG2E = 1.4426950408889634


def block_kernel(
    SP,
    TP,
    X,
    CH,
    tokens,
    lru_in,
    gate_in,
    query_w,
    key_w,
    value_w,
    conv_w,
    rg_w,
    ig_w,
    rate,
    decay_extra,
    forget,
    out_lru,
    out_fox,
    out,
    tok_buf,
    w_buf,
    acc,
    sq,
    lru_ref,
    halo,
    pad,
    conv_v,
    rg_v,
    ig_v,
    rate_v,
    forget_v,
    bd_r,
    bd_i,
    gate_ref,
    q_ref,
    decay_buf,
    prefix_ref,
    local_ref,
    seg_a,
    seg_b,
    carry_ref,
    ends,
    kv_buf,
    cum_buf,
    m_ref,
    o_ref,
    q_far,
    m_far,
    o_far,
    part_out,
    stat_out,
    part_in,
    stat_in,
    wl_buf,
    wf_buf,
    br_lru,
    br_fox,
    oacc,
    load_sem,
    tsend,
    trecv,
    hsend,
    hrecv,
    esend,
    erecv,
    csend,
    crecv,
    zsend,
    xsend,
    zfwd,
    xfwd,
    kvrecv,
    wsend,
    wrecv_own,
    wrecv,
    lsend,
    lrecv,
    fsend,
    frecv,
    qsend,
    qrecv,
    osend,
    orecv,
):
    rows, dcols = tokens.shape
    D, lw = lru_in.shape
    fw = query_w.shape[1]
    H = fw // HEAD_DIM
    oc = out.shape[1]
    Z = SP // X
    rc = rows // CH
    half = rows // 2
    wh = out_lru.shape[0] // X
    sp = lax.axis_index("sp")
    tp = lax.axis_index("tp")
    z = lax.div(sp, X)
    x = lax.rem(sp, X)
    xo = 1 - x
    y = lax.div(tp, 2)
    partner = tp + 1 - 2 * lax.rem(tp, 2)
    far = lax.rem(tp + 2, TP)
    pfar = lax.rem(partner + 2, TP)
    j_xo = z * X + xo
    to_xo = {"sp": j_xo}
    to_up = {"sp": lax.rem(sp + X, SP)}
    j_b = lax.rem(sp + SP - X, SP)
    j_bo = lax.rem(j_xo + SP - X, SP)
    helper = z <= Z - 3
    helped = z >= 2
    not_top = z < Z - 1
    above0 = z >= 1
    order = list(range(CH - 1, -1, -1))
    second_top = z == Z - 2
    climbs = {order[1]: not_top, order[3]: second_top}
    crosses = {
        order[0]: above0,
        order[2]: above0,
        order[3]: jnp.logical_and(above0, not_top),
    }
    whalf = lax.rem(x + z, X)
    top = z == Z - 1
    PARTNER, FAR, PFAR = 0, 1, 2
    ACROSS, BELOW, DIAG = 0, 1, 2
    score_k = HEAD_DIM ** (-0.5) * LOG2E

    def chunk(c):
        return pl.ds(c * rc, rc)

    pieces = [(c * rc, rc) for c in range(CH - 1)]
    pieces += [(rows - rc, rc // 2), (rows - rc // 2, rc // 2)]
    PC = len(pieces)

    def piece(k):
        return pl.ds(*pieces[k])

    def pieces_of(c):
        return [k for k, (at, n) in enumerate(pieces) if at // rc == c]

    barrier = pltpu.get_barrier_semaphore()
    for k in range(1, SP):
        pl.semaphore_signal(
            barrier, inc=1, device_id={"sp": lax.rem(sp + k, SP)}, device_id_type=MESH
        )
    for k in range(1, TP):
        pl.semaphore_signal(
            barrier, inc=1, device_id={"tp": lax.rem(tp + k, TP)}, device_id_type=MESH
        )

    def load(i, src, dst):
        c = pltpu.make_async_copy(src, dst, load_sem.at[i])
        c.start()
        return c

    tok_loads = [
        load(n, tokens.at[chunk(c)], tok_buf.at[tp, chunk(c)]) for n, c in enumerate(order)
    ]
    cols = (0, fw, 2 * fw, 2 * fw + lw, 3 * fw + lw, 3 * fw + 2 * lw)
    for i, w in enumerate((key_w, value_w, lru_in, query_w, gate_in)):
        load(CH, w, w_buf.at[:, cols[i] : cols[i + 1]])
    mine = pl.ds(pl.multiple_of(tp * oc, 128), oc)
    bw = rg_w.shape[1]
    nb = lw // bw
    gates = pl.ds(tp * nb, nb)
    forget_load = load(CH + 1, forget, forget_v)
    small_loads = [
        load(CH + 2, conv_w, conv_v),
        load(CH + 3, rg_w.at[gates], rg_v),
        load(CH + 4, ig_w.at[gates], ig_v),
        load(CH + 5, rate, rate_v),
        load(CH + 6, decay_extra, decay_buf),
    ]
    own_loads = [
        load(CH + 7, out_lru.at[:, mine], wl_buf.at[tp]),
        load(CH + 8, out_fox.at[:, mine], wf_buf.at[tp]),
    ]
    pl.semaphore_wait(barrier, SP - 1 + TP - 1)

    def send(ref, send_sem, recv_sem, device):
        remote(ref, ref, send_sem, recv_sem, device).start()

    def arrived(ref, recv_sem):
        remote(ref, ref, recv_sem, recv_sem, to_xo).wait_recv()

    def sent(ref, send_sem):
        remote(ref, ref, send_sem, send_sem, to_xo).wait_send()

    for n, c in enumerate(order):
        tok_loads[n].wait()
        ref = tok_buf.at[tp, chunk(c)]
        send(ref, tsend.at[0], trecv.at[FAR, c], {"tp": far})
        send(ref, tsend.at[1], trecv.at[PARTNER, c], {"tp": partner})

    forget_load.wait()
    cum_buf[sp] = forget_v[...] * LOG2E
    own_cum = cum_buf.at[sp]
    send(own_cum, csend.at[0], crecv.at[ACROSS], to_xo)

    @pl.when(not_top)
    def _():
        send(own_cum, csend.at[1], crecv.at[BELOW], to_up)
        send(own_cum, csend.at[1], crecv.at[DIAG], {"sp": lax.rem(j_xo + X, SP)})

    for c in small_loads:
        c.wait()
    bd_r[...] = jnp.zeros_like(bd_r)
    bd_i[...] = jnp.zeros_like(bd_i)
    for n in range(nb):
        sl = pl.ds(n * bw, bw)
        bd_r[sl, sl] = rg_v[n]
        bd_i[sl, sl] = ig_v[n]
    pltpu.make_async_copy(w_buf, w_buf, load_sem.at[CH]).wait()

    def tok_wait(src, role, c):
        arrived(tok_buf.at[src, chunk(c)], trecv.at[role, c])

    def features(side, c):
        first = 2 * side
        return jnp.concatenate([tok_buf[first, chunk(c), :], tok_buf[first + 1, chunk(c), :]], axis=1)

    def w_rows(side):
        return pl.ds(pl.multiple_of(side * 2 * dcols, 2 * dcols), 2 * dcols)

    def squares(v):
        v32 = v.astype(F32)
        return jnp.sum(v32 * v32, axis=1, keepdims=True)

    def near_part(c, slot):
        tok_wait(partner, PARTNER, c)
        v = features(y, c)
        sq[slot] = squares(v)
        acc[slot] = jnp.dot(v, w_buf[w_rows(y), :], preferred_element_type=F32)

    halo_copy = remote(
        lru_ref.at[pl.ds(rows - halo.shape[0], halo.shape[0])],
        halo,
        hsend.at[0],
        hrecv.at[0],
        {"sp": lax.rem(sp + 1, SP)},
    )

    def kv_send(j, c, send_sem, role, device):
        send(kv_buf.at[j, chunk(c)], send_sem.at[0], kvrecv.at[role, c], device)

    def kv_wait(j, c, role):
        arrived(kv_buf.at[j, chunk(c)], kvrecv.at[role, c])

    def all_across(own_x):
        return jnp.logical_or(own_x, helper)

    def across(own_x, c):
        need = all_across(own_x)
        return jnp.logical_or(need, climbs[c]) if c in climbs else need

    def q_copy(c):
        return remote(
            q_ref.at[chunk(c)],
            q_far.at[chunk(c)],
            qsend.at[0],
            qrecv.at[0 if c in order[0:2] else 1],
            {"sp": lax.rem(sp + SP - 2 * X, SP)},
        )

    def far_part(i, c, slot):
        tok_wait(far, FAR, c)
        send(tok_buf.at[far, chunk(c)], tsend.at[2], trecv.at[PFAR, c], {"tp": partner})
        if i + 1 < CH:
            near_part(order[i + 1], 1 - slot)
        tok_wait(pfar, PFAR, c)
        if i == CH - 1:
            send_weights()
        v = features(1 - y, c)
        row_scale = lax.rsqrt((sq[slot] + squares(v)) / D + epsilon_norm)

        def part(a, b):
            w = w_buf[w_rows(1 - y), cols[a] : cols[b]]
            both = acc[slot, :, cols[a] : cols[b]] + jnp.dot(v, w, preferred_element_type=F32)
            return (both * row_scale).astype(BF16)

        kv_buf[sp, chunk(c), :] = part(0, 2)

        @pl.when(across(x == 0, c))
        def _():
            kv_send(sp, c, xsend, ACROSS, to_xo)

        @pl.when(not_top)
        def _():
            kv_send(sp, c, zsend, BELOW, to_up)

        rest = part(2, 5)
        lru_ref[chunk(c), :] = rest[:, 0:lw]
        q_ref[chunk(c), :] = rest[:, lw : lw + fw]
        gate_ref[chunk(c), :] = rest[:, lw + fw :]

        @pl.when(helped)
        def _():
            q_copy(c).start()

        if i == 0:

            @pl.when(sp < SP - 1)
            def _():
                halo_copy.start()

    banks = ((out_lru, wl_buf), (out_fox, wf_buf))

    def send_weights():
        r = pl.ds(pl.multiple_of(whalf * wh, wh), wh)

        def over_y(n):
            w, buf = banks[n]
            for role, t in ((FAR, far), (PFAR, pfar)):
                c = pl.ds(pl.multiple_of(t * oc, 128), oc)
                remote(
                    w.at[r, c], buf.at[tp, r], wsend.at[n], wrecv.at[n, role - 1, whalf], {"tp": t}
                ).start()

        pl.when(above0)(lambda: over_y(0))
        over_y(1)
        c = pl.ds(pl.multiple_of(partner * oc, 128), oc)
        for n, (w, buf) in enumerate(banks):
            remote(w.at[:, c], buf.at[tp], wsend.at[2], wrecv_own.at[n], {"tp": partner}).start()

    def weight_part(n, role, k):
        t = far if role == FAR else pfar
        ref = banks[n][1].at[t, pl.ds(pl.multiple_of(k * wh, wh), wh)]
        return ref, wrecv.at[n, role - 1, k]

    def weight_pass(n, role):
        ref, sem = weight_part(n, role, whalf)

        def take():
            arrived(ref, sem)

        if n == 0:
            pl.when(above0)(take)
        else:
            take()

        @pl.when(above0)
        def _():
            send(ref, wsend.at[3], sem, {"sp": lax.rem(sp + SP - X, SP)})

        @pl.when(top)
        def _():
            send(ref, wsend.at[4], sem, to_xo)

    def weight_pass_bottom(role):
        @pl.when(z == 0)
        def _():
            ref, sem = weight_part(0, role, 1 - whalf)
            arrived(ref, sem)
            send(ref, wsend.at[4], sem, to_xo)

    def weight_wait(n, role):
        k = 1 - whalf
        if n == 0:
            k = jnp.where(z == 0, whalf, k)
        arrived(*weight_part(n, role, k))

    def pass_up(c):
        @pl.when(climbs[c])
        def _():
            kv_wait(j_xo, c, ACROSS)
            kv_send(j_xo, c, zfwd, DIAG, to_up)

    def pass_across(c):
        @pl.when(crosses[c])
        def _():
            kv_wait(j_b, c, BELOW)
            kv_send(j_b, c, xfwd, DIAG, to_xo)

    near_part(order[0], 0)
    for i, c in enumerate(order):
        far_part(i, c, i % 2)

    pass_across(order[0])
    pass_up(order[1])

    @pl.when(sp == 0)
    def _():
        pad[0:8, :] = jnp.zeros((8, lw), F32)

    @pl.when(sp > 0)
    def _():
        halo_copy.wait_recv()
        hb = halo.shape[0]
        pad[0:8, :] = halo[...].astype(F32)[hb - 8 : hb, :]

    pad[8 : 8 + rows, :] = lru_ref[...].astype(F32)
    chans = pl.ds(pl.multiple_of(tp * lw, 128), lw)
    taps = conv_w.shape[0]
    taps_f32 = conv_v[:, chans].astype(F32)
    conv = jnp.zeros((rows, lw), F32)
    for j in range(taps):
        conv = conv + taps_f32[j : j + 1, :] * pad[8 - (taps - 1) + j : 8 - (taps - 1) + j + rows, :]
    conv_b = conv.astype(BF16)

    def sigmoid(v):
        return 1.0 / (1.0 + jnp.exp(-v))

    recur_gate = sigmoid(jnp.dot(conv_b, bd_r[...], preferred_element_type=F32))
    input_gate = sigmoid(jnp.dot(conv_b, bd_i[...], preferred_element_type=F32))
    own_rate = rate_v[:, chans]
    softplus = jnp.maximum(-own_rate, 0.0) + jnp.log1p(jnp.exp(-jnp.abs(own_rate)))
    log_decay = -decay_sharpness * softplus * recur_gate + decay_buf[...]
    decay = jnp.exp(log_decay)
    driven = jnp.sqrt(one_minus_exp(2.0 * log_decay)) * input_gate * conv_b.astype(F32)
    for n in range(lw // 128):
        prefix_ref[n] = decay[:, n * 128 : (n + 1) * 128]
        local_ref[n] = driven[:, n * 128 : (n + 1) * 128]

    segs = 8
    seg_len = rows // segs
    run_a = jnp.ones((segs, lw), F32)
    run_b = jnp.zeros((segs, lw), F32)
    for i in range(seg_len):
        at = pl.ds(i, segs, stride=seg_len)
        a = [prefix_ref[n, at, :] for n in range(lw // 128)]
        b = [local_ref[n, at, :] for n in range(lw // 128)]
        a = jnp.concatenate(a, axis=1)
        b = jnp.concatenate(b, axis=1)
        run_a = run_a * a
        run_b = a * run_b + b
        for n in range(lw // 128):
            prefix_ref[n, at, :] = run_a[:, n * 128 : (n + 1) * 128]
            local_ref[n, at, :] = run_b[:, n * 128 : (n + 1) * 128]
    seg_a[...] = run_a
    seg_b[...] = run_b
    end_a = seg_a[0:1, :]
    end_b = seg_b[0:1, :]
    for i in range(1, segs):
        end_b = seg_a[i : i + 1, :] * end_b + seg_b[i : i + 1, :]
        end_a = end_a * seg_a[i : i + 1, :]
    ends[sp, 0:1, :] = end_a
    ends[sp, 1:2, :] = end_b

    def end_copy(k):
        return remote(
            ends.at[sp],
            ends.at[sp],
            esend.at[0],
            erecv.at[0],
            {"sp": lax.rem(sp + k, SP)},
        )

    for k in range(1, SP):
        end_copy(k).start()

    pass_across(order[2])

    def attend(qs, st, j, lo, hi, first=False, diagonal=False, qc=half, after=None, parts=None):
        ms, os = st
        items = [(i, h) for i in (parts or range(rows // qc)) for h in range(H)]

        def width(i):
            return (lo, (i + 1) * qc) if diagonal else (lo, hi)

        def scores(i, h):
            a, b = width(i)
            hs = slice(h * HEAD_DIM, (h + 1) * HEAD_DIM)
            s = lax.dot_general(
                qs[i * qc : (i + 1) * qc, hs],
                kv_buf[j, a:b, hs],
                (((1,), (1,)), ((), ())),
                preferred_element_type=F32,
            )
            s = s * score_k - cum_buf[j, h : h + 1, a:b]
            if diagonal:
                causal = (
                    lax.broadcasted_iota(jnp.int32, (qc, b - a), 0) + (i * qc - a)
                    >= lax.broadcasted_iota(jnp.int32, (qc, b - a), 1)
                )
                s = jnp.where(causal, s, -1e30)
            return s

        def update(i, h, s):
            a, b = width(i)
            r = slice(i * qc, (i + 1) * qc)
            top = jnp.max(s, axis=1, keepdims=True)
            if first:
                new = jnp.broadcast_to(top, (qc, 128))
            else:
                old = ms[h, r, :]
                new = jnp.maximum(old, top)
            ms[h, r, :] = new
            p = jnp.exp2(s - jnp.concatenate([new] * ((b - a) // 128), axis=1)).astype(BF16)
            v = kv_buf[j, a:b, fw + h * HEAD_DIM : fw + (h + 1) * HEAD_DIM]
            v1 = jnp.concatenate([v, jnp.ones((b - a, 128), BF16)], axis=1)
            pv = jnp.dot(p, v1, preferred_element_type=F32)
            if first:
                os[h, r, :] = pv
            else:
                fade = jnp.exp2(old - new)
                os[h, r, :] = os[h, r, :] * jnp.concatenate([fade, fade], axis=1) + pv

        s = scores(*items[0])
        for n, (i, h) in enumerate(items):
            nxt = scores(*items[n + 1]) if n + 1 < len(items) else None
            update(i, h, s)
            s = nxt
            if after is not None and h == H - 1:
                after(i)

    own_st = (m_ref, o_ref)
    far_st = (m_far, o_far)
    up2 = {"sp": lax.rem(sp + 2 * X, SP)}

    def part_copy(k):
        r = piece(k)
        return remote(part_out.at[r], part_in.at[r], osend.at[0], orecv.at[k], up2)

    def stat_copy(c):
        return remote(stat_out.at[c], stat_in.at[c], osend.at[1], orecv.at[PC + c], up2)

    def send_partial(c):
        r = slice(c * rc, (c + 1) * rc)
        lane = lax.broadcasted_iota(jnp.int32, (rc, 128), 1)
        stats = jnp.zeros((rc, 128), F32)
        for h in range(H):
            part_out[r, h * HEAD_DIM : (h + 1) * HEAD_DIM] = o_far[h, r, 0:HEAD_DIM].astype(BF16)
            stats = jnp.where(lane == h, m_far[h, r, :], stats)
            stats = jnp.where(lane == H + h, o_far[h, r, HEAD_DIM:], stats)
        stat_out[c] = stats.T[0 : 2 * H, :]
        stat_copy(c).start()
        for k in pieces_of(c):
            part_copy(k).start()

    attend(q_ref, own_st, sp, 0, rows, True, True)

    @pl.when(helper)
    def _():
        arrived(q_far.at[pl.ds(half, half)], qrecv.at[0])
        attend(q_far, far_st, sp, 0, rows, True, parts=(1,))

    pass_up(order[3])
    pass_across(order[3])

    weight_pass(0, FAR)
    arrived(cum_buf.at[j_xo], crecv.at[ACROSS])

    for c in order:
        need = all_across(x == 1)
        if c in climbs:
            need = jnp.logical_and(need, jnp.logical_not(climbs[c]))

        @pl.when(need)
        def _():
            kv_wait(j_xo, c, ACROSS)

    @pl.when(z == 0)
    def _():
        late = range(CH // 2, CH)
        attend(q_far, far_st, j_xo, 0, rows, qc=rc, after=send_partial, parts=late)
        arrived(q_far.at[pl.ds(0, half)], qrecv.at[1])
        attend(q_far, far_st, sp, 0, rows, True, parts=(0,))
        early = range(CH // 2)
        attend(q_far, far_st, j_xo, 0, rows, qc=rc, after=send_partial, parts=early)

    middle = jnp.logical_and(above0, helper)

    @pl.when(middle)
    def _():
        arrived(q_far.at[pl.ds(0, half)], qrecv.at[1])
        attend(q_far, far_st, sp, 0, rows, True, parts=(0,))
        attend(q_far, far_st, j_xo, 0, rows)

    weight_pass(0, PFAR)

    @pl.when(above0)
    def _():
        for c in climbs:

            @pl.when(jnp.logical_not(crosses.get(c, False)))
            def _():
                kv_wait(j_b, c, BELOW)

        arrived(cum_buf.at[j_b], crecv.at[BELOW])
        arrived(cum_buf.at[j_bo], crecv.at[DIAG])

    @pl.when(middle)
    def _():
        attend(q_far, far_st, j_b, 0, rows)

    @pl.when(above0)
    def _():
        attend(q_ref, own_st, j_b, 0, rows)

    carry_ref[0:1, :] = jnp.zeros((1, lw), F32)
    others = ends.at[pl.ds(0, SP - 1)]
    arrived(others, erecv.at[0])
    for j in range(SP - 1):

        @pl.when(j < sp)
        def _():
            carry_ref[0:1, :] = ends[j, 0:1, :] * carry_ref[0:1, :] + ends[j, 1:2, :]

    carry = carry_ref[0:1, :]
    for i in range(segs):
        r = slice(i * seg_len, (i + 1) * seg_len)
        g = gate_ref[r, :].astype(F32)
        gelu = 0.5 * g * (1.0 + jnp.tanh(0.7978845608028654 * (g + 0.044715 * (g * g * g))))
        for n in range(lw // 128):
            cs = slice(n * 128, (n + 1) * 128)
            states = local_ref[n, r, :] + prefix_ref[n, r, :] * carry[:, cs]
            br_lru[tp, r, cs] = (states * gelu[:, cs]).astype(BF16)
        if i + 1 < segs:
            carry = seg_a[i : i + 1, :] * carry + seg_b[i : i + 1, :]
    own_lru = br_lru.at[tp]
    send(own_lru, lsend.at[0], lrecv.at[FAR], {"tp": far})
    send(own_lru, lsend.at[0], lrecv.at[PARTNER], {"tp": partner})
    weight_pass(1, FAR)

    @pl.when(jnp.logical_and(helper, above0))
    def _():
        for c in order[0:2]:
            kv_wait(j_bo, c, DIAG)
        attend(q_far, far_st, j_bo, half, rows)

    @pl.when(x == 1)
    def _():
        attend(q_ref, own_st, j_xo, 0, rows)

    weight_pass(1, PFAR)

    upper = jnp.logical_and(above0, jnp.logical_not(helper))

    def heads_of(h):
        return slice(h * HEAD_DIM, (h + 1) * HEAD_DIM)

    def send_fox(k):
        ref = br_fox.at[tp, piece(k)]
        send(ref, fsend.at[0], frecv.at[FAR, k], {"tp": far})
        send(ref, fsend.at[1], frecv.at[PARTNER, k], {"tp": partner})

    def finish_rows(c):
        r = slice(c * rc, (c + 1) * rc)
        for h in range(H):
            br_fox[tp, r, heads_of(h)] = (o_ref[h, r, 0:HEAD_DIM] / o_ref[h, r, HEAD_DIM:]).astype(
                BF16
            )
        for k in pieces_of(c):
            send_fox(k)

    def merge_rows(c):
        for k in pieces_of(c):
            at, n = pieces[k]
            arrived(part_in.at[piece(k)], orecv.at[k])
            if k == pieces_of(c)[0]:
                arrived(stat_in.at[c], orecv.at[PC + c])
                pad_rows = jnp.zeros((128 - 2 * H, rc), F32)
                stats = jnp.concatenate([stat_in[c], pad_rows], axis=0).T
            r = slice(at, at + n)
            mine = slice(at - c * rc, at - c * rc + n)
            for h in range(H):
                m_in = stats[mine, h : h + 1]
                l_in = stats[mine, H + h : H + h + 1]
                part = part_in[r, heads_of(h)].astype(F32)
                old = m_ref[h, r, :]
                new = jnp.maximum(old, m_in)
                fade = jnp.exp2(old - new)
                grow = jnp.exp2(m_in - new)
                total = o_ref[h, r, HEAD_DIM:] * fade + l_in * grow
                br_fox[tp, r, heads_of(h)] = (
                    (o_ref[h, r, 0:HEAD_DIM] * fade + part * grow) / total
                ).astype(BF16)
            send_fox(k)

    def pair_dot(br, buf, side, r):
        first = 2 * side
        return jnp.dot(br[first, r, :], buf[first], preferred_element_type=F32) + jnp.dot(
            br[first + 1, r, :], buf[first + 1], preferred_element_type=F32
        )

    def lru_near():
        for c in own_loads:
            c.wait()
        for n in range(2):
            arrived(banks[n][1].at[partner], wrecv_own.at[n])
        arrived(br_lru.at[partner], lrecv.at[PARTNER])
        for c in range(CH):
            oacc[chunk(c), :] = pair_dot(br_lru, wl_buf, y, chunk(c))

    def lru_relay():
        arrived(br_lru.at[far], lrecv.at[FAR])
        send(br_lru.at[far], lsend.at[1], lrecv.at[PFAR], {"tp": partner})

    def lru_far():
        for role in (FAR, PFAR):
            weight_wait(0, role)
        arrived(br_lru.at[pfar], lrecv.at[PFAR])
        for c in range(CH):
            oacc[chunk(c), :] += pair_dot(br_lru, wl_buf, 1 - y, chunk(c))

    @pl.when(upper)
    def _():
        for c in order[0:2]:
            kv_wait(j_bo, c, DIAG)
        attend(q_ref, own_st, j_bo, half, rows)

    @pl.when(above0)
    def _():
        for c in order[2:]:
            kv_wait(j_bo, c, DIAG)

    @pl.when(middle)
    def _():
        attend(q_far, far_st, j_bo, 0, half, qc=rc, after=send_partial)
        attend(q_ref, own_st, j_bo, 0, rows, qc=rc, after=finish_rows)

    @pl.when(upper)
    def _():
        attend(q_ref, own_st, j_bo, 0, half)

    @pl.when(top)
    def _():
        lru_near()
        merge_rows(0)
        merge_rows(1)
        lru_relay()
        merge_rows(2)
        lru_far()
        merge_rows(3)

    @pl.when(second_top)
    def _():
        for c in range(CH):
            merge_rows(c)

    @pl.when(z == 0)
    def _():
        for c in range(CH):
            finish_rows(c)

    weight_pass_bottom(FAR)
    weight_pass_bottom(PFAR)

    @pl.when(not_top)
    def _():
        lru_near()
        lru_relay()
        lru_far()

    for role in (FAR, PFAR):
        weight_wait(1, role)

    def fox_pass(k):
        arrived(br_fox.at[far, piece(k)], frecv.at[FAR, k])
        send(br_fox.at[far, piece(k)], fsend.at[2], frecv.at[PFAR, k], {"tp": partner})

    fox_pass(0)
    for k in range(PC):
        r = piece(k)
        if k + 1 < PC:
            fox_pass(k + 1)
        arrived(br_fox.at[partner, r], frecv.at[PARTNER, k])
        oacc[r, :] += pair_dot(br_fox, wf_buf, y, r)
        arrived(br_fox.at[pfar, r], frecv.at[PFAR, k])
        out[r, :] = (oacc[r, :] + pair_dot(br_fox, wf_buf, 1 - y, r)).astype(out.dtype)

    for k in range(3):
        sent(tok_buf.at[0], tsend.at[k])
        sent(br_fox.at[0], fsend.at[k])
    sent(br_lru.at[pl.ds(0, 2)], lsend.at[0])
    sent(br_lru.at[0], lsend.at[1])
    sent(wl_buf.at[0], wsend.at[1])
    sent(wl_buf.at[pl.ds(0, 2)], wsend.at[2])

    @pl.when(above0)
    def _():
        sent(wl_buf.at[0], wsend.at[0])
        sent(wl_buf.at[pl.ds(0, 2)], wsend.at[3])

    @pl.when(top)
    def _():
        sent(wl_buf.at[pl.ds(0, 2)], wsend.at[4])

    @pl.when(z == 0)
    def _():
        sent(wl_buf.at[0], wsend.at[4])

    sent(own_cum, csend.at[0])
    top_half = pl.ds(0, half)
    need = all_across(x == 0)

    @pl.when(need)
    def _():
        sent(kv_buf.at[0], xsend.at[0])

    @pl.when(jnp.logical_and(second_top, jnp.logical_not(need)))
    def _():
        sent(kv_buf.at[0, top_half], xsend.at[0])

    for level in range(Z):

        @pl.when(z == level)
        def _():
            ups = (level < Z - 1) + (level == Z - 2)
            if ups:
                sent(kv_buf.at[0, pl.ds(0, ups * rc)], zfwd.at[0])
            overs = (2 if level else 0) + (0 < level < Z - 1)
            if overs:
                sent(kv_buf.at[0, pl.ds(0, overs * rc)], xfwd.at[0])

    @pl.when(not_top)
    def _():
        sent(kv_buf.at[0], zsend.at[0])
        sent(cum_buf.at[pl.ds(0, 2)], csend.at[1])

    @pl.when(helped)
    def _():
        sent(q_ref, qsend.at[0])

    @pl.when(helper)
    def _():
        sent(part_out, osend.at[0])
        sent(stat_out, osend.at[1])

    @pl.when(sp < SP - 1)
    def _():
        halo_copy.wait_send()

    sent(others, esend.at[0])


def block_shards(SP, TP, X, *args):
    tokens, lru_in, gate_in, query_w = args[:4]
    (conv_weight, rg_w, ig_w, rate, decay_extra, forget, out_lru, out_fox) = args[6:]
    rows, dcols = tokens.shape
    D, lw = lru_in.shape
    fw = query_w.shape[1]
    oc = out_lru.shape[1] // TP
    tot = 2 * lw + 3 * fw
    H = fw // HEAD_DIM
    CH = 4
    rc = rows // CH
    bw = rg_w.shape[1]
    hbm = pl.BlockSpec(memory_space=pl.ANY)
    dma = pltpu.SemaphoreType.DMA
    V = pltpu.VMEM
    scratch = [
        V((TP, rows, dcols), BF16),
        V((D, tot), BF16),
        V((2, rc, tot), F32),
        V((2, rc, 1), F32),
        V((rows, lw), BF16),
        V((16, lw), BF16),
        V((rows + 8, lw), F32),
        V(conv_weight.shape, BF16),
        V((lw // bw, bw, bw), BF16),
        V((lw // bw, bw, bw), BF16),
        V((1, rate.shape[0]), F32),
        V((H, rows), F32),
        V((lw, lw), BF16),
        V((lw, lw), BF16),
        V((rows, lw), BF16),
        V((rows, fw), BF16),
        V((rows, lw), F32),
        V((lw // 128, rows, 128), F32),
        V((lw // 128, rows, 128), F32),
        V((8, lw), F32),
        V((8, lw), F32),
        V((8, lw), F32),
        V((SP, 2, lw), F32),
        V((SP, rows, 2 * fw), BF16),
        V((SP, H, rows), F32),
        V((H, rows, 128), F32),
        V((H, rows, 2 * HEAD_DIM), F32),
        V((rows, fw), BF16),
        V((H, rows, 128), F32),
        V((H, rows, 2 * HEAD_DIM), F32),
        V((rows, fw), BF16),
        V((CH, 2 * H, rc), F32),
        V((rows, fw), BF16),
        V((CH, 2 * H, rc), F32),
        V((TP, lw, oc), BF16),
        V((TP, fw, oc), BF16),
        V((TP, rows, lw), BF16),
        V((TP, rows, fw), BF16),
        V((rows, oc), F32),
        dma((CH + 9,)),
        dma((3,)),
        dma((3, CH)),
        dma((1,)),
        dma((1,)),
        dma((1,)),
        dma((1,)),
        dma((2,)),
        dma((3,)),
        dma((1,)),
        dma((1,)),
        dma((1,)),
        dma((1,)),
        dma((3, CH)),
        dma((5,)),
        dma((2,)),
        dma((2, 2, X)),
        dma((2,)),
        dma((3,)),
        dma((3,)),
        dma((3, CH + 1)),
        dma((1,)),
        dma((2,)),
        dma((2,)),
        dma((2 * CH + 1,)),
    ]
    return pl.pallas_call(
        functools.partial(block_kernel, SP, TP, X, CH),
        out_shape=pltpu.VMEM((rows, oc), BF16),
        in_specs=[hbm] * 14,
        out_specs=pl.BlockSpec(memory_space=pltpu.VMEM),
        scratch_shapes=scratch,
        compiler_params=pltpu.CompilerParams(
            collective_id=1, has_side_effects=True, vmem_limit_bytes=60 * 1024 * 1024
        ),
    )(*args[:9], rate.reshape(1, -1), decay_extra, forget.T, out_lru, out_fox)


def columns_of(mesh):
    SP = mesh.shape["sp"]
    try:
        X = len({d.coords[0] for d in mesh.devices.flat})
    except AttributeError:
        X = 2
    return X if SP % X == 0 else 1


def solution(mesh):
    placed = (
        P("sp", "tp"),
        P(None, "tp"),
        P(None, "tp"),
        P(None, "tp"),
        P(None, "tp"),
        P(None, "tp"),
        P(),
        P(),
        P(),
        P(),
        P("sp", "tp"),
        P("sp", "tp"),
        P("tp", None),
        P("tp", None),
    )
    SP, TP, X = mesh.shape["sp"], mesh.shape["tp"], columns_of(mesh)
    small = X == 2 and TP == 4 and SP // X == 4
    body = functools.partial(block_shards if small else shards, SP, TP, X)
    return jax.shard_map(
        body, mesh=mesh, in_specs=placed, out_specs=P("sp", "tp"), check_vma=False
    )
```

```python
import functools

import jax
import jax.numpy as jnp
from jax import lax
from jax.experimental import pallas as pl
from jax.experimental.pallas import tpu as pltpu
from jax.sharding import PartitionSpec as P

HEAD_DIM = 128
decay_sharpness = 8.0
epsilon_norm = 1e-06
MESH = pl.DeviceIdType.MESH
F32 = jnp.float32
BF16 = jnp.bfloat16


def one_minus_exp(w):
    u = -w
    series = 1.0 - u / 9.0
    for n in range(8, 1, -1):
        series = 1.0 - u / n * series
    return jnp.where(u < 0.5, u * series, 1.0 - jnp.exp(w))


def remote(src, dst, send_sem, recv_sem, device):
    return pltpu.make_async_remote_copy(
        src_ref=src,
        dst_ref=dst,
        send_sem=send_sem,
        recv_sem=recv_sem,
        device_id=device,
        device_id_type=MESH,
    )


def kernel(
    SP,
    TP,
    X,
    tokens,
    lru_in,
    gate_in,
    query_w,
    key_w,
    value_w,
    conv_w,
    rg_w,
    ig_w,
    rate,
    decay_extra,
    forget,
    out_lru,
    out_fox,
    out,
    tok_buf,
    w_buf,
    acc,
    sq,
    lru_ref,
    halo,
    pad,
    bd_r,
    bd_i,
    gate_ref,
    q_ref,
    decay_buf,
    prefix_ref,
    local_ref,
    ends,
    incoming,
    kv_buf,
    cum_buf,
    cum_pad,
    wide,
    fcol,
    m_ref,
    l_ref,
    o_ref,
    q_far,
    m_far,
    l_far,
    o_far,
    part_out,
    stat_out,
    part_in,
    stat_in,
    wl_buf,
    wf_buf,
    br_lru,
    br_fox,
    oacc,
    load_sem,
    tsend,
    tfwd,
    trecv,
    hsend,
    hrecv,
    esend,
    erecv,
    zsend,
    xsend,
    kvrecv,
    wsend,
    wrecv,
    lsend,
    lrecv,
    fsend,
    ffwd,
    frecv,
    lfwd,
    qsend,
    qrecv,
    osend,
    orecv,
):
    rows, dcols = tokens.shape
    D, lw = lru_in.shape
    fw = query_w.shape[1]
    H = fw // HEAD_DIM
    oc = out.shape[1]
    Y = TP // 2
    Z = SP // X
    CH = tsend.shape[1]
    rc = rows // CH
    sp = lax.axis_index("sp")
    tp = lax.axis_index("tp")
    z = lax.div(sp, X)
    x = lax.rem(sp, X)
    partner = tp + 1 - 2 * lax.rem(tp, 2)
    far = [lax.rem(tp + 2 * k, TP) for k in range(Y)]
    pfar = [lax.rem(partner + 2 * k, TP) for k in range(Y)]
    offs = [0, lw, lw + fw, lw + 2 * fw, 2 * lw + 2 * fw, 2 * lw + 3 * fw]

    barrier = pltpu.get_barrier_semaphore()
    for k in range(1, SP):
        pl.semaphore_signal(
            barrier, inc=1, device_id={"sp": lax.rem(sp + k, SP)}, device_id_type=MESH
        )
    for k in range(1, TP):
        pl.semaphore_signal(
            barrier, inc=1, device_id={"tp": lax.rem(tp + k, TP)}, device_id_type=MESH
        )
    loads = []
    for i, w in enumerate((lru_in, key_w, value_w, gate_in, query_w)):
        c = pltpu.make_async_copy(w, w_buf.at[:, offs[i] : offs[i + 1]], load_sem.at[i])
        c.start()
        loads.append(c)
    mine = pl.ds(pl.multiple_of(tp * oc, 128), oc)
    own_loads = [
        pltpu.make_async_copy(decay_extra, decay_buf, load_sem.at[5]),
        pltpu.make_async_copy(out_lru.at[:, mine], wl_buf.at[tp], load_sem.at[6]),
        pltpu.make_async_copy(out_fox.at[:, mine], wf_buf.at[tp], load_sem.at[7]),
    ]
    for c in own_loads:
        c.start()
    pl.semaphore_wait(barrier, SP - 1 + TP - 1)

    pending = []

    def chunk(c):
        return pl.ds(c * rc, rc)

    for c in range(CH):
        for k in range(1, Y):
            s = remote(
                tokens.at[chunk(c)],
                tok_buf.at[tp, chunk(c)],
                tsend.at[k, c],
                trecv.at[tp, c],
                {"tp": far[k]},
            )
            s.start()
            pending.append(s)
    for c in range(CH):
        s = remote(
            tokens.at[chunk(c)],
            tok_buf.at[tp, chunk(c)],
            tsend.at[0, c],
            trecv.at[tp, c],
            {"tp": partner},
        )
        s.start()
        pending.append(s)

    bw = rg_w.shape[1]
    nb = lw // bw
    bd_r[...] = jnp.zeros_like(bd_r)
    bd_i[...] = jnp.zeros_like(bd_i)
    for n in range(nb):
        sl = pl.ds(n * bw, bw)
        bd_r[sl, sl] = rg_w[tp * nb + n]
        bd_i[sl, sl] = ig_w[tp * nb + n]
    cum_pad[...] = jnp.zeros_like(cum_pad)
    wide[...] = jnp.zeros_like(wide)
    wide[0:H, :] = forget[...]
    fcol[...] = wide[...].T
    cum_buf[sp] = wide[0:8, :]

    for c in loads:
        c.wait()

    def project(val, src, r, first=False):
        w_rows = pl.ds(pl.multiple_of(src * dcols, dcols), dcols)
        v32 = val.astype(F32)
        part = jnp.sum(v32 * v32, axis=1, keepdims=True)
        dot = jnp.dot(val, w_buf[w_rows, :], preferred_element_type=F32)
        if first:
            sq[r, :] = part
            acc[r, :] = dot
        else:
            sq[r, :] += part
            acc[r, :] += dot

    def tok_wait(src, c):
        ref = tok_buf.at[src, chunk(c)]
        remote(ref, ref, tsend.at[0, c], trecv.at[src, c], {"tp": partner}).wait_recv()

    for c in range(CH):
        project(tokens[chunk(c), :], tp, chunk(c), True)
    for c in range(CH):
        tok_wait(partner, c)
        project(tok_buf[partner, chunk(c), :], partner, chunk(c))
    for c in range(CH):
        for k in range(1, Y):
            tok_wait(far[k], c)
            ref = tok_buf.at[far[k], chunk(c)]
            s = remote(ref, ref, tfwd.at[k, c], trecv.at[far[k], c], {"tp": partner})
            s.start()
            pending.append(s)
            project(tok_buf[far[k], chunk(c), :], far[k], chunk(c))
        for k in range(1, Y):
            tok_wait(pfar[k], c)
            project(tok_buf[pfar[k], chunk(c), :], pfar[k], chunk(c))

    row_scale = lax.rsqrt(sq[...] / D + epsilon_norm)

    def scaled(i, n=1):
        return (acc[:, offs[i] : offs[i + n]] * row_scale).astype(BF16)

    lru_ref[...] = scaled(0)
    hb = halo.shape[0]
    halo_copy = remote(
        lru_ref.at[pl.ds(rows - hb, hb)],
        halo,
        hsend.at[0],
        hrecv.at[0],
        {"sp": lax.rem(sp + 1, SP)},
    )

    @pl.when(sp < SP - 1)
    def _():
        halo_copy.start()

    kv_buf[sp] = scaled(1, 2)

    paired = Z in (3, 4)
    helper = jnp.logical_and(z <= Z - 3, paired)
    helped = jnp.logical_and(z >= 2, paired)

    def block_copies(j, a, send_sem, device):
        return (
            remote(kv_buf.at[j], kv_buf.at[j], send_sem.at[a, 0], kvrecv.at[j, 0], device),
            remote(cum_buf.at[j], cum_buf.at[j], send_sem.at[a, 1], kvrecv.at[j, 1], device),
        )

    def z_copies(dz):
        j = (z - dz) * X + x
        return block_copies(j, dz, zsend, {"sp": lax.rem(sp + X, SP)})

    def x_copies(dz, dx):
        j = (z - dz) * X + x
        xo = lax.rem(x + dx, X)
        return block_copies(j, dz, xsend.at[dx - 1], {"sp": z * X + xo})

    def for_sends(dz, own, act):
        if own or not paired:

            @pl.when(z < Z - 1)
            def _():
                for c in z_copies(dz):
                    act(c)

        for dx in range(1, X):
            if own:

                @pl.when(jnp.logical_or(lax.rem(x + dx, X) > x, helper))
                def _():
                    for c in x_copies(dz, dx):
                        act(c)
            else:
                for c in x_copies(dz, dx):
                    act(c)

    def kv_wait(j):
        for c in block_copies(j, 0, zsend, {"sp": lax.rem(sp + X, SP)}):
            c.wait_recv()

    for_sends(0, True, lambda c: c.start())

    q_ref[...] = scaled(4)
    q_copy = remote(
        q_ref, q_far, qsend.at[0], qrecv.at[0], {"sp": lax.rem(sp + SP - 2 * X, SP)}
    )

    @pl.when(helped)
    def _():
        q_copy.start()

    for i, (w, buf) in enumerate(((out_lru, wl_buf), (out_fox, wf_buf))):
        for k in range(1, TP):
            t = lax.rem(tp + k, TP)
            cols = pl.ds(pl.multiple_of(t * oc, 128), oc)
            s = remote(w.at[:, cols], buf.at[tp], wsend.at[i, k], wrecv.at[i, tp], {"tp": t})
            s.start()
            pending.append(s)

    gate_ref[...] = scaled(3)

    @pl.when(sp == 0)
    def _():
        pad[0:8, :] = jnp.zeros((8, lw), F32)

    @pl.when(sp > 0)
    def _():
        halo_copy.wait_recv()
        pad[0:8, :] = halo[...].astype(F32)[hb - 8 : hb, :]

    pad[8 : 8 + rows, :] = lru_ref[...].astype(F32)
    chans = pl.ds(pl.multiple_of(tp * lw, 128), lw)
    taps = conv_w.shape[0]
    taps_f32 = conv_w[:, chans].astype(F32)
    conv = jnp.zeros((rows, lw), F32)
    for j in range(taps):
        conv = conv + taps_f32[j : j + 1, :] * pad[8 - (taps - 1) + j : 8 - (taps - 1) + j + rows, :]
    conv_b = conv.astype(BF16)

    def sigmoid(v):
        return 1.0 / (1.0 + jnp.exp(-v))

    recur_gate = sigmoid(jnp.dot(conv_b, bd_r[...], preferred_element_type=F32))
    input_gate = sigmoid(jnp.dot(conv_b, bd_i[...], preferred_element_type=F32))
    own_rate = rate[:, chans]
    softplus = jnp.maximum(-own_rate, 0.0) + jnp.log1p(jnp.exp(-jnp.abs(own_rate)))
    for c in own_loads:
        c.wait()
    log_decay = -decay_sharpness * softplus * recur_gate + decay_buf[...]
    prefix_ref[...] = jnp.exp(log_decay)
    local_ref[...] = jnp.sqrt(one_minus_exp(2.0 * log_decay)) * input_gate * conv_b.astype(F32)
    row_id = lax.broadcasted_iota(jnp.int32, (rows, lw), 0)
    step = 1
    while step < rows:
        a = prefix_ref[...]
        b = local_ref[...]
        keep = row_id >= step
        a_prev = jnp.where(keep, pltpu.roll(a, step, 0), 1.0)
        b_prev = jnp.where(keep, pltpu.roll(b, step, 0), 0.0)
        local_ref[...] = b + a * b_prev
        prefix_ref[...] = a * a_prev
        step *= 2
    ends[sp, 0:1, :] = prefix_ref[rows - 1 : rows, :]
    ends[sp, 1:2, :] = local_ref[rows - 1 : rows, :]

    def end_copy(k):
        return remote(
            ends.at[sp], ends.at[sp], esend.at[k], erecv.at[sp], {"sp": lax.rem(sp + k, SP)}
        )

    for k in range(1, SP):

        @pl.when(sp + k < SP)
        def _():
            end_copy(k).start()

    score_scale = HEAD_DIM ** (-0.5)
    qc = rows // 2

    def attend(j, diagonal, far_first=None):
        other = far_first is not None
        first = diagonal or far_first
        qs, ms, ls, os = (q_far, m_far, l_far, o_far) if other else (q_ref, m_ref, l_ref, o_ref)

        def some(i, carry):
            r = pl.ds(pl.multiple_of(i * qc, qc), qc)
            for h in range(H):
                hs = slice(h * HEAD_DIM, (h + 1) * HEAD_DIM)
                vs = slice(fw + h * HEAD_DIM, fw + (h + 1) * HEAD_DIM)
                s = lax.dot_general(
                    qs[r, hs],
                    kv_buf[j, :, hs],
                    (((1,), (1,)), ((), ())),
                    preferred_element_type=F32,
                )
                s = s * score_scale
                if not other:
                    s = s + fcol[r, h : h + 1]
                s = s - cum_buf[j, h : h + 1, :]
                if diagonal:
                    causal = (
                        lax.broadcasted_iota(jnp.int32, (qc, rows), 0) + i * qc
                        >= lax.broadcasted_iota(jnp.int32, (qc, rows), 1)
                    )
                    s = jnp.where(causal, s, -1e30)
                top = jnp.max(s, axis=1, keepdims=True)
                if first:
                    p = jnp.exp(s - top)
                    ms[h, r, :] = top
                    ls[h, r, :] = jnp.sum(p, axis=1, keepdims=True)
                    os[h, r, :] = jnp.dot(
                        p.astype(BF16), kv_buf[j, :, vs], preferred_element_type=F32
                    )
                else:
                    old = ms[h, r, :]
                    new = jnp.maximum(old, top)
                    p = jnp.exp(s - new)
                    fade = jnp.exp(old - new)
                    ms[h, r, :] = new
                    ls[h, r, :] = ls[h, r, :] * fade + jnp.sum(p, axis=1, keepdims=True)
                    os[h, r, :] = os[h, r, :] * fade + jnp.dot(
                        p.astype(BF16), kv_buf[j, :, vs], preferred_element_type=F32
                    )
            return carry

        lax.fori_loop(0, rows // qc, some, 0)

    attend(sp, True)

    def row_blocks(dz):
        for dx in range(1, X):
            xo = lax.rem(x + dx, X)

            @pl.when(jnp.logical_or(dz > 0, xo < x))
            def _():
                j = (z - dz) * X + xo
                kv_wait(j)
                attend(j, False)

    def finish_lru():
        incoming[...] = jnp.zeros_like(incoming)
        for j in range(SP - 1):

            @pl.when(j < sp)
            def _():
                remote(
                    ends.at[j], ends.at[j], esend.at[0], erecv.at[j], {"sp": lax.rem(sp + 1, SP)}
                ).wait_recv()
                incoming[...] = ends[j, 0:1, :] * incoming[...] + ends[j, 1:2, :]

        states = local_ref[...] + prefix_ref[...] * incoming[...]
        g = gate_ref[...].astype(F32)
        gelu = 0.5 * g * (1.0 + jnp.tanh(0.7978845608028654 * (g + 0.044715 * (g * g * g))))
        br_lru[tp] = (states * gelu).astype(BF16)
        for k in range(Y - 1, -1, -1):
            lru_copy(k).start()

    def lru_copy(k):
        to = far[k] if k else partner
        return remote(br_lru.at[tp], br_lru.at[tp], lsend.at[k], lrecv.at[tp], {"tp": to})

    lru_step = min(2, Z - 1)
    if Z == 1:
        finish_lru()

    def hop(dz, carry):
        @pl.when(dz <= z)
        def _():
            j = (z - dz) * X + x
            kv_wait(j)
            for_sends(dz, False, lambda c: c.start())
            row_blocks(dz - 1)
            attend(j, False)

        @pl.when(dz == lru_step)
        def _():
            finish_lru()

        return carry

    up = {"sp": lax.rem(sp + 2 * X, SP)}
    part_copies = (
        remote(part_out, part_in, osend.at[0], orecv.at[0], up),
        remote(stat_out, stat_in, osend.at[1], orecv.at[1], up),
    )

    def send_partial():
        for h in range(H):
            part_out[:, h * HEAD_DIM : (h + 1) * HEAD_DIM] = o_far[h].astype(BF16)
            cum_pad[:, h : h + 1] = m_far[h]
            cum_pad[:, H + h : H + h + 1] = l_far[h]
        stat_out[...] = cum_pad[...].T[0:8, :]
        for c in part_copies:
            c.start()

    if paired:
        below = (z - 1) * X

        @pl.when(helper)
        def _():
            q_copy.wait_recv()
            attend(sp, False, True)

        @pl.when(z >= 1)
        def _():
            kv_wait(below + x)
            for_sends(1, False, lambda c: c.start())

        for dx in range(1, X):
            xo = lax.rem(x + dx, X)

            @pl.when(jnp.logical_or(xo < x, helper))
            def _():
                kv_wait(z * X + xo)

            @pl.when(helper)
            def _():
                attend(z * X + xo, False, False)

        @pl.when(jnp.logical_and(helper, z == 0))
        def _():
            send_partial()

        for dx in range(1, X):
            xo = lax.rem(x + dx, X)

            @pl.when(xo < x)
            def _():
                attend(z * X + xo, False)

        finish_lru()

        @pl.when(jnp.logical_and(helper, z >= 1))
        def _():
            attend(below + x, False, False)

        @pl.when(z >= 1)
        def _():
            attend(below + x, False)
            for dx in range(1, X):
                j = below + lax.rem(x + dx, X)
                kv_wait(j)

                @pl.when(helper)
                def _():
                    attend(j, False, False)

            @pl.when(helper)
            def _():
                send_partial()

            for dx in range(1, X):
                attend(below + lax.rem(x + dx, X), False)

    else:
        lax.fori_loop(1, Z, hop, 0)

    def lru_wait(t):
        remote(br_lru.at[t], br_lru.at[t], lsend.at[0], lrecv.at[t], {"tp": partner}).wait_recv()

    def lru_dot(t):
        return jnp.dot(br_lru[t], wl_buf[t], preferred_element_type=F32)

    oacc[...] = lru_dot(tp)
    for k in range(1, TP):
        t = lax.rem(tp + k, TP)
        for i, buf in enumerate((wl_buf, wf_buf)):
            remote(buf.at[t], buf.at[t], wsend.at[i, k], wrecv.at[i, t], {"tp": t}).wait_recv()
    for k in range(1, Y):
        lru_wait(far[k])
        ref = br_lru.at[far[k]]
        s = remote(ref, ref, lfwd.at[k], lrecv.at[far[k]], {"tp": partner})
        s.start()
        pending.append(s)
    lru_wait(partner)
    oacc[...] += lru_dot(partner)
    for k in range(1, Y):
        oacc[...] += lru_dot(far[k])
        lru_wait(pfar[k])
        oacc[...] += lru_dot(pfar[k])

    if paired:

        @pl.when(helped)
        def _():
            for c in part_copies:
                c.wait_recv()
            wide[0:8, :] = stat_in[...]
            stats = wide[...].T
            for h in range(H):
                m_in = stats[:, h : h + 1] + fcol[:, h : h + 1]
                l_in = stats[:, H + h : H + h + 1]
                part = part_in[:, h * HEAD_DIM : (h + 1) * HEAD_DIM].astype(F32)
                new = jnp.maximum(m_ref[h], m_in)
                fade = jnp.exp(m_ref[h] - new)
                grow = jnp.exp(m_in - new)
                l_ref[h] = l_ref[h] * fade + l_in * grow
                o_ref[h] = o_ref[h] * fade + part * grow

    else:
        row_blocks(z)

    for c in range(CH):
        r = chunk(c)
        for h in range(H):
            br_fox[tp, r, h * HEAD_DIM : (h + 1) * HEAD_DIM] = (
                o_ref[h, r, :] / l_ref[h, r, :]
            ).astype(BF16)
        ref = br_fox.at[tp, r]
        for k in list(range(1, Y)) + [0]:
            to = far[k] if k else partner
            s = remote(ref, ref, fsend.at[k, c], frecv.at[tp, c], {"tp": to})
            s.start()
            pending.append(s)

    def fox_wait(src, c):
        ref = br_fox.at[src, chunk(c)]
        remote(ref, ref, fsend.at[0, c], frecv.at[src, c], {"tp": partner}).wait_recv()

    def fox_dot(src, r):
        return jnp.dot(br_fox[src, r, :], wf_buf[src], preferred_element_type=F32)

    for c in range(CH):
        fox_wait(partner, c)
        oacc[chunk(c), :] += fox_dot(tp, chunk(c)) + fox_dot(partner, chunk(c))
    for c in range(CH):
        r = chunk(c)
        for k in range(1, Y):
            fox_wait(far[k], c)
            ref = br_fox.at[far[k], r]
            s = remote(ref, ref, ffwd.at[k, c], frecv.at[far[k], c], {"tp": partner})
            s.start()
            pending.append(s)
            oacc[r, :] += fox_dot(far[k], r)
        for k in range(1, Y):
            fox_wait(pfar[k], c)
            oacc[r, :] += fox_dot(pfar[k], r)
        out[r, :] = oacc[r, :].astype(out.dtype)

    for s in pending:
        s.wait_send()
    for k in range(Y):
        lru_copy(k).wait_send()

    @pl.when(helped)
    def _():
        q_copy.wait_send()

    @pl.when(helper)
    def _():
        for c in part_copies:
            c.wait_send()

    @pl.when(sp < SP - 1)
    def _():
        halo_copy.wait_send()

    for k in range(1, SP):

        @pl.when(sp + k < SP)
        def _():
            end_copy(k).wait_send()

    for_sends(0, True, lambda c: c.wait_send())

    def drain(dz, carry):
        @pl.when(dz <= z)
        def _():
            for_sends(dz, False, lambda c: c.wait_send())

        return carry

    if paired:

        @pl.when(z >= 1)
        def _():
            for_sends(1, False, lambda c: c.wait_send())

    else:
        lax.fori_loop(1, Z, drain, 0)


def shards(SP, TP, X, *args):
    tokens, lru_in, gate_in, query_w = args[:4]
    (conv_weight, rg_w, ig_w, rate, decay_extra, forget, out_lru, out_fox) = args[6:]
    rows, dcols = tokens.shape
    D, lw = lru_in.shape
    fw = query_w.shape[1]
    oc = out_lru.shape[1] // TP
    tot = 2 * lw + 3 * fw
    H = fw // HEAD_DIM
    Y = TP // 2
    Z = SP // X
    CH = 4
    vm = pl.BlockSpec(memory_space=pltpu.VMEM)
    hbm = pl.BlockSpec(memory_space=pl.ANY)
    dma = pltpu.SemaphoreType.DMA
    V = pltpu.VMEM
    scratch = [
        V((TP, rows, dcols), BF16),
        V((D, tot), BF16),
        V((rows, tot), F32),
        V((rows, 1), F32),
        V((rows, lw), BF16),
        V((16, lw), BF16),
        V((rows + 8, lw), F32),
        V((lw, lw), BF16),
        V((lw, lw), BF16),
        V((rows, lw), BF16),
        V((rows, fw), BF16),
        V((rows, lw), F32),
        V((rows, lw), F32),
        V((rows, lw), F32),
        V((SP, 8, lw), F32),
        V((1, lw), F32),
        V((SP, rows, 2 * fw), BF16),
        V((SP, 8, rows), F32),
        V((rows, 128), F32),
        V((128, rows), F32),
        V((rows, 128), F32),
        V((H, rows, 1), F32),
        V((H, rows, 1), F32),
        V((H, rows, HEAD_DIM), F32),
        V((rows, fw), BF16),
        V((H, rows, 1), F32),
        V((H, rows, 1), F32),
        V((H, rows, HEAD_DIM), F32),
        V((rows, fw), BF16),
        V((8, rows), F32),
        V((rows, fw), BF16),
        V((8, rows), F32),
        V((TP, lw, oc), BF16),
        V((TP, fw, oc), BF16),
        V((TP, rows, lw), BF16),
        V((TP, rows, fw), BF16),
        V((rows, oc), F32),
        dma((8,)),
        dma((Y, CH)),
        dma((Y, CH)),
        dma((TP, CH)),
        dma((1,)),
        dma((1,)),
        dma((SP,)),
        dma((SP,)),
        dma((Z, 2)),
        dma((max(X - 1, 1), Z, 2)),
        dma((SP, 2)),
        dma((2, TP)),
        dma((2, TP)),
        dma((TP,)),
        dma((TP,)),
        dma((Y, CH)),
        dma((Y, CH)),
        dma((TP, CH)),
        dma((Y,)),
        dma((1,)),
        dma((1,)),
        dma((2,)),
        dma((2,)),
    ]
    return pl.pallas_call(
        functools.partial(kernel, SP, TP, X),
        out_shape=jax.ShapeDtypeStruct((rows, oc), BF16),
        in_specs=[vm] + [hbm] * 5 + [vm] * 4 + [hbm, vm, hbm, hbm],
        out_specs=vm,
        scratch_shapes=scratch,
        compiler_params=pltpu.CompilerParams(
            collective_id=0, has_side_effects=True, vmem_limit_bytes=60 * 1024 * 1024
        ),
    )(*args[:9], rate.reshape(1, -1), decay_extra, forget.T, out_lru, out_fox)


LOG2E = 1.4426950408889634


def block_kernel(
    SP,
    TP,
    X,
    CH,
    tokens,
    lru_in,
    gate_in,
    query_w,
    key_w,
    value_w,
    conv_w,
    rg_w,
    ig_w,
    rate,
    decay_extra,
    forget,
    out_lru,
    out_fox,
    out,
    tok_buf,
    w_buf,
    acc,
    sq,
    lru_ref,
    halo,
    pad,
    conv_v,
    rg_v,
    ig_v,
    rate_v,
    forget_v,
    bd_r,
    bd_i,
    gate_ref,
    q_ref,
    decay_buf,
    prefix_ref,
    local_ref,
    seg_a,
    seg_b,
    carry_ref,
    ends,
    kv_buf,
    cum_buf,
    m_ref,
    o_ref,
    q_far,
    m_far,
    o_far,
    part_out,
    stat_out,
    part_in,
    stat_in,
    wl_buf,
    wf_buf,
    br_lru,
    br_fox,
    oacc,
    load_sem,
    tsend,
    trecv,
    hsend,
    hrecv,
    esend,
    erecv,
    csend,
    crecv,
    zsend,
    xsend,
    zfwd,
    xfwd,
    kvrecv,
    wsend,
    wrecv_own,
    wrecv,
    lsend,
    lrecv,
    fsend,
    frecv,
    qsend,
    qrecv,
    osend,
    orecv,
):
    rows, dcols = tokens.shape
    D, lw = lru_in.shape
    fw = query_w.shape[1]
    H = fw // HEAD_DIM
    oc = out.shape[1]
    Z = SP // X
    rc = rows // CH
    half = rows // 2
    wh = out_lru.shape[0] // X
    sp = lax.axis_index("sp")
    tp = lax.axis_index("tp")
    z = lax.div(sp, X)
    x = lax.rem(sp, X)
    xo = 1 - x
    y = lax.div(tp, 2)
    partner = tp + 1 - 2 * lax.rem(tp, 2)
    far = lax.rem(tp + 2, TP)
    pfar = lax.rem(partner + 2, TP)
    j_xo = z * X + xo
    to_xo = {"sp": j_xo}
    to_up = {"sp": lax.rem(sp + X, SP)}
    j_b = lax.rem(sp + SP - X, SP)
    j_bo = lax.rem(j_xo + SP - X, SP)
    helper = z <= Z - 3
    helped = z >= 2
    not_top = z < Z - 1
    above0 = z >= 1
    order = list(range(CH - 1, -1, -1))
    second_top = z == Z - 2
    last = order[3]
    last_climbs = jnp.logical_and(not_top, z != Z - 3)
    last_crosses = jnp.logical_and(above0, not_top)
    climbs = {order[1]: not_top, last: last_climbs}
    crosses = {order[0]: above0, order[2]: above0, last: last_crosses}
    whalf = lax.rem(x + z, X)
    top = z == Z - 1
    PARTNER, FAR, PFAR = 0, 1, 2
    ACROSS, BELOW, DIAG = 0, 1, 2
    score_k = HEAD_DIM ** (-0.5) * LOG2E

    def chunk(c):
        return pl.ds(c * rc, rc)

    pieces = [(c * rc, rc) for c in range(CH - 1)]
    pieces += [(rows - rc, rc // 2), (rows - rc // 2, rc // 2)]
    PC = len(pieces)

    def piece(k):
        return pl.ds(*pieces[k])

    def pieces_of(c):
        return [k for k, (at, n) in enumerate(pieces) if at // rc == c]

    barrier = pltpu.get_barrier_semaphore()
    for k in range(1, SP):
        pl.semaphore_signal(
            barrier, inc=1, device_id={"sp": lax.rem(sp + k, SP)}, device_id_type=MESH
        )
    for k in range(1, TP):
        pl.semaphore_signal(
            barrier, inc=1, device_id={"tp": lax.rem(tp + k, TP)}, device_id_type=MESH
        )

    def load(i, src, dst):
        c = pltpu.make_async_copy(src, dst, load_sem.at[i])
        c.start()
        return c

    tok_loads = [
        load(n, tokens.at[chunk(c)], tok_buf.at[tp, chunk(c)]) for n, c in enumerate(order)
    ]
    cols = (0, fw, 2 * fw, 2 * fw + lw, 3 * fw + lw, 3 * fw + 2 * lw)
    for i, w in enumerate((key_w, value_w, lru_in, query_w, gate_in)):
        load(CH, w, w_buf.at[:, cols[i] : cols[i + 1]])
    mine = pl.ds(pl.multiple_of(tp * oc, 128), oc)
    bw = rg_w.shape[1]
    nb = lw // bw
    gates = pl.ds(tp * nb, nb)
    forget_load = load(CH + 1, forget, forget_v)
    small_loads = [
        load(CH + 2, conv_w, conv_v),
        load(CH + 3, rg_w.at[gates], rg_v),
        load(CH + 4, ig_w.at[gates], ig_v),
        load(CH + 5, rate, rate_v),
        load(CH + 6, decay_extra, decay_buf),
    ]
    own_loads = [
        load(CH + 7, out_lru.at[:, mine], wl_buf.at[tp]),
        load(CH + 8, out_fox.at[:, mine], wf_buf.at[tp]),
    ]
    pl.semaphore_wait(barrier, SP - 1 + TP - 1)

    def send(ref, send_sem, recv_sem, device):
        remote(ref, ref, send_sem, recv_sem, device).start()

    def arrived(ref, recv_sem):
        remote(ref, ref, recv_sem, recv_sem, to_xo).wait_recv()

    def sent(ref, send_sem):
        remote(ref, ref, send_sem, send_sem, to_xo).wait_send()

    for n, c in enumerate(order):
        tok_loads[n].wait()
        ref = tok_buf.at[tp, chunk(c)]
        send(ref, tsend.at[0], trecv.at[FAR, c], {"tp": far})
        send(ref, tsend.at[1], trecv.at[PARTNER, c], {"tp": partner})

    forget_load.wait()
    cum_buf[sp] = forget_v[...] * LOG2E
    own_cum = cum_buf.at[sp]
    send(own_cum, csend.at[0], crecv.at[ACROSS], to_xo)

    @pl.when(not_top)
    def _():
        send(own_cum, csend.at[1], crecv.at[BELOW], to_up)
        send(own_cum, csend.at[1], crecv.at[DIAG], {"sp": lax.rem(j_xo + X, SP)})

    for c in small_loads:
        c.wait()
    bd_r[...] = jnp.zeros_like(bd_r)
    bd_i[...] = jnp.zeros_like(bd_i)
    for n in range(nb):
        sl = pl.ds(n * bw, bw)
        bd_r[sl, sl] = rg_v[n]
        bd_i[sl, sl] = ig_v[n]
    pltpu.make_async_copy(w_buf, w_buf, load_sem.at[CH]).wait()

    def tok_wait(src, role, c):
        arrived(tok_buf.at[src, chunk(c)], trecv.at[role, c])

    def features(side, c):
        first = 2 * side
        return jnp.concatenate([tok_buf[first, chunk(c), :], tok_buf[first + 1, chunk(c), :]], axis=1)

    def w_rows(side):
        return pl.ds(pl.multiple_of(side * 2 * dcols, 2 * dcols), 2 * dcols)

    def squares(v):
        v32 = v.astype(F32)
        return jnp.sum(v32 * v32, axis=1, keepdims=True)

    def near_part(c, slot):
        tok_wait(partner, PARTNER, c)
        v = features(y, c)
        sq[slot] = squares(v)
        acc[slot] = jnp.dot(v, w_buf[w_rows(y), :], preferred_element_type=F32)

    halo_copy = remote(
        lru_ref.at[pl.ds(rows - halo.shape[0], halo.shape[0])],
        halo,
        hsend.at[0],
        hrecv.at[0],
        {"sp": lax.rem(sp + 1, SP)},
    )

    def kv_send(j, c, send_sem, role, device):
        send(kv_buf.at[j, chunk(c)], send_sem.at[0], kvrecv.at[role, c], device)

    def kv_wait(j, c, role):
        arrived(kv_buf.at[j, chunk(c)], kvrecv.at[role, c])

    def all_across(own_x):
        return jnp.logical_or(own_x, helper)

    def across(own_x, c):
        need = all_across(own_x)
        return jnp.logical_or(need, climbs[c]) if c in climbs else need

    def q_copy(c):
        return remote(
            q_ref.at[chunk(c)],
            q_far.at[chunk(c)],
            qsend.at[0],
            qrecv.at[0 if c in order[0:2] else 1],
            {"sp": lax.rem(sp + SP - 2 * X, SP)},
        )

    def far_part(i, c, slot):
        tok_wait(far, FAR, c)
        send(tok_buf.at[far, chunk(c)], tsend.at[2], trecv.at[PFAR, c], {"tp": partner})
        if i + 1 < CH:
            near_part(order[i + 1], 1 - slot)
        tok_wait(pfar, PFAR, c)
        if i == CH - 1:
            send_weights()
        v = features(1 - y, c)
        row_scale = lax.rsqrt((sq[slot] + squares(v)) / D + epsilon_norm)

        def part(a, b):
            w = w_buf[w_rows(1 - y), cols[a] : cols[b]]
            both = acc[slot, :, cols[a] : cols[b]] + jnp.dot(v, w, preferred_element_type=F32)
            return (both * row_scale).astype(BF16)

        kv_buf[sp, chunk(c), :] = part(0, 2)

        @pl.when(across(x == 0, c))
        def _():
            kv_send(sp, c, xsend, ACROSS, to_xo)

        @pl.when(not_top)
        def _():
            kv_send(sp, c, zsend, BELOW, to_up)

        rest = part(2, 5)
        lru_ref[chunk(c), :] = rest[:, 0:lw]
        q_ref[chunk(c), :] = rest[:, lw : lw + fw]
        gate_ref[chunk(c), :] = rest[:, lw + fw :]

        @pl.when(helped)
        def _():
            q_copy(c).start()

        if i == 0:

            @pl.when(sp < SP - 1)
            def _():
                halo_copy.start()

    banks = ((out_lru, wl_buf), (out_fox, wf_buf))

    def send_weights():
        r = pl.ds(pl.multiple_of(whalf * wh, wh), wh)

        def over_y(n):
            w, buf = banks[n]
            for role, t in ((FAR, far), (PFAR, pfar)):
                c = pl.ds(pl.multiple_of(t * oc, 128), oc)
                remote(
                    w.at[r, c], buf.at[tp, r], wsend.at[n], wrecv.at[n, role - 1, whalf], {"tp": t}
                ).start()

        pl.when(above0)(lambda: over_y(0))
        over_y(1)
        c = pl.ds(pl.multiple_of(partner * oc, 128), oc)
        for n, (w, buf) in enumerate(banks):
            remote(w.at[:, c], buf.at[tp], wsend.at[2], wrecv_own.at[n], {"tp": partner}).start()

    def weight_part(n, role, k):
        t = far if role == FAR else pfar
        ref = banks[n][1].at[t, pl.ds(pl.multiple_of(k * wh, wh), wh)]
        return ref, wrecv.at[n, role - 1, k]

    def weight_pass(n, role):
        ref, sem = weight_part(n, role, whalf)

        def take():
            arrived(ref, sem)

        if n == 0:
            pl.when(above0)(take)
        else:
            take()

        @pl.when(above0)
        def _():
            send(ref, wsend.at[3], sem, {"sp": lax.rem(sp + SP - X, SP)})

        @pl.when(top)
        def _():
            send(ref, wsend.at[4], sem, to_xo)

    def weight_pass_bottom(role):
        @pl.when(z == 0)
        def _():
            ref, sem = weight_part(0, role, 1 - whalf)
            arrived(ref, sem)
            send(ref, wsend.at[4], sem, to_xo)

    def weight_wait(n, role):
        k = 1 - whalf
        if n == 0:
            k = jnp.where(z == 0, whalf, k)
        arrived(*weight_part(n, role, k))

    def pass_up(c):
        @pl.when(climbs[c])
        def _():
            kv_wait(j_xo, c, ACROSS)
            kv_send(j_xo, c, zfwd, DIAG, to_up)

    def pass_across(c):
        @pl.when(crosses[c])
        def _():
            kv_wait(j_b, c, BELOW)
            kv_send(j_b, c, xfwd, DIAG, to_xo)

    cut = rc - rc // 4

    def half_ref(j, upper_part):
        at, n = (cut, rc - cut) if upper_part else (0, cut)
        return kv_buf.at[j, pl.ds(last * rc + at, n)]

    def half_sem(upper_part):
        return kvrecv.at[DIAG, last] if upper_part else kvrecv.at[DIAG, CH]

    def pass_up_last():
        @pl.when(last_climbs)
        def _():
            kv_wait(j_xo, last, ACROSS)
            send(half_ref(j_xo, True), zfwd.at[0], half_sem(True), to_up)

        @pl.when(second_top)
        def _():
            send(half_ref(j_xo, False), zfwd.at[0], half_sem(False), to_up)

    def pass_across_last():
        @pl.when(last_crosses)
        def _():
            kv_wait(j_b, last, BELOW)
            send(half_ref(j_b, False), xfwd.at[0], half_sem(False), to_xo)

        @pl.when(second_top)
        def _():
            send(half_ref(j_b, True), xfwd.at[0], half_sem(True), to_xo)

    def diag_wait(c):
        if c == last:
            for upper_part in (True, False):
                arrived(half_ref(j_bo, upper_part), half_sem(upper_part))
        else:
            kv_wait(j_bo, c, DIAG)

    near_part(order[0], 0)
    for i, c in enumerate(order):
        far_part(i, c, i % 2)

    pass_across(order[0])
    pass_up(order[1])

    @pl.when(sp == 0)
    def _():
        pad[0:8, :] = jnp.zeros((8, lw), F32)

    @pl.when(sp > 0)
    def _():
        halo_copy.wait_recv()
        hb = halo.shape[0]
        pad[0:8, :] = halo[...].astype(F32)[hb - 8 : hb, :]

    pad[8 : 8 + rows, :] = lru_ref[...].astype(F32)
    chans = pl.ds(pl.multiple_of(tp * lw, 128), lw)
    taps = conv_w.shape[0]
    taps_f32 = conv_v[:, chans].astype(F32)
    conv = jnp.zeros((rows, lw), F32)
    for j in range(taps):
        conv = conv + taps_f32[j : j + 1, :] * pad[8 - (taps - 1) + j : 8 - (taps - 1) + j + rows, :]
    conv_b = conv.astype(BF16)

    def sigmoid(v):
        return 1.0 / (1.0 + jnp.exp(-v))

    recur_gate = sigmoid(jnp.dot(conv_b, bd_r[...], preferred_element_type=F32))
    input_gate = sigmoid(jnp.dot(conv_b, bd_i[...], preferred_element_type=F32))
    own_rate = rate_v[:, chans]
    softplus = jnp.maximum(-own_rate, 0.0) + jnp.log1p(jnp.exp(-jnp.abs(own_rate)))
    log_decay = -decay_sharpness * softplus * recur_gate + decay_buf[...]
    decay = jnp.exp(log_decay)
    driven = jnp.sqrt(one_minus_exp(2.0 * log_decay)) * input_gate * conv_b.astype(F32)
    for n in range(lw // 128):
        prefix_ref[n] = decay[:, n * 128 : (n + 1) * 128]
        local_ref[n] = driven[:, n * 128 : (n + 1) * 128]

    segs = 8
    seg_len = rows // segs
    run_a = jnp.ones((segs, lw), F32)
    run_b = jnp.zeros((segs, lw), F32)
    for i in range(seg_len):
        at = pl.ds(i, segs, stride=seg_len)
        a = [prefix_ref[n, at, :] for n in range(lw // 128)]
        b = [local_ref[n, at, :] for n in range(lw // 128)]
        a = jnp.concatenate(a, axis=1)
        b = jnp.concatenate(b, axis=1)
        run_a = run_a * a
        run_b = a * run_b + b
        for n in range(lw // 128):
            prefix_ref[n, at, :] = run_a[:, n * 128 : (n + 1) * 128]
            local_ref[n, at, :] = run_b[:, n * 128 : (n + 1) * 128]
    seg_a[...] = run_a
    seg_b[...] = run_b
    end_a = seg_a[0:1, :]
    end_b = seg_b[0:1, :]
    for i in range(1, segs):
        end_b = seg_a[i : i + 1, :] * end_b + seg_b[i : i + 1, :]
        end_a = end_a * seg_a[i : i + 1, :]
    ends[sp, 0:1, :] = end_a
    ends[sp, 1:2, :] = end_b

    def end_copy(k):
        return remote(
            ends.at[sp],
            ends.at[sp],
            esend.at[0],
            erecv.at[0],
            {"sp": lax.rem(sp + k, SP)},
        )

    for k in range(1, SP):
        end_copy(k).start()

    pass_across(order[2])

    def attend(qs, st, j, lo, hi, first=False, diagonal=False, qc=half, after=None, parts=None):
        ms, os = st
        items = [(i, h) for i in (parts or range(rows // qc)) for h in range(H)]

        def width(i):
            return (lo, (i + 1) * qc) if diagonal else (lo, hi)

        def scores(i, h):
            a, b = width(i)
            hs = slice(h * HEAD_DIM, (h + 1) * HEAD_DIM)
            s = lax.dot_general(
                qs[i * qc : (i + 1) * qc, hs],
                kv_buf[j, a:b, hs],
                (((1,), (1,)), ((), ())),
                preferred_element_type=F32,
            )
            s = s * score_k - cum_buf[j, h : h + 1, a:b]
            if diagonal:
                causal = (
                    lax.broadcasted_iota(jnp.int32, (qc, b - a), 0) + (i * qc - a)
                    >= lax.broadcasted_iota(jnp.int32, (qc, b - a), 1)
                )
                s = jnp.where(causal, s, -1e30)
            return s

        def update(i, h, s):
            a, b = width(i)
            r = slice(i * qc, (i + 1) * qc)
            top = jnp.max(s, axis=1, keepdims=True)
            if first:
                new = jnp.broadcast_to(top, (qc, 128))
            else:
                old = ms[h, r, :]
                new = jnp.maximum(old, top)
            ms[h, r, :] = new
            p = jnp.exp2(s - jnp.concatenate([new] * ((b - a) // 128), axis=1)).astype(BF16)
            v = kv_buf[j, a:b, fw + h * HEAD_DIM : fw + (h + 1) * HEAD_DIM]
            v1 = jnp.concatenate([v, jnp.ones((b - a, 128), BF16)], axis=1)
            pv = jnp.dot(p, v1, preferred_element_type=F32)
            if first:
                os[h, r, :] = pv
            else:
                fade = jnp.exp2(old - new)
                os[h, r, :] = os[h, r, :] * jnp.concatenate([fade, fade], axis=1) + pv

        s = scores(*items[0])
        for n, (i, h) in enumerate(items):
            nxt = scores(*items[n + 1]) if n + 1 < len(items) else None
            update(i, h, s)
            s = nxt
            if after is not None and h == H - 1:
                after(i)

    own_st = (m_ref, o_ref)
    far_st = (m_far, o_far)
    up2 = {"sp": lax.rem(sp + 2 * X, SP)}

    def part_copy(k):
        r = piece(k)
        return remote(part_out.at[r], part_in.at[r], osend.at[0], orecv.at[k], up2)

    def stat_copy(c):
        return remote(stat_out.at[c], stat_in.at[c], osend.at[1], orecv.at[PC + c], up2)

    def send_partial(c):
        r = slice(c * rc, (c + 1) * rc)
        lane = lax.broadcasted_iota(jnp.int32, (rc, 128), 1)
        stats = jnp.zeros((rc, 128), F32)
        for h in range(H):
            part_out[r, h * HEAD_DIM : (h + 1) * HEAD_DIM] = o_far[h, r, 0:HEAD_DIM].astype(BF16)
            stats = jnp.where(lane == h, m_far[h, r, :], stats)
            stats = jnp.where(lane == H + h, o_far[h, r, HEAD_DIM:], stats)
        stat_out[c] = stats.T[0 : 2 * H, :]
        stat_copy(c).start()
        for k in pieces_of(c):
            part_copy(k).start()

    attend(q_ref, own_st, sp, 0, rows, True, True)

    @pl.when(helper)
    def _():
        arrived(q_far.at[pl.ds(half, half)], qrecv.at[0])
        attend(q_far, far_st, sp, 0, rows, True, parts=(1,))

    pass_up_last()
    pass_across_last()

    weight_pass(0, FAR)
    arrived(cum_buf.at[j_xo], crecv.at[ACROSS])

    for c in order:
        need = all_across(x == 1)
        if c in climbs:
            need = jnp.logical_and(need, jnp.logical_not(climbs[c]))

        @pl.when(need)
        def _():
            kv_wait(j_xo, c, ACROSS)

    @pl.when(z == 0)
    def _():
        late = range(CH // 2, CH)
        attend(q_far, far_st, j_xo, 0, rows, qc=rc, after=send_partial, parts=late)
        arrived(q_far.at[pl.ds(0, half)], qrecv.at[1])
        attend(q_far, far_st, sp, 0, rows, True, parts=(0,))
        early = range(CH // 2)
        attend(q_far, far_st, j_xo, 0, rows, qc=rc, after=send_partial, parts=early)

    middle = jnp.logical_and(above0, helper)

    @pl.when(middle)
    def _():
        arrived(q_far.at[pl.ds(0, half)], qrecv.at[1])
        attend(q_far, far_st, sp, 0, rows, True, parts=(0,))
        attend(q_far, far_st, j_xo, 0, rows)

    weight_pass(0, PFAR)

    @pl.when(above0)
    def _():
        for c in climbs:

            @pl.when(jnp.logical_not(crosses.get(c, False)))
            def _():
                kv_wait(j_b, c, BELOW)

        arrived(cum_buf.at[j_b], crecv.at[BELOW])
        arrived(cum_buf.at[j_bo], crecv.at[DIAG])

    @pl.when(middle)
    def _():
        attend(q_far, far_st, j_b, 0, rows)

    @pl.when(above0)
    def _():
        attend(q_ref, own_st, j_b, 0, rows)

    carry_ref[0:1, :] = jnp.zeros((1, lw), F32)
    others = ends.at[pl.ds(0, SP - 1)]
    arrived(others, erecv.at[0])
    for j in range(SP - 1):

        @pl.when(j < sp)
        def _():
            carry_ref[0:1, :] = ends[j, 0:1, :] * carry_ref[0:1, :] + ends[j, 1:2, :]

    carry = carry_ref[0:1, :]
    for i in range(segs):
        r = slice(i * seg_len, (i + 1) * seg_len)
        g = gate_ref[r, :].astype(F32)
        gelu = 0.5 * g * (1.0 + jnp.tanh(0.7978845608028654 * (g + 0.044715 * (g * g * g))))
        for n in range(lw // 128):
            cs = slice(n * 128, (n + 1) * 128)
            states = local_ref[n, r, :] + prefix_ref[n, r, :] * carry[:, cs]
            br_lru[tp, r, cs] = (states * gelu[:, cs]).astype(BF16)
        if i + 1 < segs:
            carry = seg_a[i : i + 1, :] * carry + seg_b[i : i + 1, :]
    own_lru = br_lru.at[tp]
    send(own_lru, lsend.at[0], lrecv.at[FAR], {"tp": far})
    send(own_lru, lsend.at[0], lrecv.at[PARTNER], {"tp": partner})
    weight_pass(1, FAR)

    @pl.when(jnp.logical_and(helper, above0))
    def _():
        for c in order[0:2]:
            diag_wait(c)
        attend(q_far, far_st, j_bo, half, rows)

    @pl.when(x == 1)
    def _():
        attend(q_ref, own_st, j_xo, 0, rows)

    weight_pass(1, PFAR)

    upper = jnp.logical_and(above0, jnp.logical_not(helper))

    def heads_of(h):
        return slice(h * HEAD_DIM, (h + 1) * HEAD_DIM)

    def send_fox(k):
        ref = br_fox.at[tp, piece(k)]
        send(ref, fsend.at[0], frecv.at[FAR, k], {"tp": far})
        if k == PC - 1:
            send(ref, fsend.at[2], frecv.at[PFAR, k], {"tp": pfar})
        send(ref, fsend.at[1], frecv.at[PARTNER, k], {"tp": partner})

    def finish_rows(c):
        r = slice(c * rc, (c + 1) * rc)
        for h in range(H):
            br_fox[tp, r, heads_of(h)] = (o_ref[h, r, 0:HEAD_DIM] / o_ref[h, r, HEAD_DIM:]).astype(
                BF16
            )
        for k in pieces_of(c):
            send_fox(k)

    def merge_rows(c):
        for k in pieces_of(c):
            at, n = pieces[k]
            arrived(part_in.at[piece(k)], orecv.at[k])
            if k == pieces_of(c)[0]:
                arrived(stat_in.at[c], orecv.at[PC + c])
                pad_rows = jnp.zeros((128 - 2 * H, rc), F32)
                stats = jnp.concatenate([stat_in[c], pad_rows], axis=0).T
            r = slice(at, at + n)
            mine = slice(at - c * rc, at - c * rc + n)
            for h in range(H):
                m_in = stats[mine, h : h + 1]
                l_in = stats[mine, H + h : H + h + 1]
                part = part_in[r, heads_of(h)].astype(F32)
                old = m_ref[h, r, :]
                new = jnp.maximum(old, m_in)
                fade = jnp.exp2(old - new)
                grow = jnp.exp2(m_in - new)
                total = o_ref[h, r, HEAD_DIM:] * fade + l_in * grow
                br_fox[tp, r, heads_of(h)] = (
                    (o_ref[h, r, 0:HEAD_DIM] * fade + part * grow) / total
                ).astype(BF16)
            send_fox(k)

    def pair_dot(br, buf, side, r):
        first = 2 * side
        return jnp.dot(br[first, r, :], buf[first], preferred_element_type=F32) + jnp.dot(
            br[first + 1, r, :], buf[first + 1], preferred_element_type=F32
        )

    def lru_near():
        for c in own_loads:
            c.wait()
        for n in range(2):
            arrived(banks[n][1].at[partner], wrecv_own.at[n])
        arrived(br_lru.at[partner], lrecv.at[PARTNER])
        for c in range(CH):
            oacc[chunk(c), :] = pair_dot(br_lru, wl_buf, y, chunk(c))

    def lru_relay():
        arrived(br_lru.at[far], lrecv.at[FAR])
        send(br_lru.at[far], lsend.at[1], lrecv.at[PFAR], {"tp": partner})

    def lru_far():
        for role in (FAR, PFAR):
            weight_wait(0, role)
        arrived(br_lru.at[pfar], lrecv.at[PFAR])
        for c in range(CH):
            oacc[chunk(c), :] += pair_dot(br_lru, wl_buf, 1 - y, chunk(c))

    @pl.when(upper)
    def _():
        for c in order[0:2]:
            diag_wait(c)
        attend(q_ref, own_st, j_bo, half, rows)

    @pl.when(above0)
    def _():
        for c in order[2:]:
            diag_wait(c)

    @pl.when(middle)
    def _():
        attend(q_far, far_st, j_bo, 0, half, qc=rc, after=send_partial)
        attend(q_ref, own_st, j_bo, 0, rows, qc=rc, after=finish_rows)

    @pl.when(upper)
    def _():
        attend(q_ref, own_st, j_bo, 0, half)

    @pl.when(top)
    def _():
        lru_near()
        merge_rows(0)
        merge_rows(1)
        lru_relay()
        merge_rows(2)
        lru_far()
        merge_rows(3)

    @pl.when(second_top)
    def _():
        for c in range(CH):
            merge_rows(c)

    @pl.when(z == 0)
    def _():
        for c in range(CH):
            finish_rows(c)

    weight_pass_bottom(FAR)
    weight_pass_bottom(PFAR)

    @pl.when(not_top)
    def _():
        lru_near()
        lru_relay()
        lru_far()

    for role in (FAR, PFAR):
        weight_wait(1, role)

    def fox_pass(k):
        arrived(br_fox.at[far, piece(k)], frecv.at[FAR, k])
        if k < PC - 1:
            send(br_fox.at[far, piece(k)], fsend.at[2], frecv.at[PFAR, k], {"tp": partner})

    fox_pass(0)
    for k in range(PC):
        r = piece(k)
        if k + 1 < PC:
            fox_pass(k + 1)
        arrived(br_fox.at[partner, r], frecv.at[PARTNER, k])
        oacc[r, :] += pair_dot(br_fox, wf_buf, y, r)
        arrived(br_fox.at[pfar, r], frecv.at[PFAR, k])
        out[r, :] = (oacc[r, :] + pair_dot(br_fox, wf_buf, 1 - y, r)).astype(out.dtype)

    for k in range(3):
        sent(tok_buf.at[0], tsend.at[k])
        sent(br_fox.at[0], fsend.at[k])
    sent(br_lru.at[pl.ds(0, 2)], lsend.at[0])
    sent(br_lru.at[0], lsend.at[1])
    sent(wl_buf.at[0], wsend.at[1])
    sent(wl_buf.at[pl.ds(0, 2)], wsend.at[2])

    @pl.when(above0)
    def _():
        sent(wl_buf.at[0], wsend.at[0])
        sent(wl_buf.at[pl.ds(0, 2)], wsend.at[3])

    @pl.when(top)
    def _():
        sent(wl_buf.at[pl.ds(0, 2)], wsend.at[4])

    @pl.when(z == 0)
    def _():
        sent(wl_buf.at[0], wsend.at[4])

    sent(own_cum, csend.at[0])
    top_half = pl.ds(0, half)
    need = all_across(x == 0)

    @pl.when(need)
    def _():
        sent(kv_buf.at[0], xsend.at[0])

    @pl.when(jnp.logical_and(second_top, jnp.logical_not(need)))
    def _():
        sent(kv_buf.at[0, top_half], xsend.at[0])

    for level in range(Z):

        @pl.when(z == level)
        def _():
            ups = (level < Z - 1) * rc + (level < Z - 1 and level != Z - 3) * (rc - cut)
            ups += (level == Z - 2) * cut
            if ups:
                sent(kv_buf.at[0, pl.ds(0, ups)], zfwd.at[0])
            overs = (2 * rc if level else 0) + (level == Z - 2) * (rc - cut)
            overs += (0 < level < Z - 1) * cut
            if overs:
                sent(kv_buf.at[0, pl.ds(0, overs)], xfwd.at[0])

    @pl.when(not_top)
    def _():
        sent(kv_buf.at[0], zsend.at[0])
        sent(cum_buf.at[pl.ds(0, 2)], csend.at[1])

    @pl.when(helped)
    def _():
        sent(q_ref, qsend.at[0])

    @pl.when(helper)
    def _():
        sent(part_out, osend.at[0])
        sent(stat_out, osend.at[1])

    @pl.when(sp < SP - 1)
    def _():
        halo_copy.wait_send()

    sent(others, esend.at[0])


def block_shards(SP, TP, X, *args):
    tokens, lru_in, gate_in, query_w = args[:4]
    (conv_weight, rg_w, ig_w, rate, decay_extra, forget, out_lru, out_fox) = args[6:]
    rows, dcols = tokens.shape
    D, lw = lru_in.shape
    fw = query_w.shape[1]
    oc = out_lru.shape[1] // TP
    tot = 2 * lw + 3 * fw
    H = fw // HEAD_DIM
    CH = 4
    rc = rows // CH
    bw = rg_w.shape[1]
    hbm = pl.BlockSpec(memory_space=pl.ANY)
    dma = pltpu.SemaphoreType.DMA
    V = pltpu.VMEM
    scratch = [
        V((TP, rows, dcols), BF16),
        V((D, tot), BF16),
        V((2, rc, tot), F32),
        V((2, rc, 1), F32),
        V((rows, lw), BF16),
        V((16, lw), BF16),
        V((rows + 8, lw), F32),
        V(conv_weight.shape, BF16),
        V((lw // bw, bw, bw), BF16),
        V((lw // bw, bw, bw), BF16),
        V((1, rate.shape[0]), F32),
        V((H, rows), F32),
        V((lw, lw), BF16),
        V((lw, lw), BF16),
        V((rows, lw), BF16),
        V((rows, fw), BF16),
        V((rows, lw), F32),
        V((lw // 128, rows, 128), F32),
        V((lw // 128, rows, 128), F32),
        V((8, lw), F32),
        V((8, lw), F32),
        V((8, lw), F32),
        V((SP, 2, lw), F32),
        V((SP, rows, 2 * fw), BF16),
        V((SP, H, rows), F32),
        V((H, rows, 128), F32),
        V((H, rows, 2 * HEAD_DIM), F32),
        V((rows, fw), BF16),
        V((H, rows, 128), F32),
        V((H, rows, 2 * HEAD_DIM), F32),
        V((rows, fw), BF16),
        V((CH, 2 * H, rc), F32),
        V((rows, fw), BF16),
        V((CH, 2 * H, rc), F32),
        V((TP, lw, oc), BF16),
        V((TP, fw, oc), BF16),
        V((TP, rows, lw), BF16),
        V((TP, rows, fw), BF16),
        V((rows, oc), F32),
        dma((CH + 9,)),
        dma((3,)),
        dma((3, CH)),
        dma((1,)),
        dma((1,)),
        dma((1,)),
        dma((1,)),
        dma((2,)),
        dma((3,)),
        dma((1,)),
        dma((1,)),
        dma((1,)),
        dma((1,)),
        dma((3, CH + 1)),
        dma((5,)),
        dma((2,)),
        dma((2, 2, X)),
        dma((2,)),
        dma((3,)),
        dma((3,)),
        dma((3, CH + 1)),
        dma((1,)),
        dma((2,)),
        dma((2,)),
        dma((2 * CH + 1,)),
    ]
    return pl.pallas_call(
        functools.partial(block_kernel, SP, TP, X, CH),
        out_shape=pltpu.VMEM((rows, oc), BF16),
        in_specs=[hbm] * 14,
        out_specs=pl.BlockSpec(memory_space=pltpu.VMEM),
        scratch_shapes=scratch,
        compiler_params=pltpu.CompilerParams(
            collective_id=1, has_side_effects=True, vmem_limit_bytes=60 * 1024 * 1024
        ),
    )(*args[:9], rate.reshape(1, -1), decay_extra, forget.T, out_lru, out_fox)


def columns_of(mesh):
    SP = mesh.shape["sp"]
    try:
        X = len({d.coords[0] for d in mesh.devices.flat})
    except AttributeError:
        X = 2
    return X if SP % X == 0 else 1


def solution(mesh):
    placed = (
        P("sp", "tp"),
        P(None, "tp"),
        P(None, "tp"),
        P(None, "tp"),
        P(None, "tp"),
        P(None, "tp"),
        P(),
        P(),
        P(),
        P(),
        P("sp", "tp"),
        P("sp", "tp"),
        P("tp", None),
        P("tp", None),
    )
    SP, TP, X = mesh.shape["sp"], mesh.shape["tp"], columns_of(mesh)
    small = X == 2 and TP == 4 and SP // X == 4
    body = functools.partial(block_shards if small else shards, SP, TP, X)
    return jax.shard_map(
        body, mesh=mesh, in_specs=placed, out_specs=P("sp", "tp"), check_vma=False
    )
```

```python
import functools

import jax
import jax.numpy as jnp
from jax import lax
from jax.experimental import pallas as pl
from jax.experimental.pallas import tpu as pltpu
from jax.sharding import PartitionSpec as P

HEAD_DIM = 128
decay_sharpness = 8.0
epsilon_norm = 1e-06
MESH = pl.DeviceIdType.MESH
F32 = jnp.float32
BF16 = jnp.bfloat16


def one_minus_exp(w):
    u = -w
    series = 1.0 - u / 9.0
    for n in range(8, 1, -1):
        series = 1.0 - u / n * series
    return jnp.where(u < 0.5, u * series, 1.0 - jnp.exp(w))


def remote(src, dst, send_sem, recv_sem, device):
    return pltpu.make_async_remote_copy(
        src_ref=src,
        dst_ref=dst,
        send_sem=send_sem,
        recv_sem=recv_sem,
        device_id=device,
        device_id_type=MESH,
    )


def kernel(
    SP,
    TP,
    X,
    tokens,
    lru_in,
    gate_in,
    query_w,
    key_w,
    value_w,
    conv_w,
    rg_w,
    ig_w,
    rate,
    decay_extra,
    forget,
    out_lru,
    out_fox,
    out,
    tok_buf,
    w_buf,
    acc,
    sq,
    lru_ref,
    halo,
    pad,
    bd_r,
    bd_i,
    gate_ref,
    q_ref,
    decay_buf,
    prefix_ref,
    local_ref,
    ends,
    incoming,
    kv_buf,
    cum_buf,
    cum_pad,
    wide,
    fcol,
    m_ref,
    l_ref,
    o_ref,
    q_far,
    m_far,
    l_far,
    o_far,
    part_out,
    stat_out,
    part_in,
    stat_in,
    wl_buf,
    wf_buf,
    br_lru,
    br_fox,
    oacc,
    load_sem,
    tsend,
    tfwd,
    trecv,
    hsend,
    hrecv,
    esend,
    erecv,
    zsend,
    xsend,
    kvrecv,
    wsend,
    wrecv,
    lsend,
    lrecv,
    fsend,
    ffwd,
    frecv,
    lfwd,
    qsend,
    qrecv,
    osend,
    orecv,
):
    rows, dcols = tokens.shape
    D, lw = lru_in.shape
    fw = query_w.shape[1]
    H = fw // HEAD_DIM
    oc = out.shape[1]
    Y = TP // 2
    Z = SP // X
    CH = tsend.shape[1]
    rc = rows // CH
    sp = lax.axis_index("sp")
    tp = lax.axis_index("tp")
    z = lax.div(sp, X)
    x = lax.rem(sp, X)
    partner = tp + 1 - 2 * lax.rem(tp, 2)
    far = [lax.rem(tp + 2 * k, TP) for k in range(Y)]
    pfar = [lax.rem(partner + 2 * k, TP) for k in range(Y)]
    offs = [0, lw, lw + fw, lw + 2 * fw, 2 * lw + 2 * fw, 2 * lw + 3 * fw]

    barrier = pltpu.get_barrier_semaphore()
    for k in range(1, SP):
        pl.semaphore_signal(
            barrier, inc=1, device_id={"sp": lax.rem(sp + k, SP)}, device_id_type=MESH
        )
    for k in range(1, TP):
        pl.semaphore_signal(
            barrier, inc=1, device_id={"tp": lax.rem(tp + k, TP)}, device_id_type=MESH
        )
    loads = []
    for i, w in enumerate((lru_in, key_w, value_w, gate_in, query_w)):
        c = pltpu.make_async_copy(w, w_buf.at[:, offs[i] : offs[i + 1]], load_sem.at[i])
        c.start()
        loads.append(c)
    mine = pl.ds(pl.multiple_of(tp * oc, 128), oc)
    own_loads = [
        pltpu.make_async_copy(decay_extra, decay_buf, load_sem.at[5]),
        pltpu.make_async_copy(out_lru.at[:, mine], wl_buf.at[tp], load_sem.at[6]),
        pltpu.make_async_copy(out_fox.at[:, mine], wf_buf.at[tp], load_sem.at[7]),
    ]
    for c in own_loads:
        c.start()
    pl.semaphore_wait(barrier, SP - 1 + TP - 1)

    pending = []

    def chunk(c):
        return pl.ds(c * rc, rc)

    for c in range(CH):
        for k in range(1, Y):
            s = remote(
                tokens.at[chunk(c)],
                tok_buf.at[tp, chunk(c)],
                tsend.at[k, c],
                trecv.at[tp, c],
                {"tp": far[k]},
            )
            s.start()
            pending.append(s)
    for c in range(CH):
        s = remote(
            tokens.at[chunk(c)],
            tok_buf.at[tp, chunk(c)],
            tsend.at[0, c],
            trecv.at[tp, c],
            {"tp": partner},
        )
        s.start()
        pending.append(s)

    bw = rg_w.shape[1]
    nb = lw // bw
    bd_r[...] = jnp.zeros_like(bd_r)
    bd_i[...] = jnp.zeros_like(bd_i)
    for n in range(nb):
        sl = pl.ds(n * bw, bw)
        bd_r[sl, sl] = rg_w[tp * nb + n]
        bd_i[sl, sl] = ig_w[tp * nb + n]
    cum_pad[...] = jnp.zeros_like(cum_pad)
    wide[...] = jnp.zeros_like(wide)
    wide[0:H, :] = forget[...]
    fcol[...] = wide[...].T
    cum_buf[sp] = wide[0:8, :]

    for c in loads:
        c.wait()

    def project(val, src, r, first=False):
        w_rows = pl.ds(pl.multiple_of(src * dcols, dcols), dcols)
        v32 = val.astype(F32)
        part = jnp.sum(v32 * v32, axis=1, keepdims=True)
        dot = jnp.dot(val, w_buf[w_rows, :], preferred_element_type=F32)
        if first:
            sq[r, :] = part
            acc[r, :] = dot
        else:
            sq[r, :] += part
            acc[r, :] += dot

    def tok_wait(src, c):
        ref = tok_buf.at[src, chunk(c)]
        remote(ref, ref, tsend.at[0, c], trecv.at[src, c], {"tp": partner}).wait_recv()

    for c in range(CH):
        project(tokens[chunk(c), :], tp, chunk(c), True)
    for c in range(CH):
        tok_wait(partner, c)
        project(tok_buf[partner, chunk(c), :], partner, chunk(c))
    for c in range(CH):
        for k in range(1, Y):
            tok_wait(far[k], c)
            ref = tok_buf.at[far[k], chunk(c)]
            s = remote(ref, ref, tfwd.at[k, c], trecv.at[far[k], c], {"tp": partner})
            s.start()
            pending.append(s)
            project(tok_buf[far[k], chunk(c), :], far[k], chunk(c))
        for k in range(1, Y):
            tok_wait(pfar[k], c)
            project(tok_buf[pfar[k], chunk(c), :], pfar[k], chunk(c))

    row_scale = lax.rsqrt(sq[...] / D + epsilon_norm)

    def scaled(i, n=1):
        return (acc[:, offs[i] : offs[i + n]] * row_scale).astype(BF16)

    lru_ref[...] = scaled(0)
    hb = halo.shape[0]
    halo_copy = remote(
        lru_ref.at[pl.ds(rows - hb, hb)],
        halo,
        hsend.at[0],
        hrecv.at[0],
        {"sp": lax.rem(sp + 1, SP)},
    )

    @pl.when(sp < SP - 1)
    def _():
        halo_copy.start()

    kv_buf[sp] = scaled(1, 2)

    paired = Z in (3, 4)
    helper = jnp.logical_and(z <= Z - 3, paired)
    helped = jnp.logical_and(z >= 2, paired)

    def block_copies(j, a, send_sem, device):
        return (
            remote(kv_buf.at[j], kv_buf.at[j], send_sem.at[a, 0], kvrecv.at[j, 0], device),
            remote(cum_buf.at[j], cum_buf.at[j], send_sem.at[a, 1], kvrecv.at[j, 1], device),
        )

    def z_copies(dz):
        j = (z - dz) * X + x
        return block_copies(j, dz, zsend, {"sp": lax.rem(sp + X, SP)})

    def x_copies(dz, dx):
        j = (z - dz) * X + x
        xo = lax.rem(x + dx, X)
        return block_copies(j, dz, xsend.at[dx - 1], {"sp": z * X + xo})

    def for_sends(dz, own, act):
        if own or not paired:

            @pl.when(z < Z - 1)
            def _():
                for c in z_copies(dz):
                    act(c)

        for dx in range(1, X):
            if own:

                @pl.when(jnp.logical_or(lax.rem(x + dx, X) > x, helper))
                def _():
                    for c in x_copies(dz, dx):
                        act(c)
            else:
                for c in x_copies(dz, dx):
                    act(c)

    def kv_wait(j):
        for c in block_copies(j, 0, zsend, {"sp": lax.rem(sp + X, SP)}):
            c.wait_recv()

    for_sends(0, True, lambda c: c.start())

    q_ref[...] = scaled(4)
    q_copy = remote(
        q_ref, q_far, qsend.at[0], qrecv.at[0], {"sp": lax.rem(sp + SP - 2 * X, SP)}
    )

    @pl.when(helped)
    def _():
        q_copy.start()

    for i, (w, buf) in enumerate(((out_lru, wl_buf), (out_fox, wf_buf))):
        for k in range(1, TP):
            t = lax.rem(tp + k, TP)
            cols = pl.ds(pl.multiple_of(t * oc, 128), oc)
            s = remote(w.at[:, cols], buf.at[tp], wsend.at[i, k], wrecv.at[i, tp], {"tp": t})
            s.start()
            pending.append(s)

    gate_ref[...] = scaled(3)

    @pl.when(sp == 0)
    def _():
        pad[0:8, :] = jnp.zeros((8, lw), F32)

    @pl.when(sp > 0)
    def _():
        halo_copy.wait_recv()
        pad[0:8, :] = halo[...].astype(F32)[hb - 8 : hb, :]

    pad[8 : 8 + rows, :] = lru_ref[...].astype(F32)
    chans = pl.ds(pl.multiple_of(tp * lw, 128), lw)
    taps = conv_w.shape[0]
    taps_f32 = conv_w[:, chans].astype(F32)
    conv = jnp.zeros((rows, lw), F32)
    for j in range(taps):
        conv = conv + taps_f32[j : j + 1, :] * pad[8 - (taps - 1) + j : 8 - (taps - 1) + j + rows, :]
    conv_b = conv.astype(BF16)

    def sigmoid(v):
        return 1.0 / (1.0 + jnp.exp(-v))

    recur_gate = sigmoid(jnp.dot(conv_b, bd_r[...], preferred_element_type=F32))
    input_gate = sigmoid(jnp.dot(conv_b, bd_i[...], preferred_element_type=F32))
    own_rate = rate[:, chans]
    softplus = jnp.maximum(-own_rate, 0.0) + jnp.log1p(jnp.exp(-jnp.abs(own_rate)))
    for c in own_loads:
        c.wait()
    log_decay = -decay_sharpness * softplus * recur_gate + decay_buf[...]
    prefix_ref[...] = jnp.exp(log_decay)
    local_ref[...] = jnp.sqrt(one_minus_exp(2.0 * log_decay)) * input_gate * conv_b.astype(F32)
    row_id = lax.broadcasted_iota(jnp.int32, (rows, lw), 0)
    step = 1
    while step < rows:
        a = prefix_ref[...]
        b = local_ref[...]
        keep = row_id >= step
        a_prev = jnp.where(keep, pltpu.roll(a, step, 0), 1.0)
        b_prev = jnp.where(keep, pltpu.roll(b, step, 0), 0.0)
        local_ref[...] = b + a * b_prev
        prefix_ref[...] = a * a_prev
        step *= 2
    ends[sp, 0:1, :] = prefix_ref[rows - 1 : rows, :]
    ends[sp, 1:2, :] = local_ref[rows - 1 : rows, :]

    def end_copy(k):
        return remote(
            ends.at[sp], ends.at[sp], esend.at[k], erecv.at[sp], {"sp": lax.rem(sp + k, SP)}
        )

    for k in range(1, SP):

        @pl.when(sp + k < SP)
        def _():
            end_copy(k).start()

    score_scale = HEAD_DIM ** (-0.5)
    qc = rows // 2

    def attend(j, diagonal, far_first=None):
        other = far_first is not None
        first = diagonal or far_first
        qs, ms, ls, os = (q_far, m_far, l_far, o_far) if other else (q_ref, m_ref, l_ref, o_ref)

        def some(i, carry):
            r = pl.ds(pl.multiple_of(i * qc, qc), qc)
            for h in range(H):
                hs = slice(h * HEAD_DIM, (h + 1) * HEAD_DIM)
                vs = slice(fw + h * HEAD_DIM, fw + (h + 1) * HEAD_DIM)
                s = lax.dot_general(
                    qs[r, hs],
                    kv_buf[j, :, hs],
                    (((1,), (1,)), ((), ())),
                    preferred_element_type=F32,
                )
                s = s * score_scale
                if not other:
                    s = s + fcol[r, h : h + 1]
                s = s - cum_buf[j, h : h + 1, :]
                if diagonal:
                    causal = (
                        lax.broadcasted_iota(jnp.int32, (qc, rows), 0) + i * qc
                        >= lax.broadcasted_iota(jnp.int32, (qc, rows), 1)
                    )
                    s = jnp.where(causal, s, -1e30)
                top = jnp.max(s, axis=1, keepdims=True)
                if first:
                    p = jnp.exp(s - top)
                    ms[h, r, :] = top
                    ls[h, r, :] = jnp.sum(p, axis=1, keepdims=True)
                    os[h, r, :] = jnp.dot(
                        p.astype(BF16), kv_buf[j, :, vs], preferred_element_type=F32
                    )
                else:
                    old = ms[h, r, :]
                    new = jnp.maximum(old, top)
                    p = jnp.exp(s - new)
                    fade = jnp.exp(old - new)
                    ms[h, r, :] = new
                    ls[h, r, :] = ls[h, r, :] * fade + jnp.sum(p, axis=1, keepdims=True)
                    os[h, r, :] = os[h, r, :] * fade + jnp.dot(
                        p.astype(BF16), kv_buf[j, :, vs], preferred_element_type=F32
                    )
            return carry

        lax.fori_loop(0, rows // qc, some, 0)

    attend(sp, True)

    def row_blocks(dz):
        for dx in range(1, X):
            xo = lax.rem(x + dx, X)

            @pl.when(jnp.logical_or(dz > 0, xo < x))
            def _():
                j = (z - dz) * X + xo
                kv_wait(j)
                attend(j, False)

    def finish_lru():
        incoming[...] = jnp.zeros_like(incoming)
        for j in range(SP - 1):

            @pl.when(j < sp)
            def _():
                remote(
                    ends.at[j], ends.at[j], esend.at[0], erecv.at[j], {"sp": lax.rem(sp + 1, SP)}
                ).wait_recv()
                incoming[...] = ends[j, 0:1, :] * incoming[...] + ends[j, 1:2, :]

        states = local_ref[...] + prefix_ref[...] * incoming[...]
        g = gate_ref[...].astype(F32)
        gelu = 0.5 * g * (1.0 + jnp.tanh(0.7978845608028654 * (g + 0.044715 * (g * g * g))))
        br_lru[tp] = (states * gelu).astype(BF16)
        for k in range(Y - 1, -1, -1):
            lru_copy(k).start()

    def lru_copy(k):
        to = far[k] if k else partner
        return remote(br_lru.at[tp], br_lru.at[tp], lsend.at[k], lrecv.at[tp], {"tp": to})

    lru_step = min(2, Z - 1)
    if Z == 1:
        finish_lru()

    def hop(dz, carry):
        @pl.when(dz <= z)
        def _():
            j = (z - dz) * X + x
            kv_wait(j)
            for_sends(dz, False, lambda c: c.start())
            row_blocks(dz - 1)
            attend(j, False)

        @pl.when(dz == lru_step)
        def _():
            finish_lru()

        return carry

    up = {"sp": lax.rem(sp + 2 * X, SP)}
    part_copies = (
        remote(part_out, part_in, osend.at[0], orecv.at[0], up),
        remote(stat_out, stat_in, osend.at[1], orecv.at[1], up),
    )

    def send_partial():
        for h in range(H):
            part_out[:, h * HEAD_DIM : (h + 1) * HEAD_DIM] = o_far[h].astype(BF16)
            cum_pad[:, h : h + 1] = m_far[h]
            cum_pad[:, H + h : H + h + 1] = l_far[h]
        stat_out[...] = cum_pad[...].T[0:8, :]
        for c in part_copies:
            c.start()

    if paired:
        below = (z - 1) * X

        @pl.when(helper)
        def _():
            q_copy.wait_recv()
            attend(sp, False, True)

        @pl.when(z >= 1)
        def _():
            kv_wait(below + x)
            for_sends(1, False, lambda c: c.start())

        for dx in range(1, X):
            xo = lax.rem(x + dx, X)

            @pl.when(jnp.logical_or(xo < x, helper))
            def _():
                kv_wait(z * X + xo)

            @pl.when(helper)
            def _():
                attend(z * X + xo, False, False)

        @pl.when(jnp.logical_and(helper, z == 0))
        def _():
            send_partial()

        for dx in range(1, X):
            xo = lax.rem(x + dx, X)

            @pl.when(xo < x)
            def _():
                attend(z * X + xo, False)

        finish_lru()

        @pl.when(jnp.logical_and(helper, z >= 1))
        def _():
            attend(below + x, False, False)

        @pl.when(z >= 1)
        def _():
            attend(below + x, False)
            for dx in range(1, X):
                j = below + lax.rem(x + dx, X)
                kv_wait(j)

                @pl.when(helper)
                def _():
                    attend(j, False, False)

            @pl.when(helper)
            def _():
                send_partial()

            for dx in range(1, X):
                attend(below + lax.rem(x + dx, X), False)

    else:
        lax.fori_loop(1, Z, hop, 0)

    def lru_wait(t):
        remote(br_lru.at[t], br_lru.at[t], lsend.at[0], lrecv.at[t], {"tp": partner}).wait_recv()

    def lru_dot(t):
        return jnp.dot(br_lru[t], wl_buf[t], preferred_element_type=F32)

    oacc[...] = lru_dot(tp)
    for k in range(1, TP):
        t = lax.rem(tp + k, TP)
        for i, buf in enumerate((wl_buf, wf_buf)):
            remote(buf.at[t], buf.at[t], wsend.at[i, k], wrecv.at[i, t], {"tp": t}).wait_recv()
    for k in range(1, Y):
        lru_wait(far[k])
        ref = br_lru.at[far[k]]
        s = remote(ref, ref, lfwd.at[k], lrecv.at[far[k]], {"tp": partner})
        s.start()
        pending.append(s)
    lru_wait(partner)
    oacc[...] += lru_dot(partner)
    for k in range(1, Y):
        oacc[...] += lru_dot(far[k])
        lru_wait(pfar[k])
        oacc[...] += lru_dot(pfar[k])

    if paired:

        @pl.when(helped)
        def _():
            for c in part_copies:
                c.wait_recv()
            wide[0:8, :] = stat_in[...]
            stats = wide[...].T
            for h in range(H):
                m_in = stats[:, h : h + 1] + fcol[:, h : h + 1]
                l_in = stats[:, H + h : H + h + 1]
                part = part_in[:, h * HEAD_DIM : (h + 1) * HEAD_DIM].astype(F32)
                new = jnp.maximum(m_ref[h], m_in)
                fade = jnp.exp(m_ref[h] - new)
                grow = jnp.exp(m_in - new)
                l_ref[h] = l_ref[h] * fade + l_in * grow
                o_ref[h] = o_ref[h] * fade + part * grow

    else:
        row_blocks(z)

    for c in range(CH):
        r = chunk(c)
        for h in range(H):
            br_fox[tp, r, h * HEAD_DIM : (h + 1) * HEAD_DIM] = (
                o_ref[h, r, :] / l_ref[h, r, :]
            ).astype(BF16)
        ref = br_fox.at[tp, r]
        for k in list(range(1, Y)) + [0]:
            to = far[k] if k else partner
            s = remote(ref, ref, fsend.at[k, c], frecv.at[tp, c], {"tp": to})
            s.start()
            pending.append(s)

    def fox_wait(src, c):
        ref = br_fox.at[src, chunk(c)]
        remote(ref, ref, fsend.at[0, c], frecv.at[src, c], {"tp": partner}).wait_recv()

    def fox_dot(src, r):
        return jnp.dot(br_fox[src, r, :], wf_buf[src], preferred_element_type=F32)

    for c in range(CH):
        fox_wait(partner, c)
        oacc[chunk(c), :] += fox_dot(tp, chunk(c)) + fox_dot(partner, chunk(c))
    for c in range(CH):
        r = chunk(c)
        for k in range(1, Y):
            fox_wait(far[k], c)
            ref = br_fox.at[far[k], r]
            s = remote(ref, ref, ffwd.at[k, c], frecv.at[far[k], c], {"tp": partner})
            s.start()
            pending.append(s)
            oacc[r, :] += fox_dot(far[k], r)
        for k in range(1, Y):
            fox_wait(pfar[k], c)
            oacc[r, :] += fox_dot(pfar[k], r)
        out[r, :] = oacc[r, :].astype(out.dtype)

    for s in pending:
        s.wait_send()
    for k in range(Y):
        lru_copy(k).wait_send()

    @pl.when(helped)
    def _():
        q_copy.wait_send()

    @pl.when(helper)
    def _():
        for c in part_copies:
            c.wait_send()

    @pl.when(sp < SP - 1)
    def _():
        halo_copy.wait_send()

    for k in range(1, SP):

        @pl.when(sp + k < SP)
        def _():
            end_copy(k).wait_send()

    for_sends(0, True, lambda c: c.wait_send())

    def drain(dz, carry):
        @pl.when(dz <= z)
        def _():
            for_sends(dz, False, lambda c: c.wait_send())

        return carry

    if paired:

        @pl.when(z >= 1)
        def _():
            for_sends(1, False, lambda c: c.wait_send())

    else:
        lax.fori_loop(1, Z, drain, 0)


def shards(SP, TP, X, *args):
    tokens, lru_in, gate_in, query_w = args[:4]
    (conv_weight, rg_w, ig_w, rate, decay_extra, forget, out_lru, out_fox) = args[6:]
    rows, dcols = tokens.shape
    D, lw = lru_in.shape
    fw = query_w.shape[1]
    oc = out_lru.shape[1] // TP
    tot = 2 * lw + 3 * fw
    H = fw // HEAD_DIM
    Y = TP // 2
    Z = SP // X
    CH = 4
    vm = pl.BlockSpec(memory_space=pltpu.VMEM)
    hbm = pl.BlockSpec(memory_space=pl.ANY)
    dma = pltpu.SemaphoreType.DMA
    V = pltpu.VMEM
    scratch = [
        V((TP, rows, dcols), BF16),
        V((D, tot), BF16),
        V((rows, tot), F32),
        V((rows, 1), F32),
        V((rows, lw), BF16),
        V((16, lw), BF16),
        V((rows + 8, lw), F32),
        V((lw, lw), BF16),
        V((lw, lw), BF16),
        V((rows, lw), BF16),
        V((rows, fw), BF16),
        V((rows, lw), F32),
        V((rows, lw), F32),
        V((rows, lw), F32),
        V((SP, 8, lw), F32),
        V((1, lw), F32),
        V((SP, rows, 2 * fw), BF16),
        V((SP, 8, rows), F32),
        V((rows, 128), F32),
        V((128, rows), F32),
        V((rows, 128), F32),
        V((H, rows, 1), F32),
        V((H, rows, 1), F32),
        V((H, rows, HEAD_DIM), F32),
        V((rows, fw), BF16),
        V((H, rows, 1), F32),
        V((H, rows, 1), F32),
        V((H, rows, HEAD_DIM), F32),
        V((rows, fw), BF16),
        V((8, rows), F32),
        V((rows, fw), BF16),
        V((8, rows), F32),
        V((TP, lw, oc), BF16),
        V((TP, fw, oc), BF16),
        V((TP, rows, lw), BF16),
        V((TP, rows, fw), BF16),
        V((rows, oc), F32),
        dma((8,)),
        dma((Y, CH)),
        dma((Y, CH)),
        dma((TP, CH)),
        dma((1,)),
        dma((1,)),
        dma((SP,)),
        dma((SP,)),
        dma((Z, 2)),
        dma((max(X - 1, 1), Z, 2)),
        dma((SP, 2)),
        dma((2, TP)),
        dma((2, TP)),
        dma((TP,)),
        dma((TP,)),
        dma((Y, CH)),
        dma((Y, CH)),
        dma((TP, CH)),
        dma((Y,)),
        dma((1,)),
        dma((1,)),
        dma((2,)),
        dma((2,)),
    ]
    return pl.pallas_call(
        functools.partial(kernel, SP, TP, X),
        out_shape=jax.ShapeDtypeStruct((rows, oc), BF16),
        in_specs=[vm] + [hbm] * 5 + [vm] * 4 + [hbm, vm, hbm, hbm],
        out_specs=vm,
        scratch_shapes=scratch,
        compiler_params=pltpu.CompilerParams(
            collective_id=0, has_side_effects=True, vmem_limit_bytes=60 * 1024 * 1024
        ),
    )(*args[:9], rate.reshape(1, -1), decay_extra, forget.T, out_lru, out_fox)


LOG2E = 1.4426950408889634


def block_kernel(
    SP,
    TP,
    X,
    CH,
    tokens,
    lru_in,
    gate_in,
    query_w,
    key_w,
    value_w,
    conv_w,
    rg_w,
    ig_w,
    rate,
    decay_extra,
    forget,
    out_lru,
    out_fox,
    out,
    tok_buf,
    w_buf,
    acc,
    sq,
    lru_ref,
    halo,
    pad,
    conv_v,
    rg_v,
    ig_v,
    rate_v,
    forget_v,
    bd_r,
    bd_i,
    gate_ref,
    q_ref,
    decay_buf,
    prefix_ref,
    local_ref,
    seg_a,
    seg_b,
    carry_ref,
    ends,
    kv_buf,
    cum_buf,
    m_ref,
    o_ref,
    q_far,
    m_far,
    o_far,
    part_out,
    stat_out,
    part_in,
    stat_in,
    wl_buf,
    wf_buf,
    br_lru,
    br_fox,
    oacc,
    load_sem,
    tsend,
    trecv_near,
    trecv,
    hsend,
    hrecv,
    esend,
    erecv,
    csend,
    crecv,
    zsend,
    xsend,
    zfwd,
    xfwd,
    kvrecv,
    wsend,
    wrecv_own,
    wrecv,
    lsend,
    lrecv,
    fsend,
    frecv_near,
    frecv,
    qsend,
    qrecv,
    osend,
    orecv,
):
    rows, dcols = tokens.shape
    D, lw = lru_in.shape
    fw = query_w.shape[1]
    H = fw // HEAD_DIM
    oc = out.shape[1]
    Z = SP // X
    rc = rows // CH
    half = rows // 2
    wh = out_lru.shape[0] // X
    sp = lax.axis_index("sp")
    tp = lax.axis_index("tp")
    z = lax.div(sp, X)
    x = lax.rem(sp, X)
    xo = 1 - x
    y = lax.div(tp, 2)
    partner = tp + 1 - 2 * lax.rem(tp, 2)
    far = lax.rem(tp + 2, TP)
    pfar = lax.rem(partner + 2, TP)
    j_xo = z * X + xo
    to_xo = {"sp": j_xo}
    to_up = {"sp": lax.rem(sp + X, SP)}
    j_b = lax.rem(sp + SP - X, SP)
    j_bo = lax.rem(j_xo + SP - X, SP)
    helper = z <= Z - 3
    helped = z >= 2
    not_top = z < Z - 1
    above0 = z >= 1
    order = list(range(CH - 1, -1, -1))
    second_top = z == Z - 2
    last = order[3]
    last_climbs = jnp.logical_and(not_top, z != Z - 3)
    last_crosses = jnp.logical_and(above0, not_top)
    climbs = {order[1]: not_top, last: last_climbs}
    crosses = {order[0]: above0, order[2]: above0, last: last_crosses}
    whalf = lax.rem(x + z, X)
    top = z == Z - 1
    PARTNER, FAR, PFAR = 0, 1, 2
    ACROSS, BELOW, DIAG = 0, 1, 2
    score_k = HEAD_DIM ** (-0.5) * LOG2E

    def chunk(c):
        return pl.ds(c * rc, rc)

    pieces = [(c * rc, rc) for c in range(CH - 1)]
    pieces += [(rows - rc, rc // 2), (rows - rc // 2, rc // 2)]
    PC = len(pieces)

    def piece(k):
        return pl.ds(*pieces[k])

    def pieces_of(c):
        return [k for k, (at, n) in enumerate(pieces) if at // rc == c]

    barrier = pltpu.get_barrier_semaphore()
    for k in range(1, SP):
        pl.semaphore_signal(
            barrier, inc=1, device_id={"sp": lax.rem(sp + k, SP)}, device_id_type=MESH
        )
    for k in range(1, TP):
        pl.semaphore_signal(
            barrier, inc=1, device_id={"tp": lax.rem(tp + k, TP)}, device_id_type=MESH
        )

    def load(i, src, dst):
        c = pltpu.make_async_copy(src, dst, load_sem.at[i])
        c.start()
        return c

    for c in order:
        load(0, tokens.at[chunk(c)], tok_buf.at[tp, chunk(c)])
    cols = (0, fw, 2 * fw, 2 * fw + lw, 3 * fw + lw, 3 * fw + 2 * lw)
    for i, w in enumerate((key_w, value_w, lru_in, query_w, gate_in)):
        load(1, w, w_buf.at[:, cols[i] : cols[i + 1]])
    mine = pl.ds(pl.multiple_of(tp * oc, 128), oc)
    bw = rg_w.shape[1]
    nb = lw // bw
    gates = pl.ds(tp * nb, nb)
    forget_load = load(2, forget, forget_v)
    small_loads = [
        load(3, conv_w, conv_v),
        load(4, rg_w.at[gates], rg_v),
        load(5, ig_w.at[gates], ig_v),
        load(6, rate, rate_v),
        load(7, decay_extra, decay_buf),
    ]
    load(8, out_lru.at[:, mine], wl_buf.at[tp])
    load(8, out_fox.at[:, mine], wf_buf.at[tp])
    pl.semaphore_wait(barrier, SP - 1 + TP - 1)

    def send(ref, send_sem, recv_sem, device):
        remote(ref, ref, send_sem, recv_sem, device).start()

    def arrived(ref, recv_sem):
        remote(ref, ref, recv_sem, recv_sem, to_xo).wait_recv()

    def sent(ref, send_sem):
        remote(ref, ref, send_sem, send_sem, to_xo).wait_send()

    own_rows = tok_buf.at[tp]
    pltpu.make_async_copy(own_rows, own_rows, load_sem.at[0]).wait()
    for c in order:
        ref = tok_buf.at[tp, chunk(c)]
        send(ref, tsend.at[0], trecv.at[0, c], {"tp": far})

    own_tok = tok_buf.at[tp]
    send(own_tok, tsend.at[1], trecv_near.at[0], {"tp": partner})
    forget_load.wait()
    cum_buf[sp] = forget_v[...] * LOG2E
    own_cum = cum_buf.at[sp]
    send(own_cum, csend.at[0], crecv.at[ACROSS], to_xo)

    @pl.when(not_top)
    def _():
        send(own_cum, csend.at[1], crecv.at[BELOW], to_up)
        send(own_cum, csend.at[1], crecv.at[DIAG], {"sp": lax.rem(j_xo + X, SP)})

    for c in small_loads:
        c.wait()
    bd_r[...] = jnp.zeros_like(bd_r)
    bd_i[...] = jnp.zeros_like(bd_i)
    for n in range(nb):
        sl = pl.ds(n * bw, bw)
        bd_r[sl, sl] = rg_v[n]
        bd_i[sl, sl] = ig_v[n]
    pltpu.make_async_copy(w_buf, w_buf, load_sem.at[1]).wait()

    def tok_wait(src, role, c):
        arrived(tok_buf.at[src, chunk(c)], trecv.at[role - 1, c])

    def features(side, c):
        first = 2 * side
        return jnp.concatenate([tok_buf[first, chunk(c), :], tok_buf[first + 1, chunk(c), :]], axis=1)

    def w_rows(side):
        return pl.ds(pl.multiple_of(side * 2 * dcols, 2 * dcols), 2 * dcols)

    def squares(v):
        v32 = v.astype(F32)
        return jnp.sum(v32 * v32, axis=1, keepdims=True)

    def near_part(c, slot):
        v = features(y, c)
        sq[slot] = squares(v)
        acc[slot] = jnp.dot(v, w_buf[w_rows(y), :], preferred_element_type=F32)

    halo_copy = remote(
        lru_ref.at[pl.ds(rows - halo.shape[0], halo.shape[0])],
        halo,
        hsend.at[0],
        hrecv.at[0],
        {"sp": lax.rem(sp + 1, SP)},
    )

    def kv_send(j, c, send_sem, role, device):
        send(kv_buf.at[j, chunk(c)], send_sem.at[0], kvrecv.at[role, c], device)

    def kv_wait(j, c, role):
        arrived(kv_buf.at[j, chunk(c)], kvrecv.at[role, c])

    def all_across(own_x):
        return jnp.logical_or(own_x, helper)

    def across(own_x, c):
        need = all_across(own_x)
        return jnp.logical_or(need, climbs[c]) if c in climbs else need

    def q_copy(c):
        return remote(
            q_ref.at[chunk(c)],
            q_far.at[chunk(c)],
            qsend.at[0],
            qrecv.at[0 if c in order[0:2] else 1],
            {"sp": lax.rem(sp + SP - 2 * X, SP)},
        )

    def far_part(i, c, slot):
        tok_wait(far, FAR, c)
        send(tok_buf.at[far, chunk(c)], tsend.at[2], trecv.at[1, c], {"tp": partner})
        if i + 1 < CH:
            near_part(order[i + 1], 1 - slot)
        tok_wait(pfar, PFAR, c)
        if i == CH - 1:
            send_weights()
        v = features(1 - y, c)
        row_scale = lax.rsqrt((sq[slot] + squares(v)) / D + epsilon_norm)

        def part(a, b):
            w = w_buf[w_rows(1 - y), cols[a] : cols[b]]
            both = acc[slot, :, cols[a] : cols[b]] + jnp.dot(v, w, preferred_element_type=F32)
            return (both * row_scale).astype(BF16)

        kv_buf[sp, chunk(c), :] = part(0, 2)

        @pl.when(across(x == 0, c))
        def _():
            kv_send(sp, c, xsend, ACROSS, to_xo)

        @pl.when(not_top)
        def _():
            kv_send(sp, c, zsend, BELOW, to_up)

        rest = part(2, 5)
        lru_ref[chunk(c), :] = rest[:, 0:lw]
        q_ref[chunk(c), :] = rest[:, lw : lw + fw]
        gate_ref[chunk(c), :] = rest[:, lw + fw :]

        @pl.when(helped)
        def _():
            q_copy(c).start()

        if i == 0:

            @pl.when(sp < SP - 1)
            def _():
                halo_copy.start()

    banks = ((out_lru, wl_buf), (out_fox, wf_buf))

    def send_weights():
        r = pl.ds(pl.multiple_of(whalf * wh, wh), wh)

        def over_y(n):
            w, buf = banks[n]
            for role, t in ((FAR, far), (PFAR, pfar)):
                c = pl.ds(pl.multiple_of(t * oc, 128), oc)
                remote(
                    w.at[r, c], buf.at[tp, r], wsend.at[n], wrecv.at[n, role - 1, whalf], {"tp": t}
                ).start()

        pl.when(above0)(lambda: over_y(0))
        over_y(1)
        c = pl.ds(pl.multiple_of(partner * oc, 128), oc)
        for n, (w, buf) in enumerate(banks):
            remote(w.at[:, c], buf.at[tp], wsend.at[2], wrecv_own.at[0], {"tp": partner}).start()

    def weight_part(n, role, k):
        t = far if role == FAR else pfar
        ref = banks[n][1].at[t, pl.ds(pl.multiple_of(k * wh, wh), wh)]
        return ref, wrecv.at[n, role - 1, k]

    def weight_pass(n, role):
        ref, sem = weight_part(n, role, whalf)

        def take():
            arrived(ref, sem)

        if n == 0:
            pl.when(above0)(take)
        else:
            take()

        @pl.when(above0)
        def _():
            send(ref, wsend.at[3], sem, {"sp": lax.rem(sp + SP - X, SP)})

        @pl.when(top)
        def _():
            send(ref, wsend.at[4], sem, to_xo)

    def weight_pass_bottom(role):
        @pl.when(z == 0)
        def _():
            ref, sem = weight_part(0, role, 1 - whalf)
            arrived(ref, sem)
            send(ref, wsend.at[4], sem, to_xo)

    def weight_wait(n, role):
        k = 1 - whalf
        if n == 0:
            k = jnp.where(z == 0, whalf, k)
        arrived(*weight_part(n, role, k))

    def pass_up(c):
        @pl.when(climbs[c])
        def _():
            kv_wait(j_xo, c, ACROSS)
            kv_send(j_xo, c, zfwd, DIAG, to_up)

    def pass_across(c):
        @pl.when(crosses[c])
        def _():
            kv_wait(j_b, c, BELOW)
            kv_send(j_b, c, xfwd, DIAG, to_xo)

    cut = rc - rc // 4

    def half_ref(j, upper_part):
        at, n = (cut, rc - cut) if upper_part else (0, cut)
        return kv_buf.at[j, pl.ds(last * rc + at, n)]

    def half_sem(upper_part):
        return kvrecv.at[DIAG, last] if upper_part else kvrecv.at[DIAG, CH]

    def pass_up_last():
        @pl.when(last_climbs)
        def _():
            kv_wait(j_xo, last, ACROSS)
            send(half_ref(j_xo, True), zfwd.at[0], half_sem(True), to_up)

        @pl.when(second_top)
        def _():
            send(half_ref(j_xo, False), zfwd.at[0], half_sem(False), to_up)

    def pass_across_last():
        @pl.when(last_crosses)
        def _():
            kv_wait(j_b, last, BELOW)
            send(half_ref(j_b, False), xfwd.at[0], half_sem(False), to_xo)

        @pl.when(second_top)
        def _():
            send(half_ref(j_b, True), xfwd.at[0], half_sem(True), to_xo)

    def diag_wait(c):
        if c == last:
            for upper_part in (True, False):
                arrived(half_ref(j_bo, upper_part), half_sem(upper_part))
        else:
            kv_wait(j_bo, c, DIAG)

    arrived(tok_buf.at[partner], trecv_near.at[0])
    near_part(order[0], 0)
    for i, c in enumerate(order):
        far_part(i, c, i % 2)

    pass_across(order[0])
    pass_up(order[1])

    @pl.when(sp == 0)
    def _():
        pad[0:8, :] = jnp.zeros((8, lw), F32)

    @pl.when(sp > 0)
    def _():
        halo_copy.wait_recv()
        hb = halo.shape[0]
        pad[0:8, :] = halo[...].astype(F32)[hb - 8 : hb, :]

    pad[8 : 8 + rows, :] = lru_ref[...].astype(F32)
    chans = pl.ds(pl.multiple_of(tp * lw, 128), lw)
    taps = conv_w.shape[0]
    taps_f32 = conv_v[:, chans].astype(F32)
    conv = jnp.zeros((rows, lw), F32)
    for j in range(taps):
        conv = conv + taps_f32[j : j + 1, :] * pad[8 - (taps - 1) + j : 8 - (taps - 1) + j + rows, :]
    conv_b = conv.astype(BF16)

    def sigmoid(v):
        return 1.0 / (1.0 + jnp.exp(-v))

    recur_gate = sigmoid(jnp.dot(conv_b, bd_r[...], preferred_element_type=F32))
    input_gate = sigmoid(jnp.dot(conv_b, bd_i[...], preferred_element_type=F32))
    own_rate = rate_v[:, chans]
    softplus = jnp.maximum(-own_rate, 0.0) + jnp.log1p(jnp.exp(-jnp.abs(own_rate)))
    log_decay = -decay_sharpness * softplus * recur_gate + decay_buf[...]
    decay = jnp.exp(log_decay)
    driven = jnp.sqrt(one_minus_exp(2.0 * log_decay)) * input_gate * conv_b.astype(F32)
    for n in range(lw // 128):
        prefix_ref[n] = decay[:, n * 128 : (n + 1) * 128]
        local_ref[n] = driven[:, n * 128 : (n + 1) * 128]

    segs = 8
    seg_len = rows // segs
    run_a = jnp.ones((segs, lw), F32)
    run_b = jnp.zeros((segs, lw), F32)
    for i in range(seg_len):
        at = pl.ds(i, segs, stride=seg_len)
        a = [prefix_ref[n, at, :] for n in range(lw // 128)]
        b = [local_ref[n, at, :] for n in range(lw // 128)]
        a = jnp.concatenate(a, axis=1)
        b = jnp.concatenate(b, axis=1)
        run_a = run_a * a
        run_b = a * run_b + b
        for n in range(lw // 128):
            prefix_ref[n, at, :] = run_a[:, n * 128 : (n + 1) * 128]
            local_ref[n, at, :] = run_b[:, n * 128 : (n + 1) * 128]
    seg_a[...] = run_a
    seg_b[...] = run_b
    end_a = seg_a[0:1, :]
    end_b = seg_b[0:1, :]
    for i in range(1, segs):
        end_b = seg_a[i : i + 1, :] * end_b + seg_b[i : i + 1, :]
        end_a = end_a * seg_a[i : i + 1, :]
    ends[sp, 0:1, :] = end_a
    ends[sp, 1:2, :] = end_b

    def end_copy(k):
        return remote(
            ends.at[sp],
            ends.at[sp],
            esend.at[0],
            erecv.at[0],
            {"sp": lax.rem(sp + k, SP)},
        )

    for k in range(1, SP):
        end_copy(k).start()

    pass_across(order[2])

    def attend(qs, st, j, lo, hi, first=False, diagonal=False, qc=half, after=None, parts=None):
        ms, os = st
        items = [(i, h) for i in (parts or range(rows // qc)) for h in range(H)]

        def width(i):
            return (lo, (i + 1) * qc) if diagonal else (lo, hi)

        def scores(i, h):
            a, b = width(i)
            hs = slice(h * HEAD_DIM, (h + 1) * HEAD_DIM)
            s = lax.dot_general(
                qs[i * qc : (i + 1) * qc, hs],
                kv_buf[j, a:b, hs],
                (((1,), (1,)), ((), ())),
                preferred_element_type=F32,
            )
            s = s * score_k - cum_buf[j, h : h + 1, a:b]
            if diagonal:
                causal = (
                    lax.broadcasted_iota(jnp.int32, (qc, b - a), 0) + (i * qc - a)
                    >= lax.broadcasted_iota(jnp.int32, (qc, b - a), 1)
                )
                s = jnp.where(causal, s, -1e30)
            return s

        def update(i, h, s):
            a, b = width(i)
            r = slice(i * qc, (i + 1) * qc)
            top = jnp.max(s, axis=1, keepdims=True)
            if first:
                new = jnp.broadcast_to(top, (qc, 128))
            else:
                old = ms[h, r, :]
                new = jnp.maximum(old, top)
            ms[h, r, :] = new
            p = jnp.exp2(s - jnp.concatenate([new] * ((b - a) // 128), axis=1)).astype(BF16)
            v = kv_buf[j, a:b, fw + h * HEAD_DIM : fw + (h + 1) * HEAD_DIM]
            v1 = jnp.concatenate([v, jnp.ones((b - a, 128), BF16)], axis=1)
            pv = jnp.dot(p, v1, preferred_element_type=F32)
            if first:
                os[h, r, :] = pv
            else:
                fade = jnp.exp2(old - new)
                os[h, r, :] = os[h, r, :] * jnp.concatenate([fade, fade], axis=1) + pv

        s = scores(*items[0])
        for n, (i, h) in enumerate(items):
            nxt = scores(*items[n + 1]) if n + 1 < len(items) else None
            update(i, h, s)
            s = nxt
            if after is not None and h == H - 1:
                after(i)

    own_st = (m_ref, o_ref)
    far_st = (m_far, o_far)
    up2 = {"sp": lax.rem(sp + 2 * X, SP)}

    def part_copy(k):
        r = piece(k)
        return remote(part_out.at[r], part_in.at[r], osend.at[0], orecv.at[k], up2)

    def stat_copy(c):
        return remote(stat_out.at[c], stat_in.at[c], osend.at[1], orecv.at[PC + c], up2)

    def send_partial(c):
        r = slice(c * rc, (c + 1) * rc)
        lane = lax.broadcasted_iota(jnp.int32, (rc, 128), 1)
        stats = jnp.zeros((rc, 128), F32)
        for h in range(H):
            part_out[r, h * HEAD_DIM : (h + 1) * HEAD_DIM] = o_far[h, r, 0:HEAD_DIM].astype(BF16)
            stats = jnp.where(lane == h, m_far[h, r, :], stats)
            stats = jnp.where(lane == H + h, o_far[h, r, HEAD_DIM:], stats)
        stat_out[c] = stats.T[0 : 2 * H, :]
        stat_copy(c).start()
        for k in pieces_of(c):
            part_copy(k).start()

    attend(q_ref, own_st, sp, 0, rows, True, True)

    @pl.when(helper)
    def _():
        arrived(q_far.at[pl.ds(half, half)], qrecv.at[0])
        attend(q_far, far_st, sp, 0, rows, True, parts=(1,))

    pass_up_last()
    pass_across_last()

    weight_pass(0, FAR)
    arrived(cum_buf.at[j_xo], crecv.at[ACROSS])

    for c in order:
        need = all_across(x == 1)
        if c in climbs:
            need = jnp.logical_and(need, jnp.logical_not(climbs[c]))

        @pl.when(need)
        def _():
            kv_wait(j_xo, c, ACROSS)

    @pl.when(z == 0)
    def _():
        late = range(CH // 2, CH)
        attend(q_far, far_st, j_xo, 0, rows, qc=rc, after=send_partial, parts=late)
        arrived(q_far.at[pl.ds(0, half)], qrecv.at[1])
        attend(q_far, far_st, sp, 0, rows, True, parts=(0,))
        early = range(CH // 2)
        attend(q_far, far_st, j_xo, 0, rows, qc=rc, after=send_partial, parts=early)

    middle = jnp.logical_and(above0, helper)

    @pl.when(middle)
    def _():
        arrived(q_far.at[pl.ds(0, half)], qrecv.at[1])
        attend(q_far, far_st, sp, 0, rows, True, parts=(0,))
        attend(q_far, far_st, j_xo, 0, rows)

    weight_pass(0, PFAR)

    @pl.when(above0)
    def _():
        for c in climbs:

            @pl.when(jnp.logical_not(crosses.get(c, False)))
            def _():
                kv_wait(j_b, c, BELOW)

        arrived(cum_buf.at[j_b], crecv.at[BELOW])
        arrived(cum_buf.at[j_bo], crecv.at[DIAG])

    @pl.when(middle)
    def _():
        attend(q_far, far_st, j_b, 0, rows)

    @pl.when(above0)
    def _():
        attend(q_ref, own_st, j_b, 0, rows)

    carry_ref[0:1, :] = jnp.zeros((1, lw), F32)
    others = ends.at[pl.ds(0, SP - 1)]
    arrived(others, erecv.at[0])
    for j in range(SP - 1):

        @pl.when(j < sp)
        def _():
            carry_ref[0:1, :] = ends[j, 0:1, :] * carry_ref[0:1, :] + ends[j, 1:2, :]

    carry = carry_ref[0:1, :]
    for i in range(segs):
        r = slice(i * seg_len, (i + 1) * seg_len)
        g = gate_ref[r, :].astype(F32)
        gelu = 0.5 * g * (1.0 + jnp.tanh(0.7978845608028654 * (g + 0.044715 * (g * g * g))))
        for n in range(lw // 128):
            cs = slice(n * 128, (n + 1) * 128)
            states = local_ref[n, r, :] + prefix_ref[n, r, :] * carry[:, cs]
            br_lru[tp, r, cs] = (states * gelu[:, cs]).astype(BF16)
        if i + 1 < segs:
            carry = seg_a[i : i + 1, :] * carry + seg_b[i : i + 1, :]
    own_lru = br_lru.at[tp]
    send(own_lru, lsend.at[0], lrecv.at[FAR], {"tp": far})
    send(own_lru, lsend.at[0], lrecv.at[PARTNER], {"tp": partner})
    weight_pass(1, FAR)

    @pl.when(jnp.logical_and(helper, above0))
    def _():
        for c in order[0:2]:
            diag_wait(c)
        attend(q_far, far_st, j_bo, half, rows)

    @pl.when(x == 1)
    def _():
        attend(q_ref, own_st, j_xo, 0, rows)

    weight_pass(1, PFAR)

    upper = jnp.logical_and(above0, jnp.logical_not(helper))

    def heads_of(h):
        return slice(h * HEAD_DIM, (h + 1) * HEAD_DIM)

    def send_fox(k):
        ref = br_fox.at[tp, piece(k)]
        send(ref, fsend.at[0], frecv.at[0, k], {"tp": far})
        if k == PC - 1:
            send(ref, fsend.at[2], frecv.at[1, k], {"tp": pfar})
        send(ref, fsend.at[1], frecv_near.at[0], {"tp": partner})

    def finish_rows(c):
        r = slice(c * rc, (c + 1) * rc)
        for h in range(H):
            br_fox[tp, r, heads_of(h)] = (o_ref[h, r, 0:HEAD_DIM] / o_ref[h, r, HEAD_DIM:]).astype(
                BF16
            )
        for k in pieces_of(c):
            send_fox(k)

    def merge_rows(c):
        for k in pieces_of(c):
            at, n = pieces[k]
            arrived(part_in.at[piece(k)], orecv.at[k])
            if k == pieces_of(c)[0]:
                arrived(stat_in.at[c], orecv.at[PC + c])
                pad_rows = jnp.zeros((128 - 2 * H, rc), F32)
                stats = jnp.concatenate([stat_in[c], pad_rows], axis=0).T
            r = slice(at, at + n)
            mine = slice(at - c * rc, at - c * rc + n)
            for h in range(H):
                m_in = stats[mine, h : h + 1]
                l_in = stats[mine, H + h : H + h + 1]
                part = part_in[r, heads_of(h)].astype(F32)
                old = m_ref[h, r, :]
                new = jnp.maximum(old, m_in)
                fade = jnp.exp2(old - new)
                grow = jnp.exp2(m_in - new)
                total = o_ref[h, r, HEAD_DIM:] * fade + l_in * grow
                br_fox[tp, r, heads_of(h)] = (
                    (o_ref[h, r, 0:HEAD_DIM] * fade + part * grow) / total
                ).astype(BF16)
            send_fox(k)

    def pair_dot(br, buf, side, r):
        first = 2 * side
        return jnp.dot(br[first, r, :], buf[first], preferred_element_type=F32) + jnp.dot(
            br[first + 1, r, :], buf[first + 1], preferred_element_type=F32
        )

    def lru_near():
        both = wl_buf.at[pl.ds(0, 2)]
        pltpu.make_async_copy(both, both, load_sem.at[8]).wait()
        arrived(both, wrecv_own.at[0])
        arrived(br_lru.at[partner], lrecv.at[PARTNER])
        for c in range(CH):
            oacc[chunk(c), :] = pair_dot(br_lru, wl_buf, y, chunk(c))

    def lru_relay():
        arrived(br_lru.at[far], lrecv.at[FAR])
        send(br_lru.at[far], lsend.at[1], lrecv.at[PFAR], {"tp": partner})

    def lru_far():
        for role in (FAR, PFAR):
            weight_wait(0, role)
        arrived(br_lru.at[pfar], lrecv.at[PFAR])
        for c in range(CH):
            oacc[chunk(c), :] += pair_dot(br_lru, wl_buf, 1 - y, chunk(c))

    @pl.when(upper)
    def _():
        for c in order[0:2]:
            diag_wait(c)
        attend(q_ref, own_st, j_bo, half, rows)

    @pl.when(above0)
    def _():
        for c in order[2:]:
            diag_wait(c)

    @pl.when(middle)
    def _():
        attend(q_far, far_st, j_bo, 0, half, qc=rc, after=send_partial)
        attend(q_ref, own_st, j_bo, 0, rows, qc=rc, after=finish_rows)

    @pl.when(upper)
    def _():
        attend(q_ref, own_st, j_bo, 0, half)

    @pl.when(top)
    def _():
        lru_near()
        merge_rows(0)
        merge_rows(1)
        lru_relay()
        merge_rows(2)
        lru_far()
        merge_rows(3)

    @pl.when(second_top)
    def _():
        for c in range(CH):
            merge_rows(c)

    @pl.when(z == 0)
    def _():
        for c in range(CH):
            finish_rows(c)

    weight_pass_bottom(FAR)
    weight_pass_bottom(PFAR)

    @pl.when(not_top)
    def _():
        lru_near()
        lru_relay()
        lru_far()

    for role in (FAR, PFAR):
        weight_wait(1, role)

    def fox_pass(k):
        arrived(br_fox.at[far, piece(k)], frecv.at[0, k])
        if k < PC - 1:
            send(br_fox.at[far, piece(k)], fsend.at[2], frecv.at[1, k], {"tp": partner})

    fox_pass(0)
    for k in range(PC):
        r = piece(k)
        if k + 1 < PC:
            fox_pass(k + 1)
        if k == 0:
            arrived(br_fox.at[partner], frecv_near.at[0])
        oacc[r, :] += pair_dot(br_fox, wf_buf, y, r)
        arrived(br_fox.at[pfar, r], frecv.at[1, k])
        out[r, :] = (oacc[r, :] + pair_dot(br_fox, wf_buf, 1 - y, r)).astype(out.dtype)

    for k in range(3):
        sent(tok_buf.at[0], tsend.at[k])
        sent(br_fox.at[0], fsend.at[k])
    sent(br_lru.at[pl.ds(0, 2)], lsend.at[0])
    sent(br_lru.at[0], lsend.at[1])
    sent(wl_buf.at[0], wsend.at[1])
    sent(wl_buf.at[pl.ds(0, 2)], wsend.at[2])

    @pl.when(above0)
    def _():
        sent(wl_buf.at[0], wsend.at[0])
        sent(wl_buf.at[pl.ds(0, 2)], wsend.at[3])

    @pl.when(top)
    def _():
        sent(wl_buf.at[pl.ds(0, 2)], wsend.at[4])

    @pl.when(z == 0)
    def _():
        sent(wl_buf.at[0], wsend.at[4])

    sent(own_cum, csend.at[0])
    top_half = pl.ds(0, half)
    need = all_across(x == 0)

    @pl.when(need)
    def _():
        sent(kv_buf.at[0], xsend.at[0])

    @pl.when(jnp.logical_and(second_top, jnp.logical_not(need)))
    def _():
        sent(kv_buf.at[0, top_half], xsend.at[0])

    for level in range(Z):

        @pl.when(z == level)
        def _():
            ups = (level < Z - 1) * rc + (level < Z - 1 and level != Z - 3) * (rc - cut)
            ups += (level == Z - 2) * cut
            if ups:
                sent(kv_buf.at[0, pl.ds(0, ups)], zfwd.at[0])
            overs = (2 * rc if level else 0) + (level == Z - 2) * (rc - cut)
            overs += (0 < level < Z - 1) * cut
            if overs:
                sent(kv_buf.at[0, pl.ds(0, overs)], xfwd.at[0])

    @pl.when(not_top)
    def _():
        sent(kv_buf.at[0], zsend.at[0])
        sent(cum_buf.at[pl.ds(0, 2)], csend.at[1])

    @pl.when(helped)
    def _():
        sent(q_ref, qsend.at[0])

    @pl.when(helper)
    def _():
        sent(part_out, osend.at[0])
        sent(stat_out, osend.at[1])

    @pl.when(sp < SP - 1)
    def _():
        halo_copy.wait_send()

    sent(others, esend.at[0])


def block_shards(SP, TP, X, *args):
    tokens, lru_in, gate_in, query_w = args[:4]
    (conv_weight, rg_w, ig_w, rate, decay_extra, forget, out_lru, out_fox) = args[6:]
    rows, dcols = tokens.shape
    D, lw = lru_in.shape
    fw = query_w.shape[1]
    oc = out_lru.shape[1] // TP
    tot = 2 * lw + 3 * fw
    H = fw // HEAD_DIM
    CH = 4
    rc = rows // CH
    bw = rg_w.shape[1]
    hbm = pl.BlockSpec(memory_space=pl.ANY)
    dma = pltpu.SemaphoreType.DMA
    V = pltpu.VMEM
    scratch = [
        V((TP, rows, dcols), BF16),
        V((D, tot), BF16),
        V((2, rc, tot), F32),
        V((2, rc, 1), F32),
        V((rows, lw), BF16),
        V((16, lw), BF16),
        V((rows + 8, lw), F32),
        V(conv_weight.shape, BF16),
        V((lw // bw, bw, bw), BF16),
        V((lw // bw, bw, bw), BF16),
        V((1, rate.shape[0]), F32),
        V((H, rows), F32),
        V((lw, lw), BF16),
        V((lw, lw), BF16),
        V((rows, lw), BF16),
        V((rows, fw), BF16),
        V((rows, lw), F32),
        V((lw // 128, rows, 128), F32),
        V((lw // 128, rows, 128), F32),
        V((8, lw), F32),
        V((8, lw), F32),
        V((8, lw), F32),
        V((SP, 2, lw), F32),
        V((SP, rows, 2 * fw), BF16),
        V((SP, H, rows), F32),
        V((H, rows, 128), F32),
        V((H, rows, 2 * HEAD_DIM), F32),
        V((rows, fw), BF16),
        V((H, rows, 128), F32),
        V((H, rows, 2 * HEAD_DIM), F32),
        V((rows, fw), BF16),
        V((CH, 2 * H, rc), F32),
        V((rows, fw), BF16),
        V((CH, 2 * H, rc), F32),
        V((TP, lw, oc), BF16),
        V((TP, fw, oc), BF16),
        V((TP, rows, lw), BF16),
        V((TP, rows, fw), BF16),
        V((rows, oc), F32),
        dma((9,)),
        dma((3,)),
        dma((1,)),
        dma((2, CH)),
        dma((1,)),
        dma((1,)),
        dma((1,)),
        dma((1,)),
        dma((2,)),
        dma((3,)),
        dma((1,)),
        dma((1,)),
        dma((1,)),
        dma((1,)),
        dma((3, CH + 1)),
        dma((5,)),
        dma((1,)),
        dma((2, 2, X)),
        dma((2,)),
        dma((3,)),
        dma((3,)),
        dma((1,)),
        dma((2, CH + 1)),
        dma((1,)),
        dma((2,)),
        dma((2,)),
        dma((2 * CH + 1,)),
    ]
    return pl.pallas_call(
        functools.partial(block_kernel, SP, TP, X, CH),
        out_shape=pltpu.VMEM((rows, oc), BF16),
        in_specs=[hbm] * 14,
        out_specs=pl.BlockSpec(memory_space=pltpu.VMEM),
        scratch_shapes=scratch,
        compiler_params=pltpu.CompilerParams(
            collective_id=1, has_side_effects=True, vmem_limit_bytes=60 * 1024 * 1024
        ),
    )(*args[:9], rate.reshape(1, -1), decay_extra, forget.T, out_lru, out_fox)


def columns_of(mesh):
    SP = mesh.shape["sp"]
    try:
        X = len({d.coords[0] for d in mesh.devices.flat})
    except AttributeError:
        X = 2
    return X if SP % X == 0 else 1


def solution(mesh):
    placed = (
        P("sp", "tp"),
        P(None, "tp"),
        P(None, "tp"),
        P(None, "tp"),
        P(None, "tp"),
        P(None, "tp"),
        P(),
        P(),
        P(),
        P(),
        P("sp", "tp"),
        P("sp", "tp"),
        P("tp", None),
        P("tp", None),
    )
    SP, TP, X = mesh.shape["sp"], mesh.shape["tp"], columns_of(mesh)
    small = X == 2 and TP == 4 and SP // X == 4
    body = functools.partial(block_shards if small else shards, SP, TP, X)
    return jax.shard_map(
        body, mesh=mesh, in_specs=placed, out_specs=P("sp", "tp"), check_vma=False
    )
```
